256 devices in a mesh: grp: 2 (over y), fs: 16 (over z), tp: 8 (over x, core).
Axes of the slice: x: 4, y: 2, z: 16, core: 2. Of those that a mesh axis runs over, the one named last changes fastest.
The devices are a block of a 4x16x16 slice.
Arguments:
- stream_in: bfloat16 [12288, 2048], P(('grp', 'fs'), 'tp'), parts along dimension 0, may hold values from -6 to 6
- gain_before: bfloat16 [2048], P('tp'), may hold values from 0.099609375 to 1.8984375
- gain_mixer: bfloat16 [2048], P('tp'), may hold values from 0.099609375 to 1.8984375
- gain_after: bfloat16 [2048], P('tp'), may hold values from 0.099609375 to 1.8984375
- w_gate: bfloat16 [2048, 5632], P('fs', 'tp'), may hold values from -0.125 to 0.125
- w_upward: bfloat16 [2048, 5632], P('fs', 'tp'), may hold values from -0.125 to 0.125
- w_down: bfloat16 [5632, 2048], P('tp', 'fs'), may hold values from -0.078125 to 0.078125
- w_value: bfloat16 [2048, 1024], P('fs', 'tp'), may hold values from -0.125 to 0.125
- w_glu_gate: bfloat16 [2048, 1024], P('fs', 'tp'), may hold values from -0.125 to 0.125
- conv_taps: bfloat16 [31, 1024], P(None, 'tp'), may hold values from -1 to 1
- chan_gain: bfloat16 [1024], P('tp'), may hold values from 0.099609375 to 1.8984375
- chan_bias: bfloat16 [1024], P('tp'), may hold values from -3 to 3
- w_mix_out: bfloat16 [1024, 2048], P('tp', 'fs'), may hold values from -0.1875 to 0.1875
Outputs:
- stream_out: bfloat16 [12288, 2048], P(('grp', 'fs'), 'tp'), parts along dimension 0
The draws below stay inside these ranges and needn't reach their ends.
There are 2 independent parts, one for each index of `grp`. The reference program is written for one: setup_inputs(seed, part) draws one part's arguments, and reference() takes and returns one part's arrays. A program takes and returns all parts, laid end to end along the dimension named above; an argument that names none is the same for every part. Nothing has to cross between parts.
All inputs are finite; a program needn't handle non-finite values.
Results may differ from the reference program's by a relative error of at most 0.017.
Values may be sent and summed in bfloat16 or wider, within the bound.
A program may use at most 64 MiB of HBM per device.

```python
import jax
import jax.numpy as jnp
from jax import lax

D = 2048
FF = 5632
CHAN = 1024
KERNEL = 31
LEN = 128
TOKENS = 6144
N_TP = 8


def steps_of(rng, dims, split, low, high):
    loudness, own = 1.0, jax.random.fold_in(rng, 6)
    for dim, parts in split:
        draws = jnp.exp(jax.random.uniform(jax.random.fold_in(own, dim), (parts,), jnp.float32, low / len(split), high / len(split)))
        loudness = loudness * jnp.repeat(draws, dims[dim] // parts).reshape([-1 if axis == dim else 1 for axis in range(len(dims))])
    return loudness


def normal_values(own_key, dims, scale, limit, shards=(), kind=jnp.bfloat16):
    entries = scale * jax.random.normal(own_key, dims, jnp.float32)
    if shards:
        entries = entries * steps_of(own_key, dims, shards, -0.22, 0.18)
    return jnp.clip(entries, -limit, limit).astype(kind)


def setup_inputs(seed: int = 0, part: int = 0) -> dict:
    keys = jax.random.split(jax.random.key(seed), 14)
    part_keys = jax.random.split(jax.random.fold_in(keys[13], part), 14)
    stream_in = normal_values(part_keys[0], (TOKENS, D), 1.0, 6.0, ((0, 16), (1, 8)))
    gain_before = jnp.clip(1.0 + 0.18 * jax.random.normal(keys[1], (D,), jnp.float32), 0.099609375, 1.8984375).astype(jnp.bfloat16)
    gain_mixer = jnp.clip(1.0 + 0.18 * jax.random.normal(keys[2], (D,), jnp.float32), 0.099609375, 1.8984375).astype(jnp.bfloat16)
    gain_after = jnp.clip(1.0 + 0.18 * jax.random.normal(keys[3], (D,), jnp.float32), 0.099609375, 1.8984375).astype(jnp.bfloat16)
    w_gate = normal_values(keys[4], (D, FF), D ** -0.5, 0.125, ((0, 16), (1, 8)))
    w_upward = normal_values(keys[5], (D, FF), D ** -0.5, 0.125, ((0, 16), (1, 8)))
    w_down = normal_values(keys[6], (FF, D), FF ** -0.5, 0.078125, ((0, 8), (1, 16)))
    w_value = normal_values(keys[7], (D, CHAN), D ** -0.5, 0.125, ((0, 16), (1, 8)))
    w_glu_gate = normal_values(keys[8], (D, CHAN), D ** -0.5, 0.125, ((0, 16), (1, 8)))
    conv_taps = normal_values(keys[9], (KERNEL, CHAN), KERNEL ** -0.5, 1.0, ((1, 8),))
    chan_gain = jnp.clip(1.0 + 0.18 * jax.random.normal(keys[10], (CHAN,), jnp.float32), 0.099609375, 1.8984375).astype(jnp.bfloat16)
    chan_bias = normal_values(keys[11], (CHAN,), 0.5, 3.0, ((0, 8),))
    w_mix_out = normal_values(keys[12], (CHAN, D), CHAN ** -0.5, 0.1875, ((0, 8), (1, 16)))
    return dict(stream_in=stream_in, gain_before=gain_before, gain_mixer=gain_mixer, gain_after=gain_after, w_gate=w_gate, w_upward=w_upward, w_down=w_down, w_value=w_value, w_glu_gate=w_glu_gate, conv_taps=conv_taps, chan_gain=chan_gain, chan_bias=chan_bias, w_mix_out=w_mix_out)


epsilon = 1e-06

def rms_rows(stream, weights):
    values = stream.astype(jnp.float32)
    inverse = lax.rsqrt(lax.optimization_barrier(jnp.mean(values * values, axis=1, keepdims=True)) + epsilon)
    return (values * inverse * weights.astype(jnp.float32)).astype(jnp.bfloat16)

def shard_sums(left, right):
    width = left.shape[1] // N_TP

    def add_shard(running, number):
        operand = lax.dynamic_slice_in_dim(left, number * width, width, 1)
        factor = lax.dynamic_slice_in_dim(right, number * width, width, 0)
        partial_term = jnp.dot(operand, factor, preferred_element_type=jnp.float32).astype(jnp.bfloat16)
        partial_term = lax.optimization_barrier(partial_term)
        return (running + partial_term.astype(jnp.float32), None)
    initial = jnp.zeros((left.shape[0], right.shape[1]), jnp.float32)
    result, unused = lax.scan(add_shard, initial, jnp.arange(N_TP, dtype=jnp.int32))
    return result

def feed_forward(rows, w_gate, w_upward, w_down):
    gate = jnp.dot(rows, w_gate, preferred_element_type=jnp.float32)
    upward = jnp.dot(rows, w_upward, preferred_element_type=jnp.float32)
    hidden = (jax.nn.silu(gate) * upward).astype(jnp.bfloat16)
    return shard_sums(hidden, w_down)

def conv_module(rows, w_value, w_glu_gate, conv_taps, chan_gain, chan_bias, w_mix_out):
    value = jnp.dot(rows, w_value, preferred_element_type=jnp.float32)
    gating = jnp.dot(rows, w_glu_gate, preferred_element_type=jnp.float32)
    glued = value * jax.nn.sigmoid(gating)
    channels = glued.shape[1]
    grouped = glued.reshape(-1, LEN, channels)
    padded = jnp.pad(grouped, ((0, 0), (KERNEL - 1, 0), (0, 0)))
    taps = conv_taps.astype(jnp.float32)
    conv_sum = jnp.zeros_like(grouped)
    for lag_index in range(KERNEL):
        conv_sum = conv_sum + taps[lag_index] * padded[:, lag_index:lag_index + LEN]
    flat = conv_sum.reshape(-1, channels)
    average = lax.optimization_barrier(jnp.mean(flat, axis=1, keepdims=True))
    spread = lax.optimization_barrier(jnp.mean(flat * flat, axis=1, keepdims=True)) - average * average
    normed = (flat - average) * lax.rsqrt(spread + epsilon) * chan_gain.astype(jnp.float32) + chan_bias.astype(jnp.float32)
    mixed = jax.nn.silu(normed).astype(jnp.bfloat16)
    return shard_sums(mixed, w_mix_out)

def reference(stream_in, gain_before, gain_mixer, gain_after, w_gate, w_upward, w_down, w_value, w_glu_gate, conv_taps, chan_gain, chan_bias, w_mix_out):
    first = (stream_in.astype(jnp.float32) + 0.5 * feed_forward(rms_rows(stream_in, gain_before), w_gate, w_upward, w_down)).astype(jnp.bfloat16)
    branch = conv_module(rms_rows(first, gain_mixer), w_value, w_glu_gate, conv_taps, chan_gain, chan_bias, w_mix_out)
    second = (first.astype(jnp.float32) + branch).astype(jnp.bfloat16)
    third = second.astype(jnp.float32) + 0.5 * feed_forward(rms_rows(second, gain_after), w_gate, w_upward, w_down)
    return third.astype(jnp.bfloat16)
```

```python
import jax
import jax.numpy as jnp
from jax import lax
from jax.experimental import pallas as pl
from jax.experimental.pallas import tpu as pltpu
from jax.sharding import PartitionSpec as P

MESH = pl.DeviceIdType.MESH
LEN = 128
EPS = 1e-06
LANES = 128
CHUNKS = 3
BF16, F32 = jnp.bfloat16, jnp.float32

GU_X, WD_X, VM_X = 512, 208, 128


def remote(src, dst, send_sem, recv_sem, where):
    return pltpu.make_async_remote_copy(
        src_ref=src,
        dst_ref=dst,
        send_sem=send_sem,
        recv_sem=recv_sem,
        device_id=where,
        device_id_type=MESH,
    )


def layer_kernel(
    n_fs,
    n_tp,
    s_in,
    gu_in,
    wd_in,
    vm_in,
    pk_in,
    taps_in,
    out,
    gu,
    wd,
    vm,
    mxb,
    pk,
    gf,
    cgb,
    sb0,
    sb1,
    sb3,
    cvb,
    ub,
    mixed,
    hid,
    pad,
    sdo,
    sdi,
    acc,
    obo,
    obi,
    nbo,
    nbi,
    load_sem,
    z_recv,
    z_send,
    y_recv,
    y_send,
    pk_recv,
    pk_send,
    mx_recv,
    mx_send,
    ag_recv,
    ag_send,
    rs_recv,
    rs_send,
):
    z, t, g = lax.axis_index("fs"), lax.axis_index("tp"), lax.axis_index("grp")
    parity = lax.rem(g, 2)
    partner = {"grp": g + 1 - 2 * parity}
    z_right = {"fs": lax.rem(z + 1, n_fs)}
    z_left = {"fs": lax.rem(z + n_fs - 1, n_fs)}
    chips = n_tp // 2
    x, core = t // 2, lax.rem(t, 2)
    xr, xl, xo = lax.rem(x + 1, chips), lax.rem(x + 3, chips), lax.rem(x + 2, chips)
    other = 1 - core
    sib = {"tp": 2 * x + other}
    x_right, x_left = {"tp": 2 * xr + core}, {"tp": 2 * xl + core}

    nq, rows, width = sb0.shape[0], sb0.shape[1], s_in.shape[1]
    half = rows // 2
    feat = width * n_tp
    k_rows = gu_in.shape[0]
    chan_w = vm_in.shape[1] // 3
    chan = chan_w * n_tp
    steps = n_fs // 2

    def own_loads():
        yield pltpu.make_async_copy(gu_in, gu.at[pl.ds(pl.multiple_of(z * k_rows, k_rows), k_rows), :], load_sem.at[0])
        yield pltpu.make_async_copy(
            wd_in, wd.at[z // 2, :, pl.ds(pl.multiple_of(lax.rem(z, 2) * LANES, LANES), LANES)], load_sem.at[1]
        )
        yield pltpu.make_async_copy(vm_in, vm.at[pl.ds(pl.multiple_of(z * k_rows, k_rows), k_rows), :], load_sem.at[2])
        yield pltpu.make_async_copy(pk_in, pk.at[t], load_sem.at[3])
        for q in range(nq):
            yield pltpu.make_async_copy(
                s_in.at[pl.ds(q * rows, rows), :],
                sb0.at[q, :, pl.ds(pl.multiple_of(t * width, width), width)],
                load_sem.at[4 + q],
            )

    for copy in own_loads():
        copy.start()

    barrier = pltpu.get_barrier_semaphore()
    peers = [z_right, z_left, partner] + [{"tp": lax.rem(t + i, n_tp)} for i in range(1, n_tp)]
    for peer in peers:
        pl.semaphore_signal(barrier, inc=1, device_id=peer, device_id_type=MESH)
    pl.semaphore_wait(barrier, len(peers))

    for copy in own_loads():
        copy.wait()

    def piece(kind, f, share):
        r0 = pl.multiple_of(f * k_rows, k_rows)
        if kind == 0:
            cols = pl.ds(pl.multiple_of(parity * GU_X, LANES), GU_X) if share == 0 else pl.ds(2 * GU_X, gu.shape[1] - 2 * GU_X)
            return gu.at[pl.ds(r0, k_rows), cols]
        if kind == 1:
            rws = pl.ds(pl.multiple_of(parity * WD_X, 16), WD_X) if share == 0 else pl.ds(2 * WD_X, wd.shape[1] - 2 * WD_X)
            return wd.at[f // 2, rws, pl.ds(pl.multiple_of(lax.rem(f, 2) * LANES, LANES), LANES)]
        cols = pl.ds(pl.multiple_of(parity * VM_X, LANES), VM_X) if share == 0 else pl.ds(2 * VM_X, vm.shape[1] - 2 * VM_X)
        return vm.at[pl.ds(r0, k_rows), cols]

    def many(kind, share, count):
        if kind == 0:
            w = GU_X if share == 0 else gu.shape[1] - 2 * GU_X
            return gu.at[pl.ds(0, count * k_rows), pl.ds(0, w)]
        if kind == 1:
            r = WD_X if share == 0 else wd.shape[1] - 2 * WD_X
            return wd.at[pl.ds(0, count), pl.ds(0, r), pl.ds(0, LANES)]
        w = VM_X if share == 0 else vm.shape[1] - 2 * VM_X
        return vm.at[pl.ds(0, count * k_rows), pl.ds(0, w)]

    def origin(way, s):
        return lax.rem(z + n_fs - s, n_fs) if way == 0 else lax.rem(z + s, n_fs)

    def reach(way, share):
        return steps if way == share else steps - 1

    def z_copy(kind, way, share, s_next):
        ref = piece(kind, origin(way, s_next - 1), share)
        return remote(
            ref,
            ref,
            z_send.at[kind, way, share],
            z_recv.at[kind, way, share, s_next - 1],
            z_right if way == 0 else z_left,
        )

    def z_arrival(kind, way, share, s):
        ref = piece(kind, origin(way, s), share)
        return remote(
            ref, ref, z_send.at[kind, way, share], z_recv.at[kind, way, share, s - 1], z_right if way == 0 else z_left
        )

    def y_copy(kind, way, s):
        ref = piece(kind, origin(way, s), 0)
        return remote(ref, ref, y_send.at[kind, way], y_recv.at[kind, way], partner)

    def spread_mix(f):
        dest, b = f // 2, lax.rem(f, 2)
        src = vm.at[pl.ds(pl.multiple_of(f * k_rows, k_rows), k_rows), pl.ds(2 * chan_w, chan_w)]
        dst = mxb.at[
            pl.ds(pl.multiple_of(t * chan_w, chan_w), chan_w), pl.ds(pl.multiple_of(b * LANES, LANES), LANES)
        ]

        @pl.when(dest != t)
        def _():
            remote(src, dst, mx_send.at[0], mx_recv.at[t, b], {"tp": dest}).start()

        @pl.when(dest == t)
        def _():
            pltpu.make_async_copy(src, dst, mx_recv.at[t, b]).start()

    def relay(kinds, s, last):
        for share in range(2):
            for way in range(2):
                for kind in kinds:
                    far = reach(way, share)
                    if isinstance(s, int) and s > far:
                        continue
                    z_arrival(kind, way, share, s).wait_recv()
                    if not isinstance(s, int) or s < far:
                        z_copy(kind, way, share, s + 1).start()
                    if share == 0:
                        y_copy(kind, way, s).start()
                    if kind == 2 and share == 1:
                        spread_mix(origin(way, s))

    def relay_loop(kinds, lo, hi, extra=None):
        @pl.loop(lo, hi)
        def _(s):
            relay(kinds, s, None)
            if extra is not None:
                extra(s)

    def y_wait(kind):
        for way in range(2):
            ref = many(kind, 0, reach(way, 0))
            remote(ref, ref, y_send.at[kind, way], y_recv.at[kind, way], partner).wait_recv()

    def block(buf, w, q, b, part=None):
        rws = slice(None) if part is None else pl.ds(part * half, half)
        return buf.at[q, rws, pl.ds(pl.multiple_of(b * w, w), w)]

    def ag_copy(n, ref, q, s_i, r_i, where):
        return remote(ref, ref, ag_send.at[n, q, s_i], ag_recv.at[n, q, r_i], where)

    def ag_start(n, buf, w, q):
        own = block(buf, w, q, t)
        ag_copy(n, own, q, 1, 1, x_right).start()
        ag_copy(n, own, q, 2, 2, x_left).start()
        ag_copy(n, own, q, 0, 0, sib).start()

    def ag_relay(n, buf, w, q):
        b_l, b_r = 2 * xl + core, 2 * xr + core
        ag_copy(n, block(buf, w, q, b_l), q, 1, 1, x_right).wait_recv()
        ag_copy(n, block(buf, w, q, b_l, 0), q, 4, 3, x_right).start()
        ag_copy(n, block(buf, w, q, b_l), q, 3, 5, sib).start()
        ag_copy(n, block(buf, w, q, b_r), q, 2, 2, x_left).wait_recv()
        ag_copy(n, block(buf, w, q, b_r, 1), q, 6, 4, x_left).start()
        ag_copy(n, block(buf, w, q, b_r), q, 5, 6, sib).start()

    def ag_opposite(n, buf, w, q):
        b_o = 2 * xo + core
        ag_copy(n, block(buf, w, q, b_o, 0), q, 4, 3, x_right).wait_recv()
        ag_copy(n, block(buf, w, q, b_o, 0), q, 7, 7, sib).start()
        ag_copy(n, block(buf, w, q, b_o, 1), q, 6, 4, x_left).wait_recv()
        ag_copy(n, block(buf, w, q, b_o, 1), q, 8, 8, sib).start()

    def ag_end(n, buf, w, q):
        ag_copy(n, block(buf, w, q, 2 * x + other), q, 0, 0, sib).wait_recv()
        ag_copy(n, block(buf, w, q, 2 * xl + other), q, 3, 5, sib).wait_recv()
        ag_copy(n, block(buf, w, q, 2 * xr + other), q, 5, 6, sib).wait_recv()
        ag_copy(n, block(buf, w, q, 2 * xo + other, 0), q, 7, 7, sib).wait_recv()
        ag_copy(n, block(buf, w, q, 2 * xo + other, 1), q, 8, 8, sib).wait_recv()

    def ag_drain(n, buf, w, q):
        whole, part = block(buf, w, q, t), block(buf, w, q, t, 0)
        for i in range(9):
            ref = part if i in (4, 6, 7, 8) else whole
            ag_copy(n, ref, q, i, 0, sib).wait_send()

    def rs_copy(src, dst, n, q, i, where):
        return remote(src, dst, rs_send.at[n, q, i], rs_recv.at[n, q, i], where)

    order = (xo, xr, xl, x)
    sib_copy = lambda n, q, k: rs_copy(sdo.at[n, q, k], sdi.at[n, q, k], n, q, k, sib)

    def opp_copy(n, q, i):
        ref = pl.ds(i * half, half)
        return rs_copy(obo.at[n, q, ref], obi.at[n, q, ref], n, q, 4 + i, x_right if i == 0 else x_left)

    def nb_copy(n, q, i):
        return rs_copy(nbo.at[n, q, i], nbi.at[n, q, i], n, q, 6 + i, x_right if i == 0 else x_left)

    def rs_partials(n, q, base):
        h = hid[pl.ds(pl.multiple_of(base, 16), rows), :]
        for k in range(4):
            sdo[n, q, k] = jnp.dot(h, wd[2 * order[k] + other], preferred_element_type=F32).astype(BF16)
            sib_copy(n, q, k).start()
            acc[q, k] = jnp.dot(h, wd[2 * order[k] + core], preferred_element_type=F32)

    def rs_opposite(n, q):
        sib_copy(n, q, 0).wait_recv()
        obo[n, q] = (acc[q, 0] + sdi[n, q, 0].astype(F32)).astype(BF16)
        opp_copy(n, q, 0).start()
        opp_copy(n, q, 1).start()

    def rs_neighbours(n, q):
        for i in range(2):
            sib_copy(n, q, 1 + i).wait_recv()
            opp_copy(n, q, i).wait_recv()
            mine, far = pl.ds(i * half, half), pl.ds((1 - i) * half, half)
            nbo[n, q, i, mine] = (
                acc[q, 1 + i, mine] + sdi[n, q, 1 + i, mine].astype(F32) + obi[n, q, mine].astype(F32)
            ).astype(BF16)
            nbo[n, q, i, far] = (acc[q, 1 + i, far] + sdi[n, q, 1 + i, far].astype(F32)).astype(BF16)
            nb_copy(n, q, i).start()

    def rs_total(n, q):
        sib_copy(n, q, 3).wait_recv()
        nb_copy(n, q, 0).wait_recv()
        nb_copy(n, q, 1).wait_recv()
        return (
            acc[q, 3] + sdi[n, q, 3].astype(F32) + nbi[n, q, 0].astype(F32) + nbi[n, q, 1].astype(F32)
        )

    def rs_drain(n, q):
        for k in range(4):
            sib_copy(n, q, k).wait_send()
        for i in range(2):
            opp_copy(n, q, i).wait_send()
            nb_copy(n, q, i).wait_send()

    def norm_rows(buf, q, r, base):
        @pl.loop(0, rows // 16)
        def _(i):
            rws = pl.ds(pl.multiple_of(i * 16, 16), 16)
            v = buf[q, rws, :].astype(F32)
            inverse = lax.rsqrt(jnp.sum(v * v, axis=1, keepdims=True) / feat + EPS)
            ub[pl.ds(pl.multiple_of(base + i * 16, 16), 16), :] = (v * inverse * gf[r : r + 1, :]).astype(BF16)

    n_full = gu.shape[1] // (2 * LANES)
    tail = gu.shape[1] - n_full * 2 * LANES

    def hidden_tile(n, lo, count):
        c0 = pl.multiple_of(n * 2 * LANES, LANES)
        r = jnp.dot(ub[pl.ds(lo, count), :], gu[:, pl.ds(c0, 2 * LANES)], preferred_element_type=F32)
        a, b = r[:, :LANES], r[:, LANES:]
        hid[pl.ds(lo, count), pl.ds(pl.multiple_of(n * LANES, LANES), LANES)] = (jax.nn.silu(a) * b).astype(BF16)

    def hidden_tail(lo, count):
        r = jnp.dot(ub[pl.ds(lo, count), :], gu[:, n_full * 2 * LANES :], preferred_element_type=F32)
        a = pltpu.roll(r, tail // 2, 1)
        hid[pl.ds(lo, count), n_full * LANES :] = (jax.nn.silu(r) * a)[:, : tail // 2].astype(BF16)

    def conv(q):
        b0 = pl.multiple_of(q * rows, 16)
        r = jnp.dot(ub[pl.ds(b0, rows), :], vm[:, : 2 * chan_w], preferred_element_type=F32)
        glued = r[:, :chan_w] * jax.nn.sigmoid(r[:, chan_w:])
        for i in range(rows // LEN):
            pad[i, 32:, :] = glued[i * LEN : (i + 1) * LEN]
        n_taps = taps_in.shape[0]
        taps = taps_in[...].astype(F32)
        for i in range(rows // LEN):
            total = jnp.zeros((LEN, chan_w), F32)
            for k in range(n_taps):
                total = total + taps[k : k + 1, :] * pad[i, 33 - n_taps + k : 33 - n_taps + k + LEN, :]
            cvb[q, i * LEN : (i + 1) * LEN, pl.ds(pl.multiple_of(t * chan_w, chan_w), chan_w)] = total.astype(BF16)

    def channel_norm(q):
        @pl.loop(0, rows // 16)
        def _(i):
            rws = pl.ds(pl.multiple_of(i * 16, 16), 16)
            v = cvb[q, rws, :].astype(F32)
            mu = jnp.sum(v, axis=1, keepdims=True) / chan
            msq = jnp.sum(v * v, axis=1, keepdims=True) / chan
            w = (v - mu) * lax.rsqrt(msq - mu * mu + EPS) * cgb[3:4, :] + cgb[11:12, :]
            mixed[rws, :] = jax.nn.silu(w).astype(BF16)

    def own_cols(buf, q):
        return buf[q, :, pl.ds(pl.multiple_of(t * width, width), width)]

    def each(fn):
        pl.loop(0, nq)(fn)

    def z_begin(kinds):
        for kind in kinds:
            for share in range(2):
                for way in range(2):
                    z_copy(kind, way, share, 1).start()

    z_begin((0,))
    each(lambda q: ag_start(0, sb0, width, q))

    def pk_copy(i):
        return remote(pk.at[t], pk.at[t], pk_send.at[i - 1], pk_recv.at[t], {"tp": lax.rem(t + i, n_tp)})

    for i in range(1, n_tp):
        pk_copy(i).start()
    z_begin((1, 2))
    spread_mix(z)

    pad[:, :32, :] = jnp.zeros((pad.shape[0], 32, chan_w), F32)

    relay((0,), 1, None)
    each(lambda q: ag_relay(0, sb0, width, q))
    relay((0,), 2, None)
    each(lambda q: ag_opposite(0, sb0, width, q))
    for i in range(1, n_tp):
        b = lax.rem(t + i, n_tp)
        remote(pk.at[b], pk.at[b], pk_send.at[i - 1], pk_recv.at[b], {"tp": b}).wait_recv()
    for b in range(n_tp):
        gf[:, b * width : (b + 1) * width] = pk[b]
        cgb[0:8, b * chan_w : (b + 1) * chan_w] = pk[b][:, :chan_w]
        cgb[8:16, b * chan_w : (b + 1) * chan_w] = pk[b][:, chan_w : 2 * chan_w]
    relay((0,), 3, None)
    each(lambda q: ag_end(0, sb0, width, q))

    def early_norm(s):
        q = s - 4

        @pl.when(q < nq)
        def _():
            norm_rows(sb0, q, 0, q * rows)

    relay_loop((0,), 4, steps - 1, early_norm)
    for s in (steps - 1, steps):
        relay((0,), s, None)

    relay_loop((1, 2), 1, 4)
    y_wait(0)

    tokens = nq * rows

    def tiles(s):
        hidden_tile(2 * (s - 4), 0, tokens)

        @pl.when(2 * (s - 4) + 1 < n_full)
        def _():
            hidden_tile(2 * (s - 4) + 1, 0, tokens)

    relay_loop((1, 2), 4, steps - 1, tiles)
    hidden_tail(0, tokens)
    for s in (steps - 1, steps):
        relay((1, 2), s, None)
    y_wait(1)

    each(lambda q: rs_partials(0, q, q * rows))
    each(lambda q: rs_opposite(0, q))
    each(lambda q: rs_neighbours(0, q))

    def first(q):
        total = rs_total(0, q)
        sb1[q, :, pl.ds(pl.multiple_of(t * width, width), width)] = (
            own_cols(sb0, q).astype(F32) + 0.5 * total
        ).astype(BF16)
        ag_start(1, sb1, width, q)

    each(first)
    each(lambda q: ag_relay(1, sb1, width, q))
    y_wait(2)
    each(lambda q: ag_opposite(1, sb1, width, q))

    def conv_stage(q):
        ag_end(1, sb1, width, q)
        norm_rows(sb1, q, 1, q * rows)
        conv(q)
        ag_start(2, cvb, chan_w, q)

    each(conv_stage)
    each(lambda q: ag_relay(2, cvb, chan_w, q))
    each(lambda q: ag_opposite(2, cvb, chan_w, q))

    for b in range(n_tp):
        for i in range(2):
            ref = mxb.at[pl.ds(b * chan_w, chan_w), pl.ds(i * LANES, LANES)]
            pltpu.make_async_copy(ref, ref, mx_recv.at[b, i]).wait()

    def mix_stage(q):
        ag_end(2, cvb, chan_w, q)
        channel_norm(q)
        branch = jnp.dot(mixed[...], mxb[...], preferred_element_type=F32)
        sb3[q, :, pl.ds(pl.multiple_of(t * width, width), width)] = (
            own_cols(sb1, q).astype(F32) + branch
        ).astype(BF16)
        ag_start(3, sb3, width, q)

    each(mix_stage)
    each(lambda q: ag_relay(3, sb3, width, q))
    each(lambda q: ag_opposite(3, sb3, width, q))

    def ffn_stage(q):
        base = pl.multiple_of(q * rows, 16)
        ag_end(3, sb3, width, q)
        norm_rows(sb3, q, 2, base)

        @pl.loop(0, n_full)
        def _(n):
            hidden_tile(n, base, rows)

        hidden_tail(base, rows)
        rs_partials(1, q, base)

    each(ffn_stage)
    each(lambda q: rs_opposite(1, q))
    each(lambda q: rs_neighbours(1, q))

    def last(q):
        total = rs_total(1, q)
        out[pl.ds(pl.multiple_of(q * rows, 16), rows), :] = (
            own_cols(sb3, q).astype(F32) + 0.5 * total
        ).astype(BF16)

    each(last)

    for kind in range(3):
        for way in range(2):
            for share in range(2):
                ref = many(kind, share, reach(way, share))
                remote(ref, ref, z_send.at[kind, way, share], z_recv.at[kind, way, share, 0], z_right).wait_send()
            ref = many(kind, 0, reach(way, 0))
            remote(ref, ref, y_send.at[kind, way], y_recv.at[kind, way], partner).wait_send()
    for i in range(1, n_tp):
        pk_copy(i).wait_send()
    ref = mxb.at[pl.ds(0, (n_tp - 1) * chan_w), :]
    remote(ref, ref, mx_send.at[0], mx_recv.at[0, 0], sib).wait_send()

    def drain(q):
        for n, buf, w in ((0, sb0, width), (1, sb1, width), (2, cvb, chan_w), (3, sb3, width)):
            ag_drain(n, buf, w, q)
        for n in range(2):
            rs_drain(n, q)

    each(drain)


def solution(mesh):
    n_fs, n_tp = mesh.shape["fs"], mesh.shape["tp"]

    def local(
        stream_in,
        gain_before,
        gain_mixer,
        gain_after,
        w_gate,
        w_upward,
        w_down,
        w_value,
        w_glu_gate,
        conv_taps,
        chan_gain,
        chan_bias,
        w_mix_out,
    ):
        tokens, width = stream_in.shape
        k_rows, hidden = w_gate.shape
        chan_w = w_value.shape[1]
        pieces = []
        for c in range(0, hidden, LANES):
            pieces += [w_gate[:, c : c + LANES], w_upward[:, c : c + LANES]]
        gu_in = jnp.concatenate(pieces, axis=1)
        vm_in = jnp.concatenate([w_value, w_glu_gate, w_mix_out], axis=1)
        zero = jnp.zeros((4, width), F32)
        pk_in = jnp.concatenate(
            [
                gain_before[None].astype(F32),
                gain_mixer[None].astype(F32),
                gain_after[None].astype(F32),
                jnp.concatenate([chan_gain, chan_bias])[None].astype(F32),
                zero,
            ],
            axis=0,
        )
        nq = CHUNKS
        rows = tokens // nq
        feat, chan = width * n_tp, chan_w * n_tp
        vmem = pltpu.VMEM
        dma = pltpu.SemaphoreType.DMA
        any_space = pl.BlockSpec(memory_space=pl.ANY)
        in_vmem = pl.BlockSpec(memory_space=pltpu.VMEM)
        return pl.pallas_call(
            lambda *refs: layer_kernel(n_fs, n_tp, *refs),
            out_shape=jax.ShapeDtypeStruct((tokens, width), BF16),
            in_specs=[any_space] * 5 + [in_vmem],
            out_specs=in_vmem,
            scratch_shapes=[
                vmem((n_fs * k_rows, 2 * hidden), BF16),
                vmem((n_fs // 2, hidden, 2 * LANES), BF16),
                vmem((n_fs * k_rows, 3 * chan_w), BF16),
                vmem((chan, 2 * LANES), BF16),
                vmem((n_tp, 8, width), F32),
                vmem((8, feat), F32),
                vmem((16, chan), F32),
                vmem((nq, rows, feat), BF16),
                vmem((nq, rows, feat), BF16),
                vmem((nq, rows, feat), BF16),
                vmem((nq, rows, chan), BF16),
                vmem((tokens, feat), BF16),
                vmem((rows, chan), BF16),
                vmem((tokens, hidden), BF16),
                vmem((rows // LEN, LEN + 32, chan_w), F32),
                vmem((2, nq, 4, rows, width), BF16),
                vmem((2, nq, 4, rows, width), BF16),
                vmem((nq, 4, rows, width), F32),
                vmem((2, nq, rows, width), BF16),
                vmem((2, nq, rows, width), BF16),
                vmem((2, nq, 2, rows, width), BF16),
                vmem((2, nq, 2, rows, width), BF16),
                dma((4 + nq,)),
                dma((3, 2, 2, n_fs // 2)),
                dma((3, 2, 2)),
                dma((3, 2)),
                dma((3, 2)),
                dma((n_tp,)),
                dma((n_tp - 1,)),
                dma((n_tp, 2)),
                dma((1,)),
                dma((4, nq, 9)),
                dma((4, nq, 9)),
                dma((2, nq, 8)),
                dma((2, nq, 8)),
            ],
            compiler_params=pltpu.CompilerParams(
                collective_id=0, has_side_effects=True, vmem_limit_bytes=60 * 1024 * 1024
            ),
        )(stream_in, gu_in, w_down, vm_in, pk_in, conv_taps)

    in_specs = (
        P(("grp", "fs"), "tp"),
        P("tp"),
        P("tp"),
        P("tp"),
        P("fs", "tp"),
        P("fs", "tp"),
        P("tp", "fs"),
        P("fs", "tp"),
        P("fs", "tp"),
        P(None, "tp"),
        P("tp"),
        P("tp"),
        P("tp", "fs"),
    )
    out_specs = P(("grp", "fs"), "tp")
    return jax.shard_map(local, mesh=mesh, in_specs=in_specs, out_specs=out_specs, check_vma=False)
```

```python
import jax
import jax.numpy as jnp
from jax import lax
from jax.experimental import pallas as pl
from jax.experimental.pallas import tpu as pltpu
from jax.sharding import PartitionSpec as P

MESH = pl.DeviceIdType.MESH
LEN = 128
EPS = 1e-06
LANES = 128
CHUNKS = 3
BF16, F32 = jnp.bfloat16, jnp.float32

GU_X, WD_X, VM_X = 512, 208, 128


def remote(src, dst, send_sem, recv_sem, where):
    return pltpu.make_async_remote_copy(
        src_ref=src,
        dst_ref=dst,
        send_sem=send_sem,
        recv_sem=recv_sem,
        device_id=where,
        device_id_type=MESH,
    )


def layer_kernel(
    n_fs,
    n_tp,
    s_in,
    gate_in,
    up_in,
    wd_in,
    value_in,
    glu_in,
    mix_in,
    taps_in,
    before_in,
    mixer_in,
    after_in,
    cgain_in,
    cbias_in,
    out,
    gu,
    wd,
    vm,
    mxb,
    pk,
    gf,
    cgb,
    sb0,
    sb1,
    sb3,
    cvb,
    ub,
    mixed,
    hid,
    pad,
    sdo,
    sdi,
    acc,
    obo,
    obi,
    nbo,
    nbi,
    load_sem,
    z_recv,
    z_send,
    y_recv,
    y_send,
    pk_recv,
    pk_send,
    mx_recv,
    mx_send,
    ag_recv,
    ag_send,
    rs_recv,
    rs_send,
):
    z, t, g = lax.axis_index("fs"), lax.axis_index("tp"), lax.axis_index("grp")
    parity = lax.rem(g, 2)
    partner = {"grp": g + 1 - 2 * parity}
    z_right = {"fs": lax.rem(z + 1, n_fs)}
    z_left = {"fs": lax.rem(z + n_fs - 1, n_fs)}
    chips = n_tp // 2
    x, core = t // 2, lax.rem(t, 2)
    xr, xl, xo = lax.rem(x + 1, chips), lax.rem(x + 3, chips), lax.rem(x + 2, chips)
    other = 1 - core
    sib = {"tp": 2 * x + other}
    x_right, x_left = {"tp": 2 * xr + core}, {"tp": 2 * xl + core}

    nq, rows, width = sb0.shape[0], sb0.shape[1], s_in.shape[1]
    half = rows // 2
    feat = width * n_tp
    k_rows, chan_w = value_in.shape
    chan = chan_w * n_tp
    steps = n_fs // 2

    own_k = pl.ds(pl.multiple_of(z * k_rows, k_rows), k_rows)

    def own_loads():
        yield pltpu.make_async_copy(
            wd_in, wd.at[z // 2, :, pl.ds(pl.multiple_of(lax.rem(z, 2) * LANES, LANES), LANES)], load_sem.at[0]
        )
        for i, ref in enumerate((value_in, glu_in, mix_in)):
            yield pltpu.make_async_copy(ref, vm.at[own_k, i * chan_w : (i + 1) * chan_w], load_sem.at[1 + i])
        for q in range(nq):
            yield pltpu.make_async_copy(
                s_in.at[pl.ds(q * rows, rows), :],
                sb0.at[q, :, pl.ds(pl.multiple_of(t * width, width), width)],
                load_sem.at[4 + q],
            )

    for copy in own_loads():
        copy.start()

    hidden = gate_in.shape[0]
    n_full = hidden // LANES
    for n in range(n_full):
        r = slice(n * LANES, (n + 1) * LANES)
        gu[own_k, 2 * n * LANES : (2 * n + 1) * LANES] = gate_in[r, :].T
        gu[own_k, (2 * n + 1) * LANES : (2 * n + 2) * LANES] = up_in[r, :].T
    gu[own_k, 2 * n_full * LANES :] = jnp.concatenate(
        [gate_in[n_full * LANES :, :], up_in[n_full * LANES :, :]], axis=0
    ).T
    for i, ref in enumerate((before_in, mixer_in, after_in)):
        pk[t, i : i + 1, :] = ref[...].astype(F32).reshape(1, width)
    pk[t, 3:4, :chan_w] = cgain_in[...].astype(F32).reshape(1, chan_w)
    pk[t, 3:4, chan_w:] = cbias_in[...].astype(F32).reshape(1, chan_w)
    pk[t, 4:8, :] = jnp.zeros((4, width), F32)

    barrier = pltpu.get_barrier_semaphore()
    peers = [z_right, z_left, partner] + [{"tp": lax.rem(t + i, n_tp)} for i in range(1, n_tp)]
    for peer in peers:
        pl.semaphore_signal(barrier, inc=1, device_id=peer, device_id_type=MESH)
    pl.semaphore_wait(barrier, len(peers))

    for copy in own_loads():
        copy.wait()

    def piece(kind, f, share):
        r0 = pl.multiple_of(f * k_rows, k_rows)
        if kind == 0:
            cols = pl.ds(pl.multiple_of(parity * GU_X, LANES), GU_X) if share == 0 else pl.ds(2 * GU_X, gu.shape[1] - 2 * GU_X)
            return gu.at[pl.ds(r0, k_rows), cols]
        if kind == 1:
            rws = pl.ds(pl.multiple_of(parity * WD_X, 16), WD_X) if share == 0 else pl.ds(2 * WD_X, wd.shape[1] - 2 * WD_X)
            return wd.at[f // 2, rws, pl.ds(pl.multiple_of(lax.rem(f, 2) * LANES, LANES), LANES)]
        cols = pl.ds(pl.multiple_of(parity * VM_X, LANES), VM_X) if share == 0 else pl.ds(2 * VM_X, vm.shape[1] - 2 * VM_X)
        return vm.at[pl.ds(r0, k_rows), cols]

    def many(kind, share, count):
        if kind == 0:
            w = GU_X if share == 0 else gu.shape[1] - 2 * GU_X
            return gu.at[pl.ds(0, count * k_rows), pl.ds(0, w)]
        if kind == 1:
            r = WD_X if share == 0 else wd.shape[1] - 2 * WD_X
            return wd.at[pl.ds(0, count), pl.ds(0, r), pl.ds(0, LANES)]
        w = VM_X if share == 0 else vm.shape[1] - 2 * VM_X
        return vm.at[pl.ds(0, count * k_rows), pl.ds(0, w)]

    def origin(way, s):
        return lax.rem(z + n_fs - s, n_fs) if way == 0 else lax.rem(z + s, n_fs)

    def reach(way, share):
        return steps if way == share else steps - 1

    def z_copy(kind, way, share, s_next):
        ref = piece(kind, origin(way, s_next - 1), share)
        return remote(
            ref,
            ref,
            z_send.at[kind, way, share],
            z_recv.at[kind, way, share, s_next - 1],
            z_right if way == 0 else z_left,
        )

    def z_arrival(kind, way, share, s):
        ref = piece(kind, origin(way, s), share)
        return remote(
            ref, ref, z_send.at[kind, way, share], z_recv.at[kind, way, share, s - 1], z_right if way == 0 else z_left
        )

    def y_copy(kind, way, s):
        ref = piece(kind, origin(way, s), 0)
        return remote(ref, ref, y_send.at[kind, way], y_recv.at[kind, way], partner)

    def spread_mix(f):
        dest, b = f // 2, lax.rem(f, 2)
        src = vm.at[pl.ds(pl.multiple_of(f * k_rows, k_rows), k_rows), pl.ds(2 * chan_w, chan_w)]
        dst = mxb.at[
            pl.ds(pl.multiple_of(t * chan_w, chan_w), chan_w), pl.ds(pl.multiple_of(b * LANES, LANES), LANES)
        ]

        @pl.when(dest != t)
        def _():
            remote(src, dst, mx_send.at[0], mx_recv.at[t, b], {"tp": dest}).start()

        @pl.when(dest == t)
        def _():
            pltpu.make_async_copy(src, dst, mx_recv.at[t, b]).start()

    def relay(kinds, s, last):
        for share in range(2):
            for way in range(2):
                for kind in kinds:
                    far = reach(way, share)
                    if isinstance(s, int) and s > far:
                        continue
                    z_arrival(kind, way, share, s).wait_recv()
                    if not isinstance(s, int) or s < far:
                        z_copy(kind, way, share, s + 1).start()
                    if share == 0:
                        y_copy(kind, way, s).start()
                    if kind == 2 and share == 1:
                        spread_mix(origin(way, s))

    def relay_loop(kinds, lo, hi, extra=None):
        @pl.loop(lo, hi)
        def _(s):
            relay(kinds, s, None)
            if extra is not None:
                extra(s)

    def y_wait(kind):
        for way in range(2):
            ref = many(kind, 0, reach(way, 0))
            remote(ref, ref, y_send.at[kind, way], y_recv.at[kind, way], partner).wait_recv()

    def block(buf, w, q, b, part=None):
        rws = slice(None) if part is None else pl.ds(part * half, half)
        return buf.at[q, rws, pl.ds(pl.multiple_of(b * w, w), w)]

    def ag_copy(n, ref, q, s_i, r_i, where):
        return remote(ref, ref, ag_send.at[n, q, s_i], ag_recv.at[n, q, r_i], where)

    def ag_start(n, buf, w, q):
        own = block(buf, w, q, t)
        ag_copy(n, own, q, 1, 1, x_right).start()
        ag_copy(n, own, q, 2, 2, x_left).start()
        ag_copy(n, own, q, 0, 0, sib).start()

    def ag_relay(n, buf, w, q):
        b_l, b_r = 2 * xl + core, 2 * xr + core
        ag_copy(n, block(buf, w, q, b_l), q, 1, 1, x_right).wait_recv()
        ag_copy(n, block(buf, w, q, b_l, 0), q, 4, 3, x_right).start()
        ag_copy(n, block(buf, w, q, b_l), q, 3, 5, sib).start()
        ag_copy(n, block(buf, w, q, b_r), q, 2, 2, x_left).wait_recv()
        ag_copy(n, block(buf, w, q, b_r, 1), q, 6, 4, x_left).start()
        ag_copy(n, block(buf, w, q, b_r), q, 5, 6, sib).start()

    def ag_opposite(n, buf, w, q):
        b_o = 2 * xo + core
        ag_copy(n, block(buf, w, q, b_o, 0), q, 4, 3, x_right).wait_recv()
        ag_copy(n, block(buf, w, q, b_o, 0), q, 7, 7, sib).start()
        ag_copy(n, block(buf, w, q, b_o, 1), q, 6, 4, x_left).wait_recv()
        ag_copy(n, block(buf, w, q, b_o, 1), q, 8, 8, sib).start()

    def ag_end(n, buf, w, q):
        ag_copy(n, block(buf, w, q, 2 * x + other), q, 0, 0, sib).wait_recv()
        ag_copy(n, block(buf, w, q, 2 * xl + other), q, 3, 5, sib).wait_recv()
        ag_copy(n, block(buf, w, q, 2 * xr + other), q, 5, 6, sib).wait_recv()
        ag_copy(n, block(buf, w, q, 2 * xo + other, 0), q, 7, 7, sib).wait_recv()
        ag_copy(n, block(buf, w, q, 2 * xo + other, 1), q, 8, 8, sib).wait_recv()

    def ag_drain(n, buf, w, q):
        whole, part = block(buf, w, q, t), block(buf, w, q, t, 0)
        for i in range(9):
            ref = part if i in (4, 6, 7, 8) else whole
            ag_copy(n, ref, q, i, 0, sib).wait_send()

    def rs_copy(src, dst, n, q, i, where):
        return remote(src, dst, rs_send.at[n, q, i], rs_recv.at[n, q, i], where)

    order = (xo, xr, xl, x)
    sib_copy = lambda n, q, k: rs_copy(sdo.at[n, q, k], sdi.at[n, q, k], n, q, k, sib)

    def opp_copy(n, q, i):
        ref = pl.ds(i * half, half)
        return rs_copy(obo.at[n, q, ref], obi.at[n, q, ref], n, q, 4 + i, x_right if i == 0 else x_left)

    def nb_copy(n, q, i):
        return rs_copy(nbo.at[n, q, i], nbi.at[n, q, i], n, q, 6 + i, x_right if i == 0 else x_left)

    def rs_partials(n, q, base):
        h = hid[pl.ds(pl.multiple_of(base, 16), rows), :]
        for k in range(4):
            sdo[n, q, k] = jnp.dot(h, wd[2 * order[k] + other], preferred_element_type=F32).astype(BF16)
            sib_copy(n, q, k).start()
            acc[q, k] = jnp.dot(h, wd[2 * order[k] + core], preferred_element_type=F32)

    def rs_opposite(n, q):
        sib_copy(n, q, 0).wait_recv()
        obo[n, q] = (acc[q, 0] + sdi[n, q, 0].astype(F32)).astype(BF16)
        opp_copy(n, q, 0).start()
        opp_copy(n, q, 1).start()

    def rs_neighbours(n, q):
        for i in range(2):
            sib_copy(n, q, 1 + i).wait_recv()
            opp_copy(n, q, i).wait_recv()
            mine, far = pl.ds(i * half, half), pl.ds((1 - i) * half, half)
            nbo[n, q, i, mine] = (
                acc[q, 1 + i, mine] + sdi[n, q, 1 + i, mine].astype(F32) + obi[n, q, mine].astype(F32)
            ).astype(BF16)
            nbo[n, q, i, far] = (acc[q, 1 + i, far] + sdi[n, q, 1 + i, far].astype(F32)).astype(BF16)
            nb_copy(n, q, i).start()

    def rs_total(n, q):
        sib_copy(n, q, 3).wait_recv()
        nb_copy(n, q, 0).wait_recv()
        nb_copy(n, q, 1).wait_recv()
        return (
            acc[q, 3] + sdi[n, q, 3].astype(F32) + nbi[n, q, 0].astype(F32) + nbi[n, q, 1].astype(F32)
        )

    def rs_drain(n, q):
        for k in range(4):
            sib_copy(n, q, k).wait_send()
        for i in range(2):
            opp_copy(n, q, i).wait_send()
            nb_copy(n, q, i).wait_send()

    def norm_rows(buf, q, r, base):
        @pl.loop(0, rows // 16, unroll=4)
        def _(i):
            rws = pl.ds(pl.multiple_of(i * 16, 16), 16)
            v = buf[q, rws, :].astype(F32)
            inverse = lax.rsqrt(jnp.sum(v * v, axis=1, keepdims=True) / feat + EPS)
            ub[pl.ds(pl.multiple_of(base + i * 16, 16), 16), :] = (v * inverse * gf[r : r + 1, :]).astype(BF16)

    def hidden_part(lo, count, first, tiles, tail):
        c0 = first * 2 * LANES
        c1 = gu.shape[1] if tail else (first + tiles) * 2 * LANES
        r = jnp.dot(ub[pl.ds(lo, count), :], gu[:, c0:c1], preferred_element_type=F32)
        for n in range(tiles):
            a, b = r[:, 2 * n * LANES : (2 * n + 1) * LANES], r[:, (2 * n + 1) * LANES : (2 * n + 2) * LANES]
            hid[pl.ds(lo, count), (first + n) * LANES : (first + n + 1) * LANES] = (jax.nn.silu(a) * b).astype(BF16)
        if tail:
            r = r[:, 2 * tiles * LANES :]
            w = r.shape[1]
            hid[pl.ds(lo, count), n_full * LANES :] = (jax.nn.silu(r) * pltpu.roll(r, w // 2, 1))[:, : w // 2].astype(BF16)

    def conv(q):
        b0 = pl.multiple_of(q * rows, 16)
        r = jnp.dot(ub[pl.ds(b0, rows), :], vm[:, : 2 * chan_w], preferred_element_type=F32)
        glued = r[:, :chan_w] * jax.nn.sigmoid(r[:, chan_w:])
        for i in range(rows // LEN):
            pad[i, 32:, :] = glued[i * LEN : (i + 1) * LEN]
        n_taps = taps_in.shape[0]
        taps = taps_in[...].astype(F32)
        for i in range(rows // LEN):
            total = jnp.zeros((LEN, chan_w), F32)
            for k in range(n_taps):
                total = total + taps[k : k + 1, :] * pad[i, 33 - n_taps + k : 33 - n_taps + k + LEN, :]
            cvb[q, i * LEN : (i + 1) * LEN, pl.ds(pl.multiple_of(t * chan_w, chan_w), chan_w)] = total.astype(BF16)

    def channel_norm(q):
        @pl.loop(0, rows // 16, unroll=4)
        def _(i):
            rws = pl.ds(pl.multiple_of(i * 16, 16), 16)
            v = cvb[q, rws, :].astype(F32)
            mu = jnp.sum(v, axis=1, keepdims=True) / chan
            msq = jnp.sum(v * v, axis=1, keepdims=True) / chan
            w = (v - mu) * lax.rsqrt(msq - mu * mu + EPS) * cgb[3:4, :] + cgb[11:12, :]
            mixed[rws, :] = jax.nn.silu(w).astype(BF16)

    def own_cols(buf, q):
        return buf[q, :, pl.ds(pl.multiple_of(t * width, width), width)]

    def each(fn):
        pl.loop(0, nq)(fn)

    def z_begin(kinds):
        for kind in kinds:
            for share in range(2):
                for way in range(2):
                    z_copy(kind, way, share, 1).start()

    z_begin((0,))
    each(lambda q: ag_start(0, sb0, width, q))

    def pk_copy(i):
        return remote(pk.at[t], pk.at[t], pk_send.at[i - 1], pk_recv.at[t], {"tp": lax.rem(t + i, n_tp)})

    for i in range(1, n_tp):
        pk_copy(i).start()
    z_begin((1, 2))
    spread_mix(z)

    pad[:, :32, :] = jnp.zeros((pad.shape[0], 32, chan_w), F32)

    relay((0,), 1, None)
    each(lambda q: ag_relay(0, sb0, width, q))
    relay((0,), 2, None)
    each(lambda q: ag_opposite(0, sb0, width, q))
    for i in range(1, n_tp):
        b = lax.rem(t + i, n_tp)
        remote(pk.at[b], pk.at[b], pk_send.at[i - 1], pk_recv.at[b], {"tp": b}).wait_recv()
    for b in range(n_tp):
        gf[:, b * width : (b + 1) * width] = pk[b]
        cgb[0:8, b * chan_w : (b + 1) * chan_w] = pk[b][:, :chan_w]
        cgb[8:16, b * chan_w : (b + 1) * chan_w] = pk[b][:, chan_w : 2 * chan_w]
    relay((0,), 3, None)
    each(lambda q: ag_end(0, sb0, width, q))

    def early_norm(s):
        q = s - 4

        @pl.when(q < nq)
        def _():
            norm_rows(sb0, q, 0, q * rows)

    relay_loop((0,), 4, steps - 1, early_norm)
    for s in (steps - 1, steps):
        relay((0,), s, None)

    relay_loop((1, 2), 1, 4)
    y_wait(0)

    tokens = nq * rows

    for s, (a, b, tail) in zip((4, 5, 6), ((0, 2, False), (2, 2, False), (4, n_full - 4, True))):
        relay((1, 2), s, None)
        hidden_part(0, tokens, a, b, tail)
    for s in (steps - 1, steps):
        relay((1, 2), s, None)
    y_wait(1)

    each(lambda q: rs_partials(0, q, q * rows))
    each(lambda q: rs_opposite(0, q))
    each(lambda q: rs_neighbours(0, q))

    def first(q):
        total = rs_total(0, q)
        sb1[q, :, pl.ds(pl.multiple_of(t * width, width), width)] = (
            own_cols(sb0, q).astype(F32) + 0.5 * total
        ).astype(BF16)
        ag_start(1, sb1, width, q)

    each(first)
    each(lambda q: ag_relay(1, sb1, width, q))
    y_wait(2)
    each(lambda q: ag_opposite(1, sb1, width, q))

    def conv_stage(q):
        ag_end(1, sb1, width, q)
        norm_rows(sb1, q, 1, q * rows)
        conv(q)
        ag_start(2, cvb, chan_w, q)

    each(conv_stage)
    each(lambda q: ag_relay(2, cvb, chan_w, q))
    each(lambda q: ag_opposite(2, cvb, chan_w, q))

    for b in range(n_tp):
        for i in range(2):
            ref = mxb.at[pl.ds(b * chan_w, chan_w), pl.ds(i * LANES, LANES)]
            pltpu.make_async_copy(ref, ref, mx_recv.at[b, i]).wait()

    def mix_stage(q):
        ag_end(2, cvb, chan_w, q)
        channel_norm(q)
        branch = jnp.dot(mixed[...], mxb[...], preferred_element_type=F32)
        sb3[q, :, pl.ds(pl.multiple_of(t * width, width), width)] = (
            own_cols(sb1, q).astype(F32) + branch
        ).astype(BF16)
        ag_start(3, sb3, width, q)

    each(mix_stage)
    each(lambda q: ag_relay(3, sb3, width, q))
    each(lambda q: ag_opposite(3, sb3, width, q))

    def ffn_stage(q):
        base = pl.multiple_of(q * rows, 16)
        ag_end(3, sb3, width, q)
        norm_rows(sb3, q, 2, base)

        hidden_part(base, rows, 0, n_full, True)
        rs_partials(1, q, base)

    each(ffn_stage)
    each(lambda q: rs_opposite(1, q))
    each(lambda q: rs_neighbours(1, q))

    def last(q):
        total = rs_total(1, q)
        out[pl.ds(pl.multiple_of(q * rows, 16), rows), :] = (
            own_cols(sb3, q).astype(F32) + 0.5 * total
        ).astype(BF16)

    each(last)

    for kind in range(3):
        for way in range(2):
            for share in range(2):
                ref = many(kind, share, reach(way, share))
                remote(ref, ref, z_send.at[kind, way, share], z_recv.at[kind, way, share, 0], z_right).wait_send()
            ref = many(kind, 0, reach(way, 0))
            remote(ref, ref, y_send.at[kind, way], y_recv.at[kind, way], partner).wait_send()
    for i in range(1, n_tp):
        pk_copy(i).wait_send()
    ref = mxb.at[pl.ds(0, (n_tp - 1) * chan_w), :]
    remote(ref, ref, mx_send.at[0], mx_recv.at[0, 0], sib).wait_send()

    def drain(q):
        for n, buf, w in ((0, sb0, width), (1, sb1, width), (2, cvb, chan_w), (3, sb3, width)):
            ag_drain(n, buf, w, q)
        for n in range(2):
            rs_drain(n, q)

    each(drain)


def solution(mesh):
    n_fs, n_tp = mesh.shape["fs"], mesh.shape["tp"]

    def local(
        stream_in,
        gain_before,
        gain_mixer,
        gain_after,
        w_gate,
        w_upward,
        w_down,
        w_value,
        w_glu_gate,
        conv_taps,
        chan_gain,
        chan_bias,
        w_mix_out,
    ):
        tokens, width = stream_in.shape
        k_rows, hidden = w_gate.shape
        chan_w = w_value.shape[1]
        nq = CHUNKS
        rows = tokens // nq
        feat, chan = width * n_tp, chan_w * n_tp
        vmem = pltpu.VMEM
        dma = pltpu.SemaphoreType.DMA
        any_space = pl.BlockSpec(memory_space=pl.ANY)
        in_vmem = pl.BlockSpec(memory_space=pltpu.VMEM)
        return pl.pallas_call(
            lambda *refs: layer_kernel(n_fs, n_tp, *refs),
            out_shape=jax.ShapeDtypeStruct((tokens, width), BF16),
            in_specs=[any_space, in_vmem, in_vmem] + [any_space] * 4 + [in_vmem] * 6,
            out_specs=in_vmem,
            scratch_shapes=[
                vmem((n_fs * k_rows, 2 * hidden), BF16),
                vmem((n_fs // 2, hidden, 2 * LANES), BF16),
                vmem((n_fs * k_rows, 3 * chan_w), BF16),
                vmem((chan, 2 * LANES), BF16),
                vmem((n_tp, 8, width), F32),
                vmem((8, feat), F32),
                vmem((16, chan), F32),
                vmem((nq, rows, feat), BF16),
                vmem((nq, rows, feat), BF16),
                vmem((nq, rows, feat), BF16),
                vmem((nq, rows, chan), BF16),
                vmem((tokens, feat), BF16),
                vmem((rows, chan), BF16),
                vmem((tokens, hidden), BF16),
                vmem((rows // LEN, LEN + 32, chan_w), F32),
                vmem((2, nq, 4, rows, width), BF16),
                vmem((2, nq, 4, rows, width), BF16),
                vmem((nq, 4, rows, width), F32),
                vmem((2, nq, rows, width), BF16),
                vmem((2, nq, rows, width), BF16),
                vmem((2, nq, 2, rows, width), BF16),
                vmem((2, nq, 2, rows, width), BF16),
                dma((4 + nq,)),
                dma((3, 2, 2, n_fs // 2)),
                dma((3, 2, 2)),
                dma((3, 2)),
                dma((3, 2)),
                dma((n_tp,)),
                dma((n_tp - 1,)),
                dma((n_tp, 2)),
                dma((1,)),
                dma((4, nq, 9)),
                dma((4, nq, 9)),
                dma((2, nq, 8)),
                dma((2, nq, 8)),
            ],
            compiler_params=pltpu.CompilerParams(
                collective_id=0, has_side_effects=True, vmem_limit_bytes=60 * 1024 * 1024
            ),
        )(
            stream_in,
            w_gate.T,
            w_upward.T,
            w_down,
            w_value,
            w_glu_gate,
            w_mix_out,
            conv_taps,
            gain_before,
            gain_mixer,
            gain_after,
            chan_gain,
            chan_bias,
        )

    in_specs = (
        P(("grp", "fs"), "tp"),
        P("tp"),
        P("tp"),
        P("tp"),
        P("fs", "tp"),
        P("fs", "tp"),
        P("tp", "fs"),
        P("fs", "tp"),
        P("fs", "tp"),
        P(None, "tp"),
        P("tp"),
        P("tp"),
        P("tp", "fs"),
    )
    out_specs = P(("grp", "fs"), "tp")
    return jax.shard_map(local, mesh=mesh, in_specs=in_specs, out_specs=out_specs, check_vma=False)
```

```python
import jax
import jax.numpy as jnp
from jax import lax
from jax.experimental import pallas as pl
from jax.experimental.pallas import tpu as pltpu
from jax.sharding import PartitionSpec as P

MESH = pl.DeviceIdType.MESH
LEN = 128
EPS = 1e-06
LANES = 128
CHUNKS = 3
BF16, F32 = jnp.bfloat16, jnp.float32


def remote(src, dst, send_sem, recv_sem, where):
    return pltpu.make_async_remote_copy(
        src_ref=src,
        dst_ref=dst,
        send_sem=send_sem,
        recv_sem=recv_sem,
        device_id=where,
        device_id_type=MESH,
    )


def layer_kernel(
    n_fs,
    n_tp,
    s_in,
    gate_in,
    up_in,
    wd_in,
    value_in,
    glu_in,
    mix_in,
    taps_in,
    before_in,
    mixer_in,
    after_in,
    cgain_in,
    cbias_in,
    out,
    gu,
    wd,
    vm,
    mxb,
    pk,
    gf,
    cgb,
    sb0,
    sb1,
    sb3,
    cvb,
    ub,
    mixed,
    hid,
    pad,
    ybo,
    ybi,
    acc,
    rs0,
    rs1,
    load_sem,
    z_recv,
    z_send,
    y_recv,
    y_send,
    pk_recv,
    pk_send,
    mx_recv,
    mx_send,
    ag_recv,
    ag_send,
    rs_recv,
    rs_send,
    yx_recv,
    yx_send,
):
    z, t, g = lax.axis_index("fs"), lax.axis_index("tp"), lax.axis_index("grp")
    parity = lax.rem(g, 2)
    partner = {"grp": g + 1 - 2 * parity}
    z_right = {"fs": lax.rem(z + 1, n_fs)}
    z_left = {"fs": lax.rem(z + n_fs - 1, n_fs)}
    chips = n_tp // 2
    x, core = t // 2, lax.rem(t, 2)
    xr, xl, xo = lax.rem(x + 1, chips), lax.rem(x + 3, chips), lax.rem(x + 2, chips)
    other = 1 - core
    sib = {"tp": 2 * x + other}
    x_right, x_left = {"tp": 2 * xr + core}, {"tp": 2 * xl + core}

    nq, rows, width = sb1.shape[0], sb1.shape[1], s_in.shape[1]
    half = rows // 2
    feat = width * n_tp
    k_rows, chan_w = value_in.shape
    chan = chan_w * n_tp
    steps = n_fs // 2
    own_units = gate_in.shape[0] // 2
    units = wd.shape[1] // 2
    pairs = units // LANES
    mine, theirs = parity, 1 - parity

    own_k = pl.ds(pl.multiple_of(z * k_rows, k_rows), k_rows)

    own_w = pl.ds(pl.multiple_of(t * width, width), width)

    def own_loads():
        for h in range(2):
            yield pltpu.make_async_copy(
                wd_in.at[h * own_units : (h + 1) * own_units, :],
                wd.at[
                    z // 2,
                    h * units : h * units + own_units,
                    pl.ds(pl.multiple_of(lax.rem(z, 2) * LANES, LANES), LANES),
                ],
                load_sem.at[h],
            )
        for i, ref in enumerate((value_in, glu_in, mix_in)):
            yield pltpu.make_async_copy(ref, vm.at[own_k, i * chan_w : (i + 1) * chan_w], load_sem.at[2 + i])
        for q in range(nq):
            yield pltpu.make_async_copy(
                s_in.at[pl.ds(q * rows, rows), :],
                sb0.at[nq + q, :, pl.ds(pl.multiple_of(t * width, width), width)],
                load_sem.at[5 + q],
            )

    for copy in own_loads():
        copy.start()

    for h in range(2):
        for i in range(pairs):
            lo = h * own_units + i * LANES
            hi = min(lo + LANES, (h + 1) * own_units)
            for j, ref in enumerate((gate_in, up_in)):
                v = ref[lo:hi, :]
                if hi - lo < LANES:
                    v = jnp.concatenate([v, jnp.zeros((LANES - hi + lo, k_rows), BF16)], axis=0)
                c = h * 2 * units + (2 * i + j) * LANES
                gu[own_k, c : c + LANES] = v.T
        wd[:, h * units + own_units : (h + 1) * units, :] = jnp.zeros((wd.shape[0], units - own_units, wd.shape[2]), BF16)
    for i, ref in enumerate((before_in, mixer_in, after_in)):
        pk[t, i : i + 1, :] = ref[...].astype(F32).reshape(1, width)
    pk[t, 3:4, :chan_w] = cgain_in[...].astype(F32).reshape(1, chan_w)
    pk[t, 3:4, chan_w:] = cbias_in[...].astype(F32).reshape(1, chan_w)
    pk[t, 4:8, :] = jnp.zeros((4, width), F32)

    barrier = pltpu.get_barrier_semaphore()
    peers = [z_right, z_left, partner] + [{"tp": lax.rem(t + i, n_tp)} for i in range(1, n_tp)]
    for peer in peers:
        pl.semaphore_signal(barrier, inc=1, device_id=peer, device_id_type=MESH)
    pl.semaphore_wait(barrier, len(peers))

    for copy in own_loads():
        copy.wait()

    wide = 2 * LANES * (pairs - 1)
    third = own_units // 2

    def piece(kind, f, share):
        r0 = pl.ds(pl.multiple_of(f * k_rows, k_rows), k_rows)
        if kind == 0:
            c0 = mine * 2 * units
            if share == 0:
                return gu.at[r0, pl.ds(pl.multiple_of(c0, LANES), wide)]
            return gu.at[r0, pl.ds(pl.multiple_of(c0 + wide, LANES), 2 * units - wide)]
        if kind == 2:
            return vm.at[r0, 0 : 2 * chan_w] if share == 0 else vm.at[r0, 2 * chan_w : 3 * chan_w]
        q0 = (mine if kind == 1 else theirs) * units + share * third
        return wd.at[
            f // 2,
            pl.ds(pl.multiple_of(q0, 16), third),
            pl.ds(pl.multiple_of(lax.rem(f, 2) * LANES, LANES), LANES),
        ]

    def many(kind, share, count):
        if kind == 0:
            return gu.at[0 : count * k_rows, 0 : (wide if share == 0 else 2 * units - wide)]
        if kind == 2:
            return vm.at[0 : count * k_rows, 0 : (2 * chan_w if share == 0 else chan_w)]
        return wd.at[0:count, 0:third, 0:LANES]

    def origin(way, s):
        return lax.rem(z + n_fs - s, n_fs) if way == 0 else lax.rem(z + s, n_fs)

    def reach(way, share):
        return steps if way == share else steps - 1

    def z_copy(kind, way, share, s_next):
        ref = piece(kind, origin(way, s_next - 1), share)
        return remote(
            ref,
            ref,
            z_send.at[kind, way, share],
            z_recv.at[kind, way, share, s_next - 1],
            z_right if way == 0 else z_left,
        )

    def z_arrival(kind, way, share, s):
        ref = piece(kind, origin(way, s), share)
        return remote(
            ref, ref, z_send.at[kind, way, share], z_recv.at[kind, way, share, s - 1], z_right if way == 0 else z_left
        )

    def y_copy(way, s):
        ref = piece(0, origin(way, s), 0)
        return remote(ref, ref, y_send.at[way], y_recv.at[way], partner)

    def y_late(f):
        ref = piece(0, f, 1)
        return remote(ref, ref, y_send.at[2], y_recv.at[2], partner)

    def y_all(i):
        ref = many(0, 0, reach(i, 0)) if i < 2 else many(0, 1, n_fs - 1)
        return remote(ref, ref, y_send.at[i], y_recv.at[i], partner)

    def stream_copy(q):
        return remote(
            sb0.at[nq + q, :, own_w], sb0.at[q, :, own_w], yx_send.at[0, q], yx_recv.at[0, q], partner
        )

    def part_copy(q):
        return remote(ybo.at[q], ybi.at[q], yx_send.at[1, q], yx_recv.at[1, q], partner)

    def spread_mix(f):
        dest, b = f // 2, lax.rem(f, 2)
        src = vm.at[pl.ds(pl.multiple_of(f * k_rows, k_rows), k_rows), pl.ds(2 * chan_w, chan_w)]
        dst = mxb.at[
            pl.ds(pl.multiple_of(t * chan_w, chan_w), chan_w), pl.ds(pl.multiple_of(b * LANES, LANES), LANES)
        ]

        @pl.when(dest != t)
        def _():
            remote(src, dst, mx_send.at[0], mx_recv.at[t, b], {"tp": dest}).start()

        @pl.when(dest == t)
        def _():
            pltpu.make_async_copy(src, dst, mx_recv.at[t, b]).start()

    def relay(kinds, s, last):
        for share in range(2):
            for way in range(2):
                for kind in kinds:
                    far = reach(way, share)
                    if isinstance(s, int) and s > far:
                        continue
                    z_arrival(kind, way, share, s).wait_recv()
                    if not isinstance(s, int) or s < far:
                        z_copy(kind, way, share, s + 1).start()
                    if kind == 0 and share == 0:
                        y_copy(way, s).start()
                    if kind == 2 and share == 1:
                        spread_mix(origin(way, s))

    def block(buf, w, q, b, part=None):
        rws = slice(None) if part is None else pl.ds(part * half, half)
        return buf.at[q, rws, pl.ds(pl.multiple_of(b * w, w), w)]

    def ag_copy(n, ref, q, s_i, r_i, where):
        return remote(ref, ref, ag_send.at[n, q, s_i], ag_recv.at[n, q, r_i], where)

    def ag_start(n, buf, w, q):
        own = block(buf, w, q, t)
        ag_copy(n, own, q, 1, 1, x_right).start()
        ag_copy(n, own, q, 2, 2, x_left).start()
        ag_copy(n, own, q, 0, 0, sib).start()

    def ag_relay(n, buf, w, q):
        b_l, b_r = 2 * xl + core, 2 * xr + core
        ag_copy(n, block(buf, w, q, b_l), q, 1, 1, x_right).wait_recv()
        ag_copy(n, block(buf, w, q, b_l, 0), q, 4, 3, x_right).start()
        ag_copy(n, block(buf, w, q, b_l), q, 3, 5, sib).start()
        ag_copy(n, block(buf, w, q, b_r), q, 2, 2, x_left).wait_recv()
        ag_copy(n, block(buf, w, q, b_r, 1), q, 6, 4, x_left).start()
        ag_copy(n, block(buf, w, q, b_r), q, 5, 6, sib).start()

    def ag_opposite(n, buf, w, q):
        b_o = 2 * xo + core
        ag_copy(n, block(buf, w, q, b_o, 0), q, 4, 3, x_right).wait_recv()
        ag_copy(n, block(buf, w, q, b_o, 0), q, 7, 7, sib).start()
        ag_copy(n, block(buf, w, q, b_o, 1), q, 6, 4, x_left).wait_recv()
        ag_copy(n, block(buf, w, q, b_o, 1), q, 8, 8, sib).start()

    def ag_end(n, buf, w, q):
        ag_copy(n, block(buf, w, q, 2 * x + other), q, 0, 0, sib).wait_recv()
        ag_copy(n, block(buf, w, q, 2 * xl + other), q, 3, 5, sib).wait_recv()
        ag_copy(n, block(buf, w, q, 2 * xr + other), q, 5, 6, sib).wait_recv()
        ag_copy(n, block(buf, w, q, 2 * xo + other, 0), q, 7, 7, sib).wait_recv()
        ag_copy(n, block(buf, w, q, 2 * xo + other, 1), q, 8, 8, sib).wait_recv()

    def ag_drain(n, buf, w, q):
        whole, part = block(buf, w, q, t), block(buf, w, q, t, 0)
        for i in range(9):
            ref = part if i in (4, 6, 7, 8) else whole
            ag_copy(n, ref, q, i, 0, sib).wait_send()

    order = (xo, xr, xl, x)
    rs_refs = (rs0, rs1)

    def rs_copy(src, dst, n, q, i, where):
        return remote(rs_refs[n].at[q, src], rs_refs[n].at[q, dst], rs_send.at[n, q, i], rs_recv.at[n, q, i], where)

    def sib_copy(n, q):
        return rs_copy(slice(0, 4), slice(4, 8), n, q, 0, sib)

    def opp_copy(n, q, i):
        part = pl.ds(i * half, half)
        return remote(
            rs_refs[n].at[q, 8, part],
            rs_refs[n].at[q, 9, part],
            rs_send.at[n, q, 1 + i],
            rs_recv.at[n, q, 1 + i],
            x_right if i == 0 else x_left,
        )

    def nb_copy(n, q, i):
        return rs_copy(10 + i, 12 + i, n, q, 3 + i, x_right if i == 0 else x_left)

    def rs_partials(n, q):
        buf = rs_refs[n]
        width_k = units if n == 0 else 2 * units
        k_range = pl.ds(pl.multiple_of(mine * units, LANES), units) if n == 0 else slice(None)
        h = hid[q * rows : (q + 1) * rows, 0:width_k]
        for k in range(4):
            buf[q, k] = jnp.dot(h, wd[2 * order[k] + other, k_range, :], preferred_element_type=F32).astype(BF16)
        sib_copy(n, q).start()
        for k in range(4):
            acc[q, k] = jnp.dot(h, wd[2 * order[k] + core, k_range, :], preferred_element_type=F32)

    def rs_opposite(n, q):
        buf = rs_refs[n]
        sib_copy(n, q).wait_recv()
        buf[q, 8] = (acc[q, 0] + buf[q, 4].astype(F32)).astype(BF16)
        opp_copy(n, q, 0).start()
        opp_copy(n, q, 1).start()

    def rs_neighbours(n, q):
        buf = rs_refs[n]
        for i in range(2):
            opp_copy(n, q, i).wait_recv()
            near, far = pl.ds(i * half, half), pl.ds((1 - i) * half, half)
            buf[q, 10 + i, near] = (
                acc[q, 1 + i, near] + buf[q, 5 + i, near].astype(F32) + buf[q, 9, near].astype(F32)
            ).astype(BF16)
            buf[q, 10 + i, far] = (acc[q, 1 + i, far] + buf[q, 5 + i, far].astype(F32)).astype(BF16)
            nb_copy(n, q, i).start()

    def rs_total(n, q):
        buf = rs_refs[n]
        nb_copy(n, q, 0).wait_recv()
        nb_copy(n, q, 1).wait_recv()
        return acc[q, 3] + buf[q, 7].astype(F32) + buf[q, 12].astype(F32) + buf[q, 13].astype(F32)

    def rs_drain(n, q):
        sib_copy(n, q).wait_send()
        for i in range(2):
            opp_copy(n, q, i).wait_send()
            nb_copy(n, q, i).wait_send()

    def norm_rows(buf, q, r, base):
        @pl.loop(0, rows // 16, unroll=4)
        def _(i):
            rws = pl.ds(pl.multiple_of(i * 16, 16), 16)
            v = buf[q, rws, :].astype(F32)
            inverse = lax.rsqrt(jnp.sum(v * v, axis=1, keepdims=True) / feat + EPS)
            ub[pl.ds(pl.multiple_of(base + i * 16, 16), 16), :] = (v * inverse * gf[r : r + 1, :]).astype(BF16)

    def hidden_rows(lo, count, columns, n_pairs):
        r = jnp.dot(ub[lo : lo + count, :], gu[:, columns], preferred_element_type=F32)
        for n in range(n_pairs):
            a, b = r[:, 2 * n * LANES : (2 * n + 1) * LANES], r[:, (2 * n + 1) * LANES : (2 * n + 2) * LANES]
            hid[lo : lo + count, n * LANES : (n + 1) * LANES] = (jax.nn.silu(a) * b).astype(BF16)

    def conv(q):
        r = jnp.dot(ub[q * rows : (q + 1) * rows, :], vm[:, : 2 * chan_w], preferred_element_type=F32)
        glued = r[:, :chan_w] * jax.nn.sigmoid(r[:, chan_w:])
        for i in range(rows // LEN):
            pad[i, 32:, :] = glued[i * LEN : (i + 1) * LEN]
        n_taps = taps_in.shape[0]
        taps = taps_in[...].astype(F32)
        for i in range(rows // LEN):
            total = jnp.zeros((LEN, chan_w), F32)
            for k in range(n_taps):
                total = total + taps[k : k + 1, :] * pad[i, 33 - n_taps + k : 33 - n_taps + k + LEN, :]
            cvb[q, i * LEN : (i + 1) * LEN, pl.ds(pl.multiple_of(t * chan_w, chan_w), chan_w)] = total.astype(BF16)

    def channel_norm(q):
        @pl.loop(0, rows // 16, unroll=4)
        def _(i):
            rws = pl.ds(pl.multiple_of(i * 16, 16), 16)
            v = cvb[q, rws, :].astype(F32)
            mu = jnp.sum(v, axis=1, keepdims=True) / chan
            msq = jnp.sum(v * v, axis=1, keepdims=True) / chan
            w = (v - mu) * lax.rsqrt(msq - mu * mu + EPS) * cgb[3:4, :] + cgb[11:12, :]
            mixed[rws, :] = jax.nn.silu(w).astype(BF16)

    def own_cols(buf, q):
        return buf[q, :, own_w]

    def z_begin(kinds):
        for share in range(2):
            for way in range(2):
                for kind in kinds:
                    z_copy(kind, way, share, 1).start()

    def phase(name):
        return jax.named_scope(name)

    chunks = range(nq)
    z_begin((0, 1))
    for q in chunks:
        stream_copy(q).start()
    pl.loop(nq, 2 * nq)(lambda q: ag_start(0, sb0, width, q))

    def pk_copy(i):
        return remote(pk.at[t], pk.at[t], pk_send.at[i - 1], pk_recv.at[t], {"tp": lax.rem(t + i, n_tp)})

    for i in range(1, n_tp):
        pk_copy(i).start()
    spread_mix(z)
    pad[:, :32, :] = jnp.zeros((pad.shape[0], 32, chan_w), F32)

    def theirs_first(fn):
        pl.loop(0, nq)(fn)

    def ours(fn):
        pl.loop(nq, 2 * nq)(fn)

    with phase("w1"):
        relay((0, 1), 1, None)
    with phase("ag0"):
        for q in chunks:
            stream_copy(q).wait_recv()
        theirs_first(lambda q: ag_start(0, sb0, width, q))
        ours(lambda q: ag_relay(0, sb0, width, q))
    with phase("w2"):
        relay((0, 1), 2, None)
    theirs_first(lambda q: ag_relay(0, sb0, width, q))
    ours(lambda q: ag_opposite(0, sb0, width, q))
    with phase("w3"):
        relay((0, 1), 3, None)
    theirs_first(lambda q: ag_opposite(0, sb0, width, q))
    ours(lambda q: ag_end(0, sb0, width, q))
    for i in range(1, n_tp):
        b = lax.rem(t + i, n_tp)
        remote(pk.at[b], pk.at[b], pk_send.at[i - 1], pk_recv.at[b], {"tp": b}).wait_recv()
    for b in range(n_tp):
        gf[:, b * width : (b + 1) * width] = pk[b]
        cgb[0:8, b * chan_w : (b + 1) * chan_w] = pk[b][:, :chan_w]
        cgb[8:16, b * chan_w : (b + 1) * chan_w] = pk[b][:, chan_w : 2 * chan_w]
    with phase("w4"):
        relay((0, 1), 4, None)
    theirs_first(lambda q: ag_end(0, sb0, width, q))
    ours(lambda q: norm_rows(sb0, q, 0, q * rows))
    with phase("w5"):
        relay((0, 1), 5, None)
    theirs_first(lambda q: norm_rows(sb0, q, 0, q * rows))
    with phase("w67"):
        relay((0, 1), 6, None)
        relay((0, 1), 7, None)
    z_begin((2,))
    with phase("w8"):
        relay((0, 1), 8, None)

    late = [((2,), 1), ((2,), 2), ((2,), 3), ((2,), 4), ((2,), 5), ((2,), 6), ((2, 3), 7), ((2, 3), 8)]
    late += [((3,), i) for i in range(3, steps + 1)]

    def background(count=1):
        for _ in range(count):
            kinds, i = late.pop(0)
            with phase(f"late{i}"):
                for kind in kinds:
                    relay((kind,), i - 6 if (kind == 3 and len(kinds) == 2) else i, None)
            if kinds == (2,) and i == 6:
                z_begin((3,))

    tokens = nq * rows
    my_half = pl.ds(pl.multiple_of(mine * 2 * units, LANES), 2 * units)
    with phase("hid_theirs"):
        hidden_rows(0, tokens, my_half, pairs)
    with phase("part_theirs"):
        for q in chunks:
            rs_partials(0, q)
    background()
    with phase("hid_ours"):
        hidden_rows(tokens, tokens, my_half, pairs)
    with phase("rs_a"):
        rs_opposite(0, 0)
        rs_opposite(0, 1)
        rs_partials(0, nq)
        rs_opposite(0, 2)
        rs_neighbours(0, 0)
        rs_partials(0, nq + 1)
    background()

    def pass_over(q):
        ybo[q] = rs_total(0, q).astype(BF16)
        part_copy(q).start()

    with phase("rs_b"):
        rs_neighbours(0, 1)
        rs_partials(0, nq + 2)
        rs_neighbours(0, 2)
        rs_opposite(0, 3)
    background()
    with phase("rs_c"):
        pass_over(0)
        rs_opposite(0, 4)
        pass_over(1)
        rs_neighbours(0, 3)
        rs_opposite(0, 5)
        pass_over(2)
        pl.loop(1, n_fs)(lambda i: y_late(lax.rem(z + i, n_fs)).start())
    background()
    with phase("rs_d"):
        rs_neighbours(0, 4)
        rs_neighbours(0, 5)

    def first(q):
        total = rs_total(0, nq + q)
        part_copy(q).wait_recv()
        sb1[q, :, own_w] = (own_cols(sb0, nq + q).astype(F32) + 0.5 * (total + ybi[q].astype(F32))).astype(BF16)
        ag_start(1, sb1, width, q)

    with phase("first0"):
        first(0)
    background()
    with phase("first12"):
        first(1)
        first(2)
    background()
    with phase("ag1"):
        ag_relay(1, sb1, width, 0)
        ag_relay(1, sb1, width, 1)
        ag_relay(1, sb1, width, 2)
    background()
    with phase("opp1"):
        ag_opposite(1, sb1, width, 0)
        ag_opposite(1, sb1, width, 1)
    background()

    def conv_stage(q):
        ag_end(1, sb1, width, q)
        norm_rows(sb1, q, 1, q * rows)
        conv(q)
        ag_start(2, cvb, chan_w, q)

    with phase("conv0"):
        conv_stage(0)
    background()
    with phase("conv1"):
        ag_opposite(1, sb1, width, 2)
        conv_stage(1)
    background()
    with phase("conv2"):
        ag_relay(2, cvb, chan_w, 0)
        conv_stage(2)
    background()
    with phase("ag2"):
        ag_relay(2, cvb, chan_w, 1)
        ag_opposite(2, cvb, chan_w, 0)
        ag_relay(2, cvb, chan_w, 2)
        ag_opposite(2, cvb, chan_w, 1)

        @pl.loop(0, n_tp)
        def _(b):
            for i in range(2):
                ref = mxb.at[pl.ds(pl.multiple_of(b * chan_w, chan_w), chan_w), pl.ds(i * LANES, LANES)]
                pltpu.make_async_copy(ref, ref, mx_recv.at[b, i]).wait()

    def mix_stage(q):
        ag_end(2, cvb, chan_w, q)
        channel_norm(q)
        branch = jnp.dot(mixed[...], mxb[...], preferred_element_type=F32)
        sb3[q, :, own_w] = (own_cols(sb1, q).astype(F32) + branch).astype(BF16)
        ag_start(3, sb3, width, q)

    with phase("mix0"):
        mix_stage(0)
    background()
    with phase("mix12"):
        ag_opposite(2, cvb, chan_w, 2)
        mix_stage(1)
        ag_relay(3, sb3, width, 0)
        mix_stage(2)
    background()
    with phase("ag3"):
        ag_relay(3, sb3, width, 1)
        ag_opposite(3, sb3, width, 0)
        ag_relay(3, sb3, width, 2)
        ag_opposite(3, sb3, width, 1)
    background()
    assert not late
    with phase("ywait"):
        for i in range(3):
            y_all(i).wait_recv()

    def ffn_stage(q):
        ag_end(3, sb3, width, q)
        norm_rows(sb3, q, 2, q * rows)
        hidden_rows(q * rows, rows, slice(None), 2 * pairs)
        rs_partials(1, q)

    def last(q):
        total = rs_total(1, q)
        out[q * rows : (q + 1) * rows, :] = (own_cols(sb3, q).astype(F32) + 0.5 * total).astype(BF16)

    with phase("ffn0"):
        ffn_stage(0)
    with phase("ffn1"):
        ag_opposite(3, sb3, width, 2)
        ffn_stage(1)
    with phase("ffn2"):
        rs_opposite(1, 0)
        ffn_stage(2)
    with phase("rs1"):
        rs_opposite(1, 1)
        rs_neighbours(1, 0)
        rs_opposite(1, 2)
        rs_neighbours(1, 1)
    with phase("last"):
        last(0)
        rs_neighbours(1, 2)
        last(1)
        last(2)

    for kind in range(4):
        for way in range(2):
            for share in range(2):
                ref = many(kind, share, reach(way, share))
                remote(ref, ref, z_send.at[kind, way, share], z_recv.at[kind, way, share, 0], z_right).wait_send()
    for i in range(3):
        y_all(i).wait_send()
    for i in range(1, n_tp):
        pk_copy(i).wait_send()
    ref = mxb.at[pl.ds(0, (n_tp - 1) * chan_w), :]
    remote(ref, ref, mx_send.at[0], mx_recv.at[0, 0], sib).wait_send()

    @pl.loop(0, nq)
    def _(q):
        stream_copy(q).wait_send()
        part_copy(q).wait_send()
        for n, buf, w in ((0, sb0, width), (1, sb1, width), (2, cvb, chan_w), (3, sb3, width)):
            ag_drain(n, buf, w, q)
        ag_drain(0, sb0, width, nq + q)
        rs_drain(0, q)
        rs_drain(0, nq + q)
        rs_drain(1, q)


def solution(mesh):
    n_fs, n_tp = mesh.shape["fs"], mesh.shape["tp"]

    def local(
        stream_in,
        gain_before,
        gain_mixer,
        gain_after,
        w_gate,
        w_upward,
        w_down,
        w_value,
        w_glu_gate,
        conv_taps,
        chan_gain,
        chan_bias,
        w_mix_out,
    ):
        tokens, width = stream_in.shape
        k_rows, hidden = w_gate.shape
        chan_w = w_value.shape[1]
        units = -(-(hidden // 2) // LANES) * LANES
        nq = CHUNKS
        rows = tokens // nq
        feat, chan = width * n_tp, chan_w * n_tp
        vmem = pltpu.VMEM
        dma = pltpu.SemaphoreType.DMA
        any_space = pl.BlockSpec(memory_space=pl.ANY)
        in_vmem = pl.BlockSpec(memory_space=pltpu.VMEM)
        return pl.pallas_call(
            lambda *refs: layer_kernel(n_fs, n_tp, *refs),
            out_shape=jax.ShapeDtypeStruct((tokens, width), BF16),
            in_specs=[any_space, in_vmem, in_vmem] + [any_space] * 4 + [in_vmem] * 6,
            out_specs=in_vmem,
            scratch_shapes=[
                vmem((n_fs * k_rows, 4 * units), BF16),
                vmem((n_fs // 2, 2 * units, 2 * LANES), BF16),
                vmem((n_fs * k_rows, 3 * chan_w), BF16),
                vmem((chan, 2 * LANES), BF16),
                vmem((n_tp, 8, width), F32),
                vmem((8, feat), F32),
                vmem((16, chan), F32),
                vmem((2 * nq, rows, feat), BF16),
                vmem((nq, rows, feat), BF16),
                vmem((nq, rows, feat), BF16),
                vmem((nq, rows, chan), BF16),
                vmem((2 * tokens, feat), BF16),
                vmem((rows, chan), BF16),
                vmem((2 * tokens, 2 * units), BF16),
                vmem((rows // LEN, LEN + 32, chan_w), F32),
                vmem((nq, rows, width), BF16),
                vmem((nq, rows, width), BF16),
                vmem((2 * nq, 4, rows, width), F32),
                vmem((2 * nq, 14, rows, width), BF16),
                vmem((nq, 14, rows, width), BF16),
                dma((5 + nq,)),
                dma((4, 2, 2, n_fs // 2)),
                dma((4, 2, 2)),
                dma((3,)),
                dma((3,)),
                dma((n_tp,)),
                dma((n_tp - 1,)),
                dma((n_tp, 2)),
                dma((1,)),
                dma((4, 2 * nq, 9)),
                dma((4, 2 * nq, 9)),
                dma((2, 2 * nq, 5)),
                dma((2, 2 * nq, 5)),
                dma((2, nq)),
                dma((2, nq)),
            ],
            compiler_params=pltpu.CompilerParams(
                collective_id=0, has_side_effects=True, vmem_limit_bytes=60 * 1024 * 1024
            ),
        )(
            stream_in,
            w_gate.T,
            w_upward.T,
            w_down,
            w_value,
            w_glu_gate,
            w_mix_out,
            conv_taps,
            gain_before,
            gain_mixer,
            gain_after,
            chan_gain,
            chan_bias,
        )

    in_specs = (
        P(("grp", "fs"), "tp"),
        P("tp"),
        P("tp"),
        P("tp"),
        P("fs", "tp"),
        P("fs", "tp"),
        P("tp", "fs"),
        P("fs", "tp"),
        P("fs", "tp"),
        P(None, "tp"),
        P("tp"),
        P("tp"),
        P("tp", "fs"),
    )
    out_specs = P(("grp", "fs"), "tp")
    return jax.shard_map(local, mesh=mesh, in_specs=in_specs, out_specs=out_specs, check_vma=False)
```

```python
import jax
import jax.numpy as jnp
from jax import lax
from jax.experimental import pallas as pl
from jax.experimental.pallas import tpu as pltpu
from jax.sharding import PartitionSpec as P

MESH = pl.DeviceIdType.MESH
LEN = 128
EPS = 1e-06
LANES = 128
CHUNKS = 3
BF16, F32 = jnp.bfloat16, jnp.float32


def remote(src, dst, send_sem, recv_sem, where):
    return pltpu.make_async_remote_copy(
        src_ref=src,
        dst_ref=dst,
        send_sem=send_sem,
        recv_sem=recv_sem,
        device_id=where,
        device_id_type=MESH,
    )


def layer_kernel(
    n_fs,
    n_tp,
    s_in,
    gate_in,
    up_in,
    wd_in,
    value_in,
    glu_in,
    mix_in,
    taps_in,
    before_in,
    mixer_in,
    after_in,
    cgain_in,
    cbias_in,
    out,
    gu,
    wd,
    vm,
    mxb,
    pk,
    gf,
    cgb,
    sb0,
    sb1,
    sb3,
    cvb,
    ub,
    mixed,
    hid,
    pad,
    ybo,
    ybi,
    acc,
    rs0,
    rs1,
    load_sem,
    z_recv,
    z_send,
    y_recv,
    y_send,
    pk_recv,
    pk_send,
    mx_recv,
    mx_send,
    ag_recv,
    ag_send,
    rs_recv,
    rs_send,
    yx_recv,
    yx_send,
):
    z, t, g = lax.axis_index("fs"), lax.axis_index("tp"), lax.axis_index("grp")
    parity = lax.rem(g, 2)
    partner = {"grp": g + 1 - 2 * parity}
    z_right = {"fs": lax.rem(z + 1, n_fs)}
    z_left = {"fs": lax.rem(z + n_fs - 1, n_fs)}
    chips = n_tp // 2
    x, core = t // 2, lax.rem(t, 2)
    xr, xl, xo = lax.rem(x + 1, chips), lax.rem(x + 3, chips), lax.rem(x + 2, chips)
    other = 1 - core
    sib = {"tp": 2 * x + other}
    x_right, x_left = {"tp": 2 * xr + core}, {"tp": 2 * xl + core}

    nq, rows, width = sb1.shape[0], sb1.shape[1], s_in.shape[1]
    half = rows // 2
    feat = width * n_tp
    k_rows, chan_w = value_in.shape
    chan = chan_w * n_tp
    steps = n_fs // 2
    own_units = gate_in.shape[0] // 2
    units = wd.shape[1] // 2
    pairs = units // LANES
    mine, theirs = parity, 1 - parity

    own_k = pl.ds(pl.multiple_of(z * k_rows, k_rows), k_rows)

    own_w = pl.ds(pl.multiple_of(t * width, width), width)

    def own_loads():
        for h in range(2):
            yield pltpu.make_async_copy(
                wd_in.at[h * own_units : (h + 1) * own_units, :],
                wd.at[
                    z // 2,
                    h * units : h * units + own_units,
                    pl.ds(pl.multiple_of(lax.rem(z, 2) * LANES, LANES), LANES),
                ],
                load_sem.at[0],
            )
        for i, ref in enumerate((value_in, glu_in, mix_in)):
            yield pltpu.make_async_copy(ref, vm.at[own_k, i * chan_w : (i + 1) * chan_w], load_sem.at[1])
        for q in range(nq):
            yield pltpu.make_async_copy(
                s_in.at[pl.ds(q * rows, rows), :],
                sb0.at[nq + q, :, pl.ds(pl.multiple_of(t * width, width), width)],
                load_sem.at[2],
            )

    for copy in own_loads():
        copy.start()

    for h in range(2):
        for i in range(pairs):
            lo = h * own_units + i * LANES
            hi = min(lo + LANES, (h + 1) * own_units)
            for j, ref in enumerate((gate_in, up_in)):
                v = ref[lo:hi, :]
                if hi - lo < LANES:
                    v = jnp.concatenate([v, jnp.zeros((LANES - hi + lo, k_rows), BF16)], axis=0)
                c = h * 2 * units + (2 * i + j) * LANES
                gu[own_k, c : c + LANES] = v.T
        wd[:, h * units + own_units : (h + 1) * units, :] = jnp.zeros((wd.shape[0], units - own_units, wd.shape[2]), BF16)
    for i, ref in enumerate((before_in, mixer_in, after_in)):
        pk[t, i : i + 1, :] = ref[...].astype(F32).reshape(1, width)
    pk[t, 3:4, :chan_w] = cgain_in[...].astype(F32).reshape(1, chan_w)
    pk[t, 3:4, chan_w:] = cbias_in[...].astype(F32).reshape(1, chan_w)
    pk[t, 4:8, :] = jnp.zeros((4, width), F32)

    barrier = pltpu.get_barrier_semaphore()
    peers = [z_right, z_left, partner] + [{"tp": lax.rem(t + i, n_tp)} for i in range(1, n_tp)]
    for peer in peers:
        pl.semaphore_signal(barrier, inc=1, device_id=peer, device_id_type=MESH)
    pl.semaphore_wait(barrier, len(peers))

    ref = vm.at[own_k, :]
    pltpu.make_async_copy(wd_in, wd_in, load_sem.at[0]).wait()
    pltpu.make_async_copy(ref, ref, load_sem.at[1]).wait()
    pltpu.make_async_copy(s_in, s_in, load_sem.at[2]).wait()

    wide = 2 * LANES * (pairs - 1)
    A0, A1, B, X, M, D = range(6)

    def piece(kind, f, part=None):
        if kind in (B, D):
            size = own_units if part is None else own_units // 2
            q0 = (mine if kind == B else theirs) * units + (0 if part is None else part * size)
            return wd.at[
                f // 2,
                pl.ds(pl.multiple_of(q0, 16), size),
                pl.ds(pl.multiple_of(lax.rem(f, 2) * LANES, LANES), LANES),
            ]
        size = k_rows if part is None else k_rows // 2
        r0 = pl.ds(pl.multiple_of(f * k_rows + (0 if part is None else part * size), size), size)
        c0 = mine * 2 * units
        if kind == A0:
            return gu.at[r0, pl.ds(pl.multiple_of(c0, LANES), wide)]
        if kind == A1:
            return gu.at[r0, pl.ds(pl.multiple_of(c0 + wide, LANES), 2 * units - wide)]
        if kind == X:
            return vm.at[r0, pl.ds(pl.multiple_of(mine * chan_w, LANES), chan_w)]
        return vm.at[r0, 2 * chan_w : 3 * chan_w]

    def many(kind, count):
        if kind in (B, D):
            if count <= wd.shape[0]:
                return wd.at[0:count, 0:own_units, 0:LANES]
            total = count * own_units // 2
            for a in range(1, wd.shape[0] + 1):
                if total % (16 * a) == 0 and total // a <= wd.shape[1]:
                    return wd.at[0:a, 0 : total // a, :]
        if kind == A0:
            return gu.at[0 : count * k_rows, 0:wide]
        if kind == A1:
            return gu.at[0 : count * k_rows, 0 : 2 * units - wide]
        return vm.at[0 : count * k_rows, 0:chan_w]

    def origin(way, s):
        return lax.rem(z + n_fs - s, n_fs) if way == 0 else lax.rem(z + s, n_fs)

    def z_sem(kind, way, s):
        if kind < X:
            return z_recv.at[(kind * 2 + way) * steps + s - 1]
        return z_recv.at[(2 * X + kind - X) * steps + s - 1]

    def z_copy(kind, way, s_next):
        ref = piece(kind, origin(way, s_next - 1), None if s_next < steps else way)
        return remote(ref, ref, z_send.at[kind], z_sem(kind, way, s_next), z_right if way == 0 else z_left)

    def y_copy(ref, i):
        return remote(ref, ref, y_send.at[i], y_recv.at[i], partner)

    def y_all(i):
        return y_copy(many((A0, A1, X)[i], n_fs - 1), i)

    def stream_copy(q):
        return remote(sb0.at[nq + q, :, own_w], sb0.at[q, :, own_w], yx_send.at[0], yx_recv.at[nq], partner)

    def part_copy(q):
        return remote(ybo.at[q], ybi.at[q], yx_send.at[1], yx_recv.at[q], partner)

    def spread_mix(f):
        dest, b = f // 2, lax.rem(f, 2)
        src = piece(M, f)
        dst = mxb.at[
            pl.ds(pl.multiple_of(t * chan_w, chan_w), chan_w), pl.ds(pl.multiple_of(b * LANES, LANES), LANES)
        ]

        @pl.when(dest != t)
        def _():
            remote(src, dst, mx_send.at[0], mx_recv.at[0], {"tp": dest}).start()

        @pl.when(dest == t)
        def _():
            pltpu.make_async_copy(src, dst, mx_recv.at[0]).start()

    def relay(kind, s):
        for way in range(2):
            part = None if s < steps else way
            if kind < X or way == 0:
                ref = piece(kind, origin(way, s), part) if kind < X else many(kind, 2 if s < steps else 1)
                remote(ref, ref, z_send.at[kind], z_sem(kind, way, s), z_right).wait_recv()
            if s < steps:
                z_copy(kind, way, s + 1).start()
            if kind in (A0, X):
                y_copy(piece(kind, origin(way, s), part), 0 if kind == A0 else 2).start()
            if kind == M and (s < steps or way == 0):
                spread_mix(origin(way, s))

    def block(buf, w, q, b, part=None):
        rws = slice(None) if part is None else pl.ds(part * half, half)
        return buf.at[q, rws, pl.ds(pl.multiple_of(b * w, w), w)]

    def ag_copy(n, ref, slot, i, where):
        return remote(ref, ref, ag_send.at[n], ag_recv.at[slot, i], where)

    def ag_slot(n, q):
        return q // nq if n == 0 else 2 + (n - 1) * nq + q

    def ag_chunks(n, q):
        return slice(q, q + nq) if n == 0 else q

    def ag_start(n, buf, w, q):
        slot, own = ag_slot(n, q), block(buf, w, ag_chunks(n, q), t)
        ag_copy(n, own, slot, 0, x_right).start()
        ag_copy(n, own, slot, 0, x_left).start()
        ag_copy(n, own, slot, 2, sib).start()

    def ag_wait(n, buf, w, q, i, count):
        ag_copy(n, buf.at[ag_chunks(n, q), :, 0 : count * w], ag_slot(n, q), i, sib).wait_recv()

    def ag_relay(n, buf, w, q):
        slot, c = ag_slot(n, q), ag_chunks(n, q)
        b_l, b_r = 2 * xl + core, 2 * xr + core
        ag_wait(n, buf, w, q, 0, 2)
        ag_copy(n, block(buf, w, c, b_l, 0), slot, 1, x_right).start()
        ag_copy(n, block(buf, w, c, b_r, 1), slot, 1, x_left).start()
        ag_copy(n, block(buf, w, c, b_l), slot, 2, sib).start()
        ag_copy(n, block(buf, w, c, b_r), slot, 2, sib).start()

    def ag_opposite(n, buf, w, q):
        ag_wait(n, buf, w, q, 1, 1)
        ag_copy(n, block(buf, w, ag_chunks(n, q), 2 * xo + core), ag_slot(n, q), 2, sib).start()

    def ag_end(n, buf, w, q):
        ag_wait(n, buf, w, q, 2, 4)

    def ag_drain(n, buf, w):
        ag_copy(n, buf.at[:, :, 0 : 7 * w], 0, 0, sib).wait_send()

    order = (xo, xr, xl, x)
    rs_refs = (rs0, rs1)

    def rs_copy(src, dst, n, q, i, where):
        return remote(
            rs_refs[n].at[(q, *src)], rs_refs[n].at[(q, *dst)], rs_send.at[n], rs_recv.at[2 * nq * n + q, i], where
        )

    def sib_copy(n, q):
        return rs_copy((slice(0, 4),), (slice(4, 8),), n, q, 0, sib)

    def opp_copy(n, q, i):
        part = pl.ds(i * half, half)
        return rs_copy((8, part), (9, part), n, q, 1, x_right if i == 0 else x_left)

    def nb_copy(n, q, i):
        return rs_copy((10 + i,), (12 + i,), n, q, 2, x_right if i == 0 else x_left)

    def rs_partials(n, q):
        buf = rs_refs[n]
        width_k = units if n == 0 else 2 * units
        k_range = pl.ds(pl.multiple_of(mine * units, LANES), units) if n == 0 else slice(None)
        h = hid[q * rows : (q + 1) * rows, 0:width_k]
        for k in range(4):
            buf[q, k] = jnp.dot(h, wd[2 * order[k] + other, k_range, :], preferred_element_type=F32).astype(BF16)
        sib_copy(n, q).start()
        for k in range(4):
            acc[q, k] = jnp.dot(h, wd[2 * order[k] + core, k_range, :], preferred_element_type=F32)

    def rs_opposite(n, q):
        buf = rs_refs[n]
        sib_copy(n, q).wait_recv()
        buf[q, 8] = (acc[q, 0] + buf[q, 4].astype(F32)).astype(BF16)
        opp_copy(n, q, 0).start()
        opp_copy(n, q, 1).start()

    def rs_neighbours(n, q):
        buf = rs_refs[n]
        rs_copy((9,), (9,), n, q, 1, sib).wait_recv()
        for i in range(2):
            near, far = pl.ds(i * half, half), pl.ds((1 - i) * half, half)
            buf[q, 10 + i, near] = (
                acc[q, 1 + i, near] + buf[q, 5 + i, near].astype(F32) + buf[q, 9, near].astype(F32)
            ).astype(BF16)
            buf[q, 10 + i, far] = (acc[q, 1 + i, far] + buf[q, 5 + i, far].astype(F32)).astype(BF16)
            nb_copy(n, q, i).start()

    def rs_total(n, q):
        buf = rs_refs[n]
        rs_copy((slice(12, 14),), (slice(12, 14),), n, q, 2, sib).wait_recv()
        return acc[q, 3] + buf[q, 7].astype(F32) + buf[q, 12].astype(F32) + buf[q, 13].astype(F32)

    def rs_drain(n):
        ref = rs_refs[n].at[:, 0:7]
        remote(ref, ref, rs_send.at[n], rs_recv.at[0, 0], sib).wait_send()

    def norm_rows(buf, q, r, base):
        @pl.loop(0, rows // 16, unroll=4)
        def _(i):
            rws = pl.ds(pl.multiple_of(i * 16, 16), 16)
            v = buf[q, rws, :].astype(F32)
            inverse = lax.rsqrt(jnp.sum(v * v, axis=1, keepdims=True) / feat + EPS)
            ub[pl.ds(pl.multiple_of(base + i * 16, 16), 16), :] = (v * inverse * gf[r : r + 1, :]).astype(BF16)

    def hidden_rows(lo, count, columns, n_pairs):
        r = jnp.dot(ub[lo : lo + count, :], gu[:, columns], preferred_element_type=F32)
        for n in range(n_pairs):
            a, b = r[:, 2 * n * LANES : (2 * n + 1) * LANES], r[:, (2 * n + 1) * LANES : (2 * n + 2) * LANES]
            hid[lo : lo + count, n * LANES : (n + 1) * LANES] = (jax.nn.silu(a) * b).astype(BF16)

    def conv(q):
        r = jnp.dot(ub[q * rows : (q + 1) * rows, :], vm[:, : 2 * chan_w], preferred_element_type=F32)
        glued = r[:, :chan_w] * jax.nn.sigmoid(r[:, chan_w:])
        for i in range(rows // LEN):
            pad[i, 32:, :] = glued[i * LEN : (i + 1) * LEN]
        n_taps = taps_in.shape[0]
        taps = taps_in[...].astype(F32)
        for i in range(rows // LEN):
            total = jnp.zeros((LEN, chan_w), F32)
            for k in range(n_taps):
                total = total + taps[k : k + 1, :] * pad[i, 33 - n_taps + k : 33 - n_taps + k + LEN, :]
            cvb[q, i * LEN : (i + 1) * LEN, pl.ds(pl.multiple_of(t * chan_w, chan_w), chan_w)] = total.astype(BF16)

    def channel_norm(q):
        @pl.loop(0, rows // 16, unroll=4)
        def _(i):
            rws = pl.ds(pl.multiple_of(i * 16, 16), 16)
            v = cvb[q, rws, :].astype(F32)
            mu = jnp.sum(v, axis=1, keepdims=True) / chan
            msq = jnp.sum(v * v, axis=1, keepdims=True) / chan
            w = (v - mu) * lax.rsqrt(msq - mu * mu + EPS) * cgb[3:4, :] + cgb[11:12, :]
            mixed[rws, :] = jax.nn.silu(w).astype(BF16)

    def own_cols(buf, q):
        return buf[q, :, own_w]

    def z_begin(kinds):
        for kind in kinds:
            for way in range(2):
                z_copy(kind, way, 1).start()

    def relays(kinds, s):
        for kind in kinds:
            relay(kind, s)

    first_kinds = (A0, A1, B)

    def phase(name):
        return jax.named_scope(name)

    chunks = range(nq)
    z_begin(first_kinds)
    for q in chunks:
        stream_copy(q).start()
    ag_start(0, sb0, width, nq)

    def pk_copy(i):
        return remote(pk.at[t], pk.at[t], pk_send.at[0], pk_recv.at[0], {"tp": lax.rem(t + i, n_tp)})

    pk_all = remote(pk.at[0 : n_tp - 1], pk.at[0 : n_tp - 1], pk_send.at[0], pk_recv.at[0], sib)

    for i in range(1, n_tp):
        pk_copy(i).start()
    spread_mix(z)
    pad[:, :32, :] = jnp.zeros((pad.shape[0], 32, chan_w), F32)

    with phase("w1"):
        relays(first_kinds, 1)
    with phase("ag0"):
        ref = sb0.at[0:nq, :, 0:width]
        remote(ref, ref, yx_send.at[0], yx_recv.at[nq], partner).wait_recv()
        ag_start(0, sb0, width, 0)
        ag_relay(0, sb0, width, nq)
    with phase("w2"):
        relays(first_kinds, 2)
    ag_relay(0, sb0, width, 0)
    ag_opposite(0, sb0, width, nq)
    with phase("w3"):
        relays(first_kinds, 3)
    ag_opposite(0, sb0, width, 0)
    ag_end(0, sb0, width, nq)
    pk_all.wait_recv()
    for b in range(n_tp):
        gf[:, b * width : (b + 1) * width] = pk[b]
        cgb[0:8, b * chan_w : (b + 1) * chan_w] = pk[b][:, :chan_w]
        cgb[8:16, b * chan_w : (b + 1) * chan_w] = pk[b][:, chan_w : 2 * chan_w]
    with phase("w4"):
        relays(first_kinds, 4)
    ag_end(0, sb0, width, 0)
    pl.loop(nq, 2 * nq)(lambda q: norm_rows(sb0, q, 0, q * rows))
    with phase("w5"):
        relays(first_kinds, 5)
    pl.loop(0, nq)(lambda q: norm_rows(sb0, q, 0, q * rows))
    with phase("w67"):
        relays(first_kinds, 6)
        relays(first_kinds, 7)
    z_begin((X,))
    with phase("w8"):
        relays(first_kinds, 8)

    def late(*steps_of):
        with phase("late"):
            for kind, i in steps_of:
                relay(kind, i)

    def y_late(lo, hi):
        @pl.loop(lo, hi)
        def _(i):
            y_copy(piece(A1, lax.rem(z + i, n_fs)), 1).start()

    tokens = nq * rows
    my_half = pl.ds(pl.multiple_of(mine * 2 * units, LANES), 2 * units)
    with phase("hid_theirs"):
        hidden_rows(0, tokens, my_half, pairs)
    with phase("part_theirs"):
        for q in chunks:
            rs_partials(0, q)
    late((X, 1))
    y_late(1, 5)
    with phase("hid_ours"):
        hidden_rows(tokens, tokens, my_half, pairs)
    with phase("rs_a"):
        rs_opposite(0, 0)
        rs_opposite(0, 1)
        rs_partials(0, nq)
        late((X, 2))
        rs_opposite(0, 2)
        rs_neighbours(0, 0)
        rs_partials(0, nq + 1)
    late((X, 3))

    def pass_over(q):
        ybo[q] = rs_total(0, q).astype(BF16)
        part_copy(q).start()

    with phase("rs_b"):
        rs_neighbours(0, 1)
        rs_partials(0, nq + 2)
        rs_neighbours(0, 2)
        rs_opposite(0, 3)
    late((X, 4))
    z_begin((M,))
    with phase("rs_c"):
        pass_over(0)
        rs_opposite(0, 4)
        pass_over(1)
        rs_neighbours(0, 3)
        rs_opposite(0, 5)
        pass_over(2)
    late((X, 5), (M, 1))
    z_begin((D,))
    with phase("rs_d"):
        rs_neighbours(0, 4)
        rs_neighbours(0, 5)

    def first(q):
        total = rs_total(0, nq + q)
        part_copy(q).wait_recv()
        sb1[q, :, own_w] = (own_cols(sb0, nq + q).astype(F32) + 0.5 * (total + ybi[q].astype(F32))).astype(BF16)
        ag_start(1, sb1, width, q)

    with phase("first0"):
        first(0)
    late((X, 6), (M, 2))
    with phase("first12"):
        first(1)
        first(2)
    late((X, 7), (M, 3), (D, 1))
    with phase("ag1"):
        ag_relay(1, sb1, width, 0)
        ag_relay(1, sb1, width, 1)
        ag_relay(1, sb1, width, 2)
    late((X, 8), (M, 4))
    y_late(5, n_fs)
    with phase("opp1"):
        ag_opposite(1, sb1, width, 0)
        ag_opposite(1, sb1, width, 1)
    late((M, 5), (D, 2))

    def conv_stage(q):
        ag_end(1, sb1, width, q)
        norm_rows(sb1, q, 1, q * rows)
        conv(q)
        ag_start(2, cvb, chan_w, q)

    with phase("ywaitx"):
        y_all(2).wait_recv()
    with phase("conv0"):
        conv_stage(0)
    late((M, 6), (D, 3))
    with phase("conv1"):
        ag_opposite(1, sb1, width, 2)
        conv_stage(1)
    late((M, 7), (D, 4))
    with phase("conv2"):
        ag_relay(2, cvb, chan_w, 0)
        conv_stage(2)
    late((M, 8), (D, 5))
    with phase("ag2"):
        ag_relay(2, cvb, chan_w, 1)
        ag_opposite(2, cvb, chan_w, 0)
        ag_relay(2, cvb, chan_w, 2)
        ag_opposite(2, cvb, chan_w, 1)

    def mix_stage(q):
        ag_end(2, cvb, chan_w, q)
        channel_norm(q)
        branch = jnp.dot(mixed[...], mxb[...], preferred_element_type=F32)
        sb3[q, :, own_w] = (own_cols(sb1, q).astype(F32) + branch).astype(BF16)
        ag_start(3, sb3, width, q)

    with phase("mixw"):
        pltpu.make_async_copy(mxb, mxb, mx_recv.at[0]).wait()
    with phase("mix0"):
        mix_stage(0)
    late((D, 6))
    with phase("mix12"):
        ag_opposite(2, cvb, chan_w, 2)
        mix_stage(1)
        ag_relay(3, sb3, width, 0)
        mix_stage(2)
    late((D, 7))
    with phase("ag3"):
        ag_relay(3, sb3, width, 1)
        ag_opposite(3, sb3, width, 0)
        ag_relay(3, sb3, width, 2)
        ag_opposite(3, sb3, width, 1)
    late((D, 8))
    with phase("ywait"):
        for i in range(2):
            y_all(i).wait_recv()

    def ffn_stage(q):
        ag_end(3, sb3, width, q)
        norm_rows(sb3, q, 2, q * rows)
        hidden_rows(q * rows, rows, slice(None), 2 * pairs)
        rs_partials(1, q)

    def last(q):
        total = rs_total(1, q)
        out[q * rows : (q + 1) * rows, :] = (own_cols(sb3, q).astype(F32) + 0.5 * total).astype(BF16)

    with phase("ffn0"):
        ffn_stage(0)
    with phase("ffn1"):
        ag_opposite(3, sb3, width, 2)
        ffn_stage(1)
    with phase("ffn2"):
        rs_opposite(1, 0)
        ffn_stage(2)
    with phase("rs1"):
        rs_opposite(1, 1)
        rs_neighbours(1, 0)
        rs_opposite(1, 2)
        rs_neighbours(1, 1)
    with phase("last"):
        last(0)
        rs_neighbours(1, 2)
        last(1)
        last(2)

    for kind in range(6):
        ref = many(kind, n_fs - 1)
        remote(ref, ref, z_send.at[kind], z_recv.at[0], z_right).wait_send()
    for i in range(3):
        y_all(i).wait_send()
    pk_all.wait_send()
    ref = mxb.at[pl.ds(0, (n_tp - 1) * chan_w), :]
    remote(ref, ref, mx_send.at[0], mx_recv.at[0], sib).wait_send()
    ref = sb0.at[0:nq, :, 0:width]
    remote(ref, ref, yx_send.at[0], yx_recv.at[0], partner).wait_send()
    remote(ybo, ybo, yx_send.at[1], yx_recv.at[0], partner).wait_send()
    for n, buf, w in ((0, sb0, width), (1, sb1, width), (2, cvb, chan_w), (3, sb3, width)):
        ag_drain(n, buf, w)
    for n in range(2):
        rs_drain(n)


def solution(mesh):
    n_fs, n_tp = mesh.shape["fs"], mesh.shape["tp"]

    def local(
        stream_in,
        gain_before,
        gain_mixer,
        gain_after,
        w_gate,
        w_upward,
        w_down,
        w_value,
        w_glu_gate,
        conv_taps,
        chan_gain,
        chan_bias,
        w_mix_out,
    ):
        tokens, width = stream_in.shape
        k_rows, hidden = w_gate.shape
        chan_w = w_value.shape[1]
        units = -(-(hidden // 2) // LANES) * LANES
        nq = CHUNKS
        rows = tokens // nq
        feat, chan = width * n_tp, chan_w * n_tp
        vmem = pltpu.VMEM
        dma = pltpu.SemaphoreType.DMA
        any_space = pl.BlockSpec(memory_space=pl.ANY)
        in_vmem = pl.BlockSpec(memory_space=pltpu.VMEM)
        return pl.pallas_call(
            lambda *refs: layer_kernel(n_fs, n_tp, *refs),
            out_shape=jax.ShapeDtypeStruct((tokens, width), BF16),
            in_specs=[any_space, in_vmem, in_vmem] + [any_space] * 4 + [in_vmem] * 6,
            out_specs=in_vmem,
            scratch_shapes=[
                vmem((n_fs * k_rows, 4 * units), BF16),
                vmem((n_fs // 2, 2 * units, 2 * LANES), BF16),
                vmem((n_fs * k_rows, 3 * chan_w), BF16),
                vmem((chan, 2 * LANES), BF16),
                vmem((n_tp, 8, width), F32),
                vmem((8, feat), F32),
                vmem((16, chan), F32),
                vmem((2 * nq, rows, feat), BF16),
                vmem((nq, rows, feat), BF16),
                vmem((nq, rows, feat), BF16),
                vmem((nq, rows, chan), BF16),
                vmem((2 * tokens, feat), BF16),
                vmem((rows, chan), BF16),
                vmem((2 * tokens, 2 * units), BF16),
                vmem((rows // LEN, LEN + 32, chan_w), F32),
                vmem((nq, rows, width), BF16),
                vmem((nq, rows, width), BF16),
                vmem((2 * nq, 4, rows, width), F32),
                vmem((2 * nq, 14, rows, width), BF16),
                vmem((nq, 14, rows, width), BF16),
                dma((3,)),
                dma((9 * (n_fs // 2),)),
                dma((6,)),
                dma((3,)),
                dma((3,)),
                dma((1,)),
                dma((1,)),
                dma((1,)),
                dma((1,)),
                dma((2 + 3 * nq, 3)),
                dma((4,)),
                dma((3 * nq, 3)),
                dma((2,)),
                dma((nq + 1,)),
                dma((2,)),
            ],
            compiler_params=pltpu.CompilerParams(
                collective_id=0, has_side_effects=True, vmem_limit_bytes=60 * 1024 * 1024
            ),
        )(
            stream_in,
            w_gate.T,
            w_upward.T,
            w_down,
            w_value,
            w_glu_gate,
            w_mix_out,
            conv_taps,
            gain_before,
            gain_mixer,
            gain_after,
            chan_gain,
            chan_bias,
        )

    in_specs = (
        P(("grp", "fs"), "tp"),
        P("tp"),
        P("tp"),
        P("tp"),
        P("fs", "tp"),
        P("fs", "tp"),
        P("tp", "fs"),
        P("fs", "tp"),
        P("fs", "tp"),
        P(None, "tp"),
        P("tp"),
        P("tp"),
        P("tp", "fs"),
    )
    out_specs = P(("grp", "fs"), "tp")
    return jax.shard_map(local, mesh=mesh, in_specs=in_specs, out_specs=out_specs, check_vma=False)
```

```python
import jax
import jax.numpy as jnp
from jax import lax
from jax.experimental import pallas as pl
from jax.experimental.pallas import tpu as pltpu
from jax.sharding import PartitionSpec as P

MESH = pl.DeviceIdType.MESH
LEN = 128
EPS = 1e-06
LANES = 128
CHUNKS = 3
BF16, F32 = jnp.bfloat16, jnp.float32


def remote(src, dst, send_sem, recv_sem, where):
    return pltpu.make_async_remote_copy(
        src_ref=src,
        dst_ref=dst,
        send_sem=send_sem,
        recv_sem=recv_sem,
        device_id=where,
        device_id_type=MESH,
    )


def layer_kernel(
    n_fs,
    n_tp,
    s_in,
    gate_in,
    up_in,
    wd_in,
    value_in,
    glu_in,
    mix_in,
    taps_in,
    before_in,
    mixer_in,
    after_in,
    cgain_in,
    cbias_in,
    out,
    gu,
    wd,
    vm,
    mxb,
    pk,
    gf,
    cgb,
    sb0,
    sb1,
    sb3,
    cvb,
    ub,
    mixed,
    hid,
    pad,
    ybo,
    ybi,
    acc,
    rs0,
    rs1,
    load_sem,
    z_recv,
    z_send,
    y_recv,
    y_send,
    pk_recv,
    pk_send,
    mx_recv,
    mx_send,
    ag_recv,
    ag_send,
    rs_recv,
    rs_send,
    yx_recv,
    yx_send,
    part,
):
    z, t, g = lax.axis_index("fs"), lax.axis_index("tp"), lax.axis_index("grp")
    parity = lax.rem(g, 2)
    partner = {"grp": g + 1 - 2 * parity}
    z_right = {"fs": lax.rem(z + 1, n_fs)}
    z_left = {"fs": lax.rem(z + n_fs - 1, n_fs)}
    z_two = ({"fs": lax.rem(z + 2, n_fs)}, {"fs": lax.rem(z + n_fs - 2, n_fs)})
    chips = n_tp // 2
    x, core = t // 2, lax.rem(t, 2)
    xr, xl, xo = lax.rem(x + 1, chips), lax.rem(x + 3, chips), lax.rem(x + 2, chips)
    other = 1 - core
    sib = {"tp": 2 * x + other}
    x_right, x_left = {"tp": 2 * xr + core}, {"tp": 2 * xl + core}

    nq, rows, width = sb1.shape[0], sb1.shape[1], s_in.shape[1]
    half = rows // 2
    feat = width * n_tp
    k_rows, chan_w = value_in.shape
    chan = chan_w * n_tp
    steps = n_fs // 2
    own_units = gate_in.shape[0] // 2
    units = wd.shape[1] // 2
    pairs = units // LANES
    mine, theirs = parity, 1 - parity

    own_k = pl.ds(pl.multiple_of(z * k_rows, k_rows), k_rows)

    own_w = pl.ds(pl.multiple_of(t * width, width), width)

    def own_loads():
        for h in range(2):
            yield pltpu.make_async_copy(
                wd_in.at[h * own_units : (h + 1) * own_units, :],
                wd.at[
                    z // 2,
                    h * units : h * units + own_units,
                    pl.ds(pl.multiple_of(lax.rem(z, 2) * LANES, LANES), LANES),
                ],
                load_sem.at[0],
            )
        for i, ref in enumerate((value_in, glu_in, mix_in)):
            yield pltpu.make_async_copy(ref, vm.at[own_k, i * chan_w : (i + 1) * chan_w], load_sem.at[1])
        for q in range(nq):
            yield pltpu.make_async_copy(
                s_in.at[pl.ds(q * rows, rows), :],
                sb0.at[nq + q, :, pl.ds(pl.multiple_of(t * width, width), width)],
                load_sem.at[2],
            )

    for copy in own_loads():
        copy.start()

    for h in range(2):
        for i in range(pairs):
            lo = h * own_units + i * LANES
            hi = min(lo + LANES, (h + 1) * own_units)
            for j, ref in enumerate((gate_in, up_in)):
                v = ref[lo:hi, :]
                if hi - lo < LANES:
                    v = jnp.concatenate([v, jnp.zeros((LANES - hi + lo, k_rows), BF16)], axis=0)
                c = h * 2 * units + (2 * i + j) * LANES
                gu[own_k, c : c + LANES] = v.T
        wd[:, h * units + own_units : (h + 1) * units, :] = jnp.zeros((wd.shape[0], units - own_units, wd.shape[2]), BF16)
    for i, ref in enumerate((before_in, mixer_in, after_in)):
        pk[t, i : i + 1, :] = ref[...].astype(F32).reshape(1, width)
    pk[t, 3:4, :chan_w] = cgain_in[...].astype(F32).reshape(1, chan_w)
    pk[t, 3:4, chan_w:] = cbias_in[...].astype(F32).reshape(1, chan_w)
    pk[t, 4:8, :] = jnp.zeros((4, width), F32)

    barrier = pltpu.get_barrier_semaphore()
    peers = [z_right, z_left, *z_two, partner] + [{"tp": lax.rem(t + i, n_tp)} for i in range(1, n_tp)]
    for peer in peers:
        pl.semaphore_signal(barrier, inc=1, device_id=peer, device_id_type=MESH)
    pl.semaphore_wait(barrier, len(peers))

    ref = vm.at[own_k, :]
    pltpu.make_async_copy(wd_in, wd_in, load_sem.at[0]).wait()
    pltpu.make_async_copy(ref, ref, load_sem.at[1]).wait()
    pltpu.make_async_copy(s_in, s_in, load_sem.at[2]).wait()

    wide = 2 * LANES * (pairs - 1)
    A0, A1, B, X, M, D = range(6)

    def piece(kind, f, part=None):
        if kind in (B, D):
            size = own_units if part is None else own_units // 2
            q0 = (mine if kind == B else theirs) * units + (0 if part is None else part * size)
            return wd.at[
                f // 2,
                pl.ds(pl.multiple_of(q0, 16), size),
                pl.ds(pl.multiple_of(lax.rem(f, 2) * LANES, LANES), LANES),
            ]
        size = k_rows if part is None else k_rows // 2
        r0 = pl.ds(pl.multiple_of(f * k_rows + (0 if part is None else part * size), size), size)
        c0 = mine * 2 * units
        if kind == A0:
            return gu.at[r0, pl.ds(pl.multiple_of(c0, LANES), wide)]
        if kind == A1:
            return gu.at[r0, pl.ds(pl.multiple_of(c0 + wide, LANES), 2 * units - wide)]
        if kind == X:
            return vm.at[r0, pl.ds(pl.multiple_of(mine * chan_w, LANES), chan_w)]
        return vm.at[r0, 2 * chan_w : 3 * chan_w]

    def many(kind, count):
        if kind in (B, D):
            if count <= wd.shape[0]:
                return wd.at[0:count, 0:own_units, 0:LANES]
            total = count * own_units // 2
            for a in range(1, wd.shape[0] + 1):
                if total % (16 * a) == 0 and total // a <= wd.shape[1]:
                    return wd.at[0:a, 0 : total // a, :]
        if kind == A0:
            return gu.at[0 : count * k_rows, 0:wide]
        if kind == A1:
            return gu.at[0 : count * k_rows, 0 : 2 * units - wide]
        return vm.at[0 : count * k_rows, 0:chan_w]

    def origin(way, s):
        return lax.rem(z + n_fs - s, n_fs) if way == 0 else lax.rem(z + s, n_fs)

    def z_sem(kind, way, s):
        return z_recv.at[(kind * 2 + way) * steps + s - 1]

    def z_copy(kind, way, s_next):
        ref = piece(kind, origin(way, s_next - 1), None if s_next < steps else way)
        return remote(ref, ref, z_send.at[kind], z_sem(kind, way, s_next), z_right if way == 0 else z_left)

    def y_copy(ref, i):
        return remote(ref, ref, y_send.at[i], y_recv.at[i], partner)

    def y_all(i):
        return y_copy(many((A0, A1, X)[i], n_fs - 1), i)

    def stream_copy(q):
        return remote(sb0.at[nq + q, :, own_w], sb0.at[q, :, own_w], yx_send.at[0], yx_recv.at[nq], partner)

    def part_copy(q):
        return remote(ybo.at[q], ybi.at[q], yx_send.at[1], yx_recv.at[q], partner)

    def spread_mix(f):
        dest, b = f // 2, lax.rem(f, 2)
        src = piece(M, f)
        dst = mxb.at[
            pl.ds(pl.multiple_of(t * chan_w, chan_w), chan_w), pl.ds(pl.multiple_of(b * LANES, LANES), LANES)
        ]

        @pl.when(dest != t)
        def _():
            remote(src, dst, mx_send.at[0], mx_recv.at[0], {"tp": dest}).start()

        @pl.when(dest == t)
        def _():
            pltpu.make_async_copy(src, dst, mx_recv.at[0]).start()

    def relay(kind, s):
        for way in range(2):
            part = None if s < steps else way
            ref = piece(kind, origin(way, s), part)
            remote(ref, ref, z_send.at[kind], z_sem(kind, way, s), z_right).wait_recv()
            if s < steps:
                z_copy(kind, way, s + 1).start()
            if kind == A0:
                y_copy(ref, 0).start()

    def leap_sem(kind, k):
        return z_recv.at[2 * X * steps + (kind - X) * (steps // 2) + k - 1]

    def leap_send(kind, k):
        for far in (True, False):
            for way in range(2):
                part = way if far and 2 * k == steps else None
                ref = piece(kind, origin(way, 2 * k - 2), part)
                where = z_two[way] if far else (z_right, z_left)[way]
                remote(ref, ref, z_send.at[kind], leap_sem(kind, k), where).start()

    def leap(kind, k):
        ref = many(kind, 4 if 2 * k < steps else 3)
        remote(ref, ref, z_send.at[kind], leap_sem(kind, k), z_right).wait_recv()
        if 2 * k < steps:
            leap_send(kind, k + 1)
        for way, d in ((0, 2 * k), (1, 2 * k), (0, 2 * k - 1), (1, 2 * k - 1)):
            if d == steps and way == 1:
                continue
            if kind == X:
                y_copy(piece(X, origin(way, d)), 2).start()
            if kind == M:
                spread_mix(origin(way, d))

    def block(buf, w, q, b, part=None):
        rws = slice(None) if part is None else pl.ds(part * half, half)
        return buf.at[q, rws, pl.ds(pl.multiple_of(b * w, w), w)]

    def ag_copy(n, ref, slot, i, where):
        return remote(ref, ref, ag_send.at[n], ag_recv.at[slot, i], where)

    def ag_slot(n, q):
        return q // nq if n == 0 else 2 + (n - 1) * nq + q

    def ag_chunks(n, q):
        return slice(q, q + nq) if n == 0 else q

    def ag_start(n, buf, w, q):
        slot, own = ag_slot(n, q), block(buf, w, ag_chunks(n, q), t)
        ag_copy(n, own, slot, 0, x_right).start()
        ag_copy(n, own, slot, 0, x_left).start()
        ag_copy(n, own, slot, 2, sib).start()

    def ag_wait(n, buf, w, q, i, count):
        ag_copy(n, buf.at[ag_chunks(n, q), :, 0 : count * w], ag_slot(n, q), i, sib).wait_recv()

    def ag_relay(n, buf, w, q):
        slot, c = ag_slot(n, q), ag_chunks(n, q)
        b_l, b_r = 2 * xl + core, 2 * xr + core
        ag_wait(n, buf, w, q, 0, 2)
        ag_copy(n, block(buf, w, c, b_l, 0), slot, 1, x_right).start()
        ag_copy(n, block(buf, w, c, b_r, 1), slot, 1, x_left).start()
        ag_copy(n, block(buf, w, c, b_l), slot, 2, sib).start()
        ag_copy(n, block(buf, w, c, b_r), slot, 2, sib).start()

    def ag_opposite(n, buf, w, q):
        ag_wait(n, buf, w, q, 1, 1)
        ag_copy(n, block(buf, w, ag_chunks(n, q), 2 * xo + core), ag_slot(n, q), 2, sib).start()

    def ag_end(n, buf, w, q):
        ag_wait(n, buf, w, q, 2, 4)

    def ag_drain(n, buf, w):
        ag_copy(n, buf.at[:, :, 0 : 7 * w], 0, 0, sib).wait_send()

    order = (xo, xr, xl, x)
    rs_refs = (rs0, rs1)

    def rs_copy(src, dst, n, q, i, where):
        return remote(
            rs_refs[n].at[(q, *src)], rs_refs[n].at[(q, *dst)], rs_send.at[n], rs_recv.at[2 * nq * n + q, i], where
        )

    def sib_copy(n, q):
        return rs_copy((slice(0, 4),), (slice(4, 8),), n, q, 0, sib)

    def opp_copy(n, q, i):
        part = pl.ds(i * half, half)
        return rs_copy((8, part), (9, part), n, q, 1, x_right if i == 0 else x_left)

    def nb_copy(n, q, i):
        return rs_copy((10 + i,), (12 + i,), n, q, 2, x_right if i == 0 else x_left)

    def rs_partials(n, q):
        buf = rs_refs[n]
        width_k = units if n == 0 else 2 * units
        k_range = pl.ds(pl.multiple_of(mine * units, LANES), units) if n == 0 else slice(None)
        h = hid[q * rows : (q + 1) * rows, 0:width_k]
        for k in range(4):
            buf[q, k] = jnp.dot(h, wd[2 * order[k] + other, k_range, :], preferred_element_type=F32).astype(BF16)
        sib_copy(n, q).start()
        for k in range(4):
            acc[q, k] = jnp.dot(h, wd[2 * order[k] + core, k_range, :], preferred_element_type=F32)

    def rs_opposite(n, q):
        buf = rs_refs[n]
        sib_copy(n, q).wait_recv()
        buf[q, 8] = (acc[q, 0] + buf[q, 4].astype(F32)).astype(BF16)
        opp_copy(n, q, 0).start()
        opp_copy(n, q, 1).start()

    def rs_neighbours(n, q):
        buf = rs_refs[n]
        rs_copy((9,), (9,), n, q, 1, sib).wait_recv()
        for i in range(2):
            near, far = pl.ds(i * half, half), pl.ds((1 - i) * half, half)
            buf[q, 10 + i, near] = (
                acc[q, 1 + i, near] + buf[q, 5 + i, near].astype(F32) + buf[q, 9, near].astype(F32)
            ).astype(BF16)
            buf[q, 10 + i, far] = (acc[q, 1 + i, far] + buf[q, 5 + i, far].astype(F32)).astype(BF16)
            nb_copy(n, q, i).start()

    def rs_total(n, q):
        buf = rs_refs[n]
        rs_copy((slice(12, 14),), (slice(12, 14),), n, q, 2, sib).wait_recv()
        return acc[q, 3] + buf[q, 7].astype(F32) + buf[q, 12].astype(F32) + buf[q, 13].astype(F32)

    def rs_drain(n):
        ref = rs_refs[n].at[:, 0:7]
        remote(ref, ref, rs_send.at[n], rs_recv.at[0, 0], sib).wait_send()

    def norm_rows(buf, q, r, base):
        @pl.loop(0, rows // 16, unroll=4)
        def _(i):
            rws = pl.ds(pl.multiple_of(i * 16, 16), 16)
            v = buf[q, rws, :].astype(F32)
            inverse = lax.rsqrt(jnp.sum(v * v, axis=1, keepdims=True) / feat + EPS)
            ub[pl.ds(pl.multiple_of(base + i * 16, 16), 16), :] = (v * inverse * gf[r : r + 1, :]).astype(BF16)

    def gate_up(a, b):
        return (jax.nn.silu(a) * b).astype(BF16)

    def hidden_rows(lo, count, columns, n_pairs):
        r = jnp.dot(ub[lo : lo + count, :], gu[:, columns], preferred_element_type=F32)
        for n in range(n_pairs):
            a, b = r[:, 2 * n * LANES : (2 * n + 1) * LANES], r[:, (2 * n + 1) * LANES : (2 * n + 2) * LANES]
            hid[lo : lo + count, n * LANES : (n + 1) * LANES] = gate_up(a, b)

    my_half = pl.ds(pl.multiple_of(mine * 2 * units, LANES), 2 * units)

    def pair_sum(s, lo, count):
        up = lax.rem(z + s, 2) == 1
        f = jnp.where(up, lax.rem(z + s - 1, n_fs), lax.rem(z + n_fs - s, n_fs))
        ks = pl.ds(pl.multiple_of(f // 2 * (2 * k_rows), 2 * k_rows), 2 * k_rows)
        return jnp.dot(ub[lo : lo + count, ks], gu[ks, my_half], preferred_element_type=F32)

    def gather_pair(s, lo, count):
        r = pair_sum(s, lo, count)
        part[lo : lo + count, :] = r if s == 1 else part[lo : lo + count, :] + r

    def last_pair(lo, count):
        r = part[lo : lo + count, :] + pair_sum(steps, lo, count)
        for n in range(pairs):
            a, b = r[:, 2 * n * LANES : (2 * n + 1) * LANES], r[:, (2 * n + 1) * LANES : (2 * n + 2) * LANES]
            hid[lo : lo + count, n * LANES : (n + 1) * LANES] = gate_up(a, b)

    def conv(q):
        r = jnp.dot(ub[q * rows : (q + 1) * rows, :], vm[:, : 2 * chan_w], preferred_element_type=F32)
        glued = r[:, :chan_w] * jax.nn.sigmoid(r[:, chan_w:])
        for i in range(rows // LEN):
            pad[i, 32:, :] = glued[i * LEN : (i + 1) * LEN]
        n_taps = taps_in.shape[0]
        taps = taps_in[...].astype(F32)
        for i in range(rows // LEN):
            total = jnp.zeros((LEN, chan_w), F32)
            for k in range(n_taps):
                total = total + taps[k : k + 1, :] * pad[i, 33 - n_taps + k : 33 - n_taps + k + LEN, :]
            cvb[q, i * LEN : (i + 1) * LEN, pl.ds(pl.multiple_of(t * chan_w, chan_w), chan_w)] = total.astype(BF16)

    def channel_norm(q):
        @pl.loop(0, rows // 16, unroll=4)
        def _(i):
            rws = pl.ds(pl.multiple_of(i * 16, 16), 16)
            v = cvb[q, rws, :].astype(F32)
            mu = jnp.sum(v, axis=1, keepdims=True) / chan
            msq = jnp.sum(v * v, axis=1, keepdims=True) / chan
            w = (v - mu) * lax.rsqrt(msq - mu * mu + EPS) * cgb[3:4, :] + cgb[11:12, :]
            mixed[rws, :] = jax.nn.silu(w).astype(BF16)

    def own_cols(buf, q):
        return buf[q, :, own_w]

    def z_begin(kinds):
        for kind in kinds:
            for way in range(2):
                z_copy(kind, way, 1).start()

    def relays(kinds, s):
        for kind in kinds:
            relay(kind, s)

    first_kinds = (A0, A1, B)

    def phase(name):
        return jax.named_scope(name)

    chunks = range(nq)
    z_begin(first_kinds)
    for q in chunks:
        stream_copy(q).start()
    ag_start(0, sb0, width, nq)

    def pk_copy(i):
        return remote(pk.at[t], pk.at[t], pk_send.at[0], pk_recv.at[0], {"tp": lax.rem(t + i, n_tp)})

    pk_all = remote(pk.at[0 : n_tp - 1], pk.at[0 : n_tp - 1], pk_send.at[0], pk_recv.at[0], sib)

    for i in range(1, n_tp):
        pk_copy(i).start()
    spread_mix(z)
    pad[:, :32, :] = jnp.zeros((pad.shape[0], 32, chan_w), F32)

    with phase("w1"):
        relays(first_kinds, 1)
    with phase("ag0"):
        ref = sb0.at[0:nq, :, 0:width]
        remote(ref, ref, yx_send.at[0], yx_recv.at[nq], partner).wait_recv()
        ag_start(0, sb0, width, 0)
        ag_relay(0, sb0, width, nq)
    with phase("w2"):
        relays(first_kinds, 2)
    ag_relay(0, sb0, width, 0)
    ag_opposite(0, sb0, width, nq)
    with phase("w3"):
        relays(first_kinds, 3)
    ag_opposite(0, sb0, width, 0)
    ag_end(0, sb0, width, nq)
    pk_all.wait_recv()
    for b in range(n_tp):
        gf[:, b * width : (b + 1) * width] = pk[b]
        cgb[0:8, b * chan_w : (b + 1) * chan_w] = pk[b][:, :chan_w]
        cgb[8:16, b * chan_w : (b + 1) * chan_w] = pk[b][:, chan_w : 2 * chan_w]
    tokens = nq * rows
    pl.loop(nq, 2 * nq)(lambda q: norm_rows(sb0, q, 0, q * rows))
    with phase("w4"):
        relays(first_kinds, 4)
    ag_end(0, sb0, width, 0)
    pl.loop(0, nq)(lambda q: norm_rows(sb0, q, 0, q * rows))

    def relay_and_sum(s, work):
        for kind, some in zip(first_kinds, work):
            relay(kind, s)
            for i, lo in some:
                gather_pair(i, lo, tokens)

    with phase("w5"):
        relay_and_sum(5, (((1, 0),), ((1, tokens),), ((2, 0), (2, tokens))))
    with phase("w6"):
        relay_and_sum(6, (((3, 0),), ((3, tokens),), ((4, 0), (4, tokens))))
    with phase("w7"):
        relay_and_sum(7, (((5, 0),), ((5, tokens), (6, 0)), ((6, tokens), (7, 0), (7, tokens))))
    leap_send(X, 1)
    with phase("w8"):
        relays((A0, A1), 8)

    def late(*steps_of):
        with phase("late"):
            for kind, i in steps_of:
                leap(kind, i)

    def y_late(lo, hi):
        @pl.loop(lo, hi)
        def _(i):
            y_copy(piece(A1, lax.rem(z + i, n_fs)), 1).start()

    with phase("hid_theirs"):
        last_pair(0, tokens)
    with phase("w8b"):
        relay(B, 8)
    with phase("part_theirs"):
        for q in chunks:
            rs_partials(0, q)
    late((X, 1))
    y_late(1, 5)
    with phase("hid_ours"):
        last_pair(tokens, tokens)
    with phase("rs_a"):
        rs_opposite(0, 0)
        rs_opposite(0, 1)
        rs_partials(0, nq)
        rs_opposite(0, 2)
        rs_neighbours(0, 0)
        rs_partials(0, nq + 1)
    late((X, 2))
    leap_send(M, 1)

    def pass_over(q):
        ybo[q] = rs_total(0, q).astype(BF16)
        part_copy(q).start()

    with phase("rs_b"):
        rs_neighbours(0, 1)
        rs_partials(0, nq + 2)
        rs_neighbours(0, 2)
        rs_opposite(0, 3)
    with phase("rs_c"):
        pass_over(0)
        rs_opposite(0, 4)
        pass_over(1)
        rs_neighbours(0, 3)
        rs_opposite(0, 5)
        pass_over(2)
    late((X, 3), (M, 1))
    with phase("rs_d"):
        rs_neighbours(0, 4)
        rs_neighbours(0, 5)

    def first(q):
        total = rs_total(0, nq + q)
        part_copy(q).wait_recv()
        sb1[q, :, own_w] = (own_cols(sb0, nq + q).astype(F32) + 0.5 * (total + ybi[q].astype(F32))).astype(BF16)
        ag_start(1, sb1, width, q)

    with phase("first0"):
        first(0)
    late((X, 4))
    leap_send(D, 1)
    with phase("first12"):
        first(1)
        first(2)
    late((M, 2), (D, 1))
    y_late(5, n_fs)
    with phase("ag1"):
        ag_relay(1, sb1, width, 0)
        ag_relay(1, sb1, width, 1)
        ag_relay(1, sb1, width, 2)
    with phase("opp1"):
        ag_opposite(1, sb1, width, 0)
        ag_opposite(1, sb1, width, 1)
    late((M, 3), (D, 2))

    def conv_stage(q):
        ag_end(1, sb1, width, q)
        norm_rows(sb1, q, 1, q * rows)
        conv(q)
        ag_start(2, cvb, chan_w, q)

    with phase("ywaitx"):
        y_all(2).wait_recv()
    with phase("conv0"):
        conv_stage(0)
    with phase("conv1"):
        ag_opposite(1, sb1, width, 2)
        conv_stage(1)
    late((M, 4))
    with phase("conv2"):
        ag_relay(2, cvb, chan_w, 0)
        conv_stage(2)
    late((D, 3))
    with phase("ag2"):
        ag_relay(2, cvb, chan_w, 1)
        ag_opposite(2, cvb, chan_w, 0)
        ag_relay(2, cvb, chan_w, 2)
        ag_opposite(2, cvb, chan_w, 1)

    def mix_stage(q):
        ag_end(2, cvb, chan_w, q)
        channel_norm(q)
        branch = jnp.dot(mixed[...], mxb[...], preferred_element_type=F32)
        sb3[q, :, own_w] = (own_cols(sb1, q).astype(F32) + branch).astype(BF16)
        ag_start(3, sb3, width, q)

    with phase("mixw"):
        pltpu.make_async_copy(mxb, mxb, mx_recv.at[0]).wait()
    with phase("mix0"):
        mix_stage(0)
    with phase("mix12"):
        ag_opposite(2, cvb, chan_w, 2)
        mix_stage(1)
        ag_relay(3, sb3, width, 0)
        mix_stage(2)
    late((D, 4))
    with phase("ag3"):
        ag_relay(3, sb3, width, 1)
        ag_opposite(3, sb3, width, 0)
        ag_relay(3, sb3, width, 2)
        ag_opposite(3, sb3, width, 1)
    with phase("ywait"):
        for i in range(2):
            y_all(i).wait_recv()

    def ffn_stage(q):
        ag_end(3, sb3, width, q)
        norm_rows(sb3, q, 2, q * rows)
        hidden_rows(q * rows, rows, slice(None), 2 * pairs)
        rs_partials(1, q)

    def last(q):
        total = rs_total(1, q)
        out[q * rows : (q + 1) * rows, :] = (own_cols(sb3, q).astype(F32) + 0.5 * total).astype(BF16)

    with phase("ffn0"):
        ffn_stage(0)
    with phase("ffn1"):
        ag_opposite(3, sb3, width, 2)
        ffn_stage(1)
    with phase("ffn2"):
        rs_opposite(1, 0)
        ffn_stage(2)
    with phase("rs1"):
        rs_opposite(1, 1)
        rs_neighbours(1, 0)
        rs_opposite(1, 2)
        rs_neighbours(1, 1)
    with phase("last"):
        last(0)
        rs_neighbours(1, 2)
        last(1)
        last(2)

    for kind in range(6):
        ref = many(kind, n_fs - 1)
        remote(ref, ref, z_send.at[kind], z_recv.at[0], z_right).wait_send()
    for i in range(3):
        y_all(i).wait_send()
    pk_all.wait_send()
    ref = mxb.at[pl.ds(0, (n_tp - 1) * chan_w), :]
    remote(ref, ref, mx_send.at[0], mx_recv.at[0], sib).wait_send()
    ref = sb0.at[0:nq, :, 0:width]
    remote(ref, ref, yx_send.at[0], yx_recv.at[0], partner).wait_send()
    remote(ybo, ybo, yx_send.at[1], yx_recv.at[0], partner).wait_send()
    for n, buf, w in ((0, sb0, width), (1, sb1, width), (2, cvb, chan_w), (3, sb3, width)):
        ag_drain(n, buf, w)
    for n in range(2):
        rs_drain(n)


def solution(mesh):
    n_fs, n_tp = mesh.shape["fs"], mesh.shape["tp"]

    def local(
        stream_in,
        gain_before,
        gain_mixer,
        gain_after,
        w_gate,
        w_upward,
        w_down,
        w_value,
        w_glu_gate,
        conv_taps,
        chan_gain,
        chan_bias,
        w_mix_out,
    ):
        tokens, width = stream_in.shape
        k_rows, hidden = w_gate.shape
        chan_w = w_value.shape[1]
        units = -(-(hidden // 2) // LANES) * LANES
        nq = CHUNKS
        rows = tokens // nq
        feat, chan = width * n_tp, chan_w * n_tp
        vmem = pltpu.VMEM
        dma = pltpu.SemaphoreType.DMA
        any_space = pl.BlockSpec(memory_space=pl.ANY)
        in_vmem = pl.BlockSpec(memory_space=pltpu.VMEM)
        return pl.pallas_call(
            lambda *refs: layer_kernel(n_fs, n_tp, *refs),
            out_shape=jax.ShapeDtypeStruct((tokens, width), BF16),
            in_specs=[any_space, in_vmem, in_vmem] + [any_space] * 4 + [in_vmem] * 6,
            out_specs=in_vmem,
            scratch_shapes=[
                vmem((n_fs * k_rows, 4 * units), BF16),
                vmem((n_fs // 2, 2 * units, 2 * LANES), BF16),
                vmem((n_fs * k_rows, 3 * chan_w), BF16),
                vmem((chan, 2 * LANES), BF16),
                vmem((n_tp, 8, width), F32),
                vmem((8, feat), F32),
                vmem((16, chan), F32),
                vmem((2 * nq, rows, feat), BF16),
                vmem((nq, rows, feat), BF16),
                vmem((nq, rows, feat), BF16),
                vmem((nq, rows, chan), BF16),
                vmem((2 * tokens, feat), BF16),
                vmem((rows, chan), BF16),
                vmem((2 * tokens, 2 * units), BF16),
                vmem((rows // LEN, LEN + 32, chan_w), F32),
                vmem((nq, rows, width), BF16),
                vmem((nq, rows, width), BF16),
                vmem((2 * nq, 4, rows, width), F32),
                vmem((2 * nq, 14, rows, width), BF16),
                vmem((nq, 14, rows, width), BF16),
                dma((3,)),
                dma((6 * (n_fs // 2) + 3 * (n_fs // 4),)),
                dma((6,)),
                dma((3,)),
                dma((3,)),
                dma((1,)),
                dma((1,)),
                dma((1,)),
                dma((1,)),
                dma((2 + 3 * nq, 3)),
                dma((4,)),
                dma((3 * nq, 3)),
                dma((2,)),
                dma((nq + 1,)),
                dma((2,)),
                vmem((2 * tokens, 2 * units), F32),
            ],
            compiler_params=pltpu.CompilerParams(
                collective_id=0, has_side_effects=True, vmem_limit_bytes=60 * 1024 * 1024
            ),
        )(
            stream_in,
            w_gate.T,
            w_upward.T,
            w_down,
            w_value,
            w_glu_gate,
            w_mix_out,
            conv_taps,
            gain_before,
            gain_mixer,
            gain_after,
            chan_gain,
            chan_bias,
        )

    in_specs = (
        P(("grp", "fs"), "tp"),
        P("tp"),
        P("tp"),
        P("tp"),
        P("fs", "tp"),
        P("fs", "tp"),
        P("tp", "fs"),
        P("fs", "tp"),
        P("fs", "tp"),
        P(None, "tp"),
        P("tp"),
        P("tp"),
        P("tp", "fs"),
    )
    out_specs = P(("grp", "fs"), "tp")
    return jax.shard_map(local, mesh=mesh, in_specs=in_specs, out_specs=out_specs, check_vma=False)
```

```python
import jax
import jax.numpy as jnp
from jax import lax
from jax.experimental import pallas as pl
from jax.experimental.pallas import tpu as pltpu
from jax.sharding import PartitionSpec as P

MESH = pl.DeviceIdType.MESH
LEN = 128
EPS = 1e-06
LANES = 128
CHUNKS = 3
BF16, F32 = jnp.bfloat16, jnp.float32


def remote(src, dst, send_sem, recv_sem, where):
    return pltpu.make_async_remote_copy(
        src_ref=src,
        dst_ref=dst,
        send_sem=send_sem,
        recv_sem=recv_sem,
        device_id=where,
        device_id_type=MESH,
    )


def layer_kernel(
    n_fs,
    n_tp,
    s_in,
    gate_in,
    up_in,
    wd_in,
    value_in,
    glu_in,
    mix_in,
    taps_in,
    before_in,
    mixer_in,
    after_in,
    cgain_in,
    cbias_in,
    out,
    gu,
    wd,
    vm,
    mxb,
    pk,
    gf,
    cgb,
    sb0,
    sb1,
    sb3,
    cvb,
    ub,
    mixed,
    hid,
    pad,
    ybo,
    ybi,
    acc,
    rs0,
    rs1,
    load_sem,
    z_recv,
    z_send,
    y_recv,
    y_send,
    pk_recv,
    pk_send,
    mx_recv,
    mx_send,
    ag_recv,
    ag_send,
    rs_recv,
    rs_send,
    yx_recv,
    yx_send,
    part,
):
    z, t, g = lax.axis_index("fs"), lax.axis_index("tp"), lax.axis_index("grp")
    parity = lax.rem(g, 2)
    partner = {"grp": g + 1 - 2 * parity}
    z_right = {"fs": lax.rem(z + 1, n_fs)}
    z_left = {"fs": lax.rem(z + n_fs - 1, n_fs)}
    z_two = ({"fs": lax.rem(z + 2, n_fs)}, {"fs": lax.rem(z + n_fs - 2, n_fs)})
    chips = n_tp // 2
    x, core = t // 2, lax.rem(t, 2)
    xr, xl, xo = lax.rem(x + 1, chips), lax.rem(x + 3, chips), lax.rem(x + 2, chips)
    other = 1 - core
    sib = {"tp": 2 * x + other}
    x_right, x_left = {"tp": 2 * xr + core}, {"tp": 2 * xl + core}

    nq, rows, width = sb1.shape[0], sb1.shape[1], s_in.shape[1]
    half = rows // 2
    feat = width * n_tp
    k_rows, chan_w = value_in.shape
    chan = chan_w * n_tp
    steps = n_fs // 2
    own_units = gate_in.shape[0] // 2
    units = wd.shape[1] // 2
    pairs = units // LANES
    mine, theirs = parity, 1 - parity

    own_k = pl.ds(pl.multiple_of(z * k_rows, k_rows), k_rows)

    own_w = pl.ds(pl.multiple_of(t * width, width), width)

    def own_loads():
        for h in range(2):
            yield pltpu.make_async_copy(
                wd_in.at[h * own_units : (h + 1) * own_units, :],
                wd.at[
                    z // 2,
                    h * units : h * units + own_units,
                    pl.ds(pl.multiple_of(lax.rem(z, 2) * LANES, LANES), LANES),
                ],
                load_sem.at[0],
            )
        for i, ref in enumerate((value_in, glu_in, mix_in)):
            yield pltpu.make_async_copy(ref, vm.at[own_k, i * chan_w : (i + 1) * chan_w], load_sem.at[1])
        for q in range(nq):
            yield pltpu.make_async_copy(
                s_in.at[pl.ds(q * rows, rows), :],
                sb0.at[nq + q, :, pl.ds(pl.multiple_of(t * width, width), width)],
                load_sem.at[2],
            )

    for copy in own_loads():
        copy.start()

    for h in range(2):
        for i in range(pairs):
            lo = h * own_units + i * LANES
            hi = min(lo + LANES, (h + 1) * own_units)
            for j, ref in enumerate((gate_in, up_in)):
                v = ref[lo:hi, :]
                if hi - lo < LANES:
                    v = jnp.concatenate([v, jnp.zeros((LANES - hi + lo, k_rows), BF16)], axis=0)
                c = h * 2 * units + (2 * i + j) * LANES
                gu[own_k, c : c + LANES] = v.T
        wd[:, h * units + own_units : (h + 1) * units, :] = jnp.zeros((wd.shape[0], units - own_units, wd.shape[2]), BF16)
    for i, ref in enumerate((before_in, mixer_in, after_in)):
        pk[t, i : i + 1, :] = ref[...].astype(F32).reshape(1, width)
    pk[t, 3:4, :chan_w] = cgain_in[...].astype(F32).reshape(1, chan_w)
    pk[t, 3:4, chan_w:] = cbias_in[...].astype(F32).reshape(1, chan_w)
    pk[t, 4:8, :] = jnp.zeros((4, width), F32)

    barrier = pltpu.get_barrier_semaphore()
    peers = [z_right, z_left, *z_two, partner] + [{"tp": lax.rem(t + i, n_tp)} for i in range(1, n_tp)]
    for peer in peers:
        pl.semaphore_signal(barrier, inc=1, device_id=peer, device_id_type=MESH)
    pl.semaphore_wait(barrier, len(peers))

    ref = vm.at[own_k, :]
    pltpu.make_async_copy(wd_in, wd_in, load_sem.at[0]).wait()
    pltpu.make_async_copy(ref, ref, load_sem.at[1]).wait()
    pltpu.make_async_copy(s_in, s_in, load_sem.at[2]).wait()

    wide = 2 * LANES * (pairs - 1)
    A0, A1, B, X, M, D = range(6)

    def piece(kind, f, part=None):
        if kind in (B, D):
            size = own_units if part is None else own_units // 2
            q0 = (mine if kind == B else theirs) * units + (0 if part is None else part * size)
            return wd.at[
                f // 2,
                pl.ds(pl.multiple_of(q0, 16), size),
                pl.ds(pl.multiple_of(lax.rem(f, 2) * LANES, LANES), LANES),
            ]
        size = k_rows if part is None else k_rows // 2
        r0 = pl.ds(pl.multiple_of(f * k_rows + (0 if part is None else part * size), size), size)
        c0 = mine * 2 * units
        if kind == A0:
            return gu.at[r0, pl.ds(pl.multiple_of(c0, LANES), wide)]
        if kind == A1:
            return gu.at[r0, pl.ds(pl.multiple_of(c0 + wide, LANES), 2 * units - wide)]
        if kind == X:
            return vm.at[r0, pl.ds(pl.multiple_of(mine * chan_w, LANES), chan_w)]
        return vm.at[r0, 2 * chan_w : 3 * chan_w]

    def many(kind, count):
        if kind in (B, D):
            if count <= wd.shape[0]:
                return wd.at[0:count, 0:own_units, 0:LANES]
            total = count * own_units // 2
            for a in range(1, wd.shape[0] + 1):
                if total % (16 * a) == 0 and total // a <= wd.shape[1]:
                    return wd.at[0:a, 0 : total // a, :]
        if kind == A0:
            return gu.at[0 : count * k_rows, 0:wide]
        if kind == A1:
            return gu.at[0 : count * k_rows, 0 : 2 * units - wide]
        return vm.at[0 : count * k_rows, 0:chan_w]

    def origin(way, s):
        return lax.rem(z + n_fs - s, n_fs) if way == 0 else lax.rem(z + s, n_fs)

    def z_sem(kind, way, s):
        return z_recv.at[(kind * 2 + way) * steps + s - 1]

    def z_copy(kind, way, s_next):
        ref = piece(kind, origin(way, s_next - 1), None if s_next < steps else way)
        return remote(ref, ref, z_send.at[kind], z_sem(kind, way, s_next), z_right if way == 0 else z_left)

    def y_copy(ref, i):
        return remote(ref, ref, y_send.at[i], y_recv.at[i], partner)

    def y_all(i):
        return y_copy(many((A0, A1, X)[i], n_fs - 1), i)

    def stream_copy(q):
        return remote(sb0.at[nq + q, :, own_w], sb0.at[q, :, own_w], yx_send.at[0], yx_recv.at[nq], partner)

    def part_copy(q):
        return remote(ybo.at[q], ybi.at[q], yx_send.at[1], yx_recv.at[q], partner)

    def spread_mix(f):
        dest, b = f // 2, lax.rem(f, 2)
        src = piece(M, f)
        dst = mxb.at[
            pl.ds(pl.multiple_of(t * chan_w, chan_w), chan_w), pl.ds(pl.multiple_of(b * LANES, LANES), LANES)
        ]

        @pl.when(dest != t)
        def _():
            remote(src, dst, mx_send.at[0], mx_recv.at[0], {"tp": dest}).start()

        @pl.when(dest == t)
        def _():
            pltpu.make_async_copy(src, dst, mx_recv.at[0]).start()

    def relay(kind, s):
        for way in range(2):
            part = None if s < steps else way
            ref = piece(kind, origin(way, s), part)
            remote(ref, ref, z_send.at[kind], z_sem(kind, way, s), z_right).wait_recv()
            if s < steps:
                z_copy(kind, way, s + 1).start()
            if kind == A0:
                y_copy(ref, 0).start()

    def leap_sem(kind, k):
        return z_recv.at[2 * X * steps + (kind - X) * (steps // 2) + k - 1]

    def leap_send(kind, k):
        for far in (True, False):
            for way in range(2):
                part = way if far and 2 * k == steps else None
                ref = piece(kind, origin(way, 2 * k - 2), part)
                where = z_two[way] if far else (z_right, z_left)[way]
                remote(ref, ref, z_send.at[kind], leap_sem(kind, k), where).start()

    def leap(kind, k):
        ref = many(kind, 4 if 2 * k < steps else 3)
        remote(ref, ref, z_send.at[kind], leap_sem(kind, k), z_right).wait_recv()
        if 2 * k < steps:
            leap_send(kind, k + 1)
        for way, d in ((0, 2 * k), (1, 2 * k), (0, 2 * k - 1), (1, 2 * k - 1)):
            if d == steps and way == 1:
                continue
            if kind == X:
                y_copy(piece(X, origin(way, d)), 2).start()
            if kind == M:
                spread_mix(origin(way, d))

    def block(buf, w, q, b, part=None):
        rws = slice(None) if part is None else pl.ds(part * half, half)
        return buf.at[q, rws, pl.ds(pl.multiple_of(b * w, w), w)]

    def ag_copy(n, ref, slot, i, where):
        return remote(ref, ref, ag_send.at[n], ag_recv.at[slot, i], where)

    def ag_slot(n, q):
        return q // nq if n == 0 else 2 + (n - 1) * nq + q

    def ag_chunks(n, q):
        return slice(q, q + nq) if n == 0 else q

    def ag_start(n, buf, w, q):
        slot, own = ag_slot(n, q), block(buf, w, ag_chunks(n, q), t)
        ag_copy(n, own, slot, 0, x_right).start()
        ag_copy(n, own, slot, 0, x_left).start()
        ag_copy(n, own, slot, 2, sib).start()

    def ag_wait(n, buf, w, q, i, count):
        ag_copy(n, buf.at[ag_chunks(n, q), :, 0 : count * w], ag_slot(n, q), i, sib).wait_recv()

    def ag_relay(n, buf, w, q):
        slot, c = ag_slot(n, q), ag_chunks(n, q)
        b_l, b_r = 2 * xl + core, 2 * xr + core
        ag_wait(n, buf, w, q, 0, 2)
        ag_copy(n, block(buf, w, c, b_l, 0), slot, 1, x_right).start()
        ag_copy(n, block(buf, w, c, b_r, 1), slot, 1, x_left).start()
        ag_copy(n, block(buf, w, c, b_l), slot, 2, sib).start()
        ag_copy(n, block(buf, w, c, b_r), slot, 2, sib).start()

    def ag_opposite(n, buf, w, q):
        ag_wait(n, buf, w, q, 1, 1)
        ag_copy(n, block(buf, w, ag_chunks(n, q), 2 * xo + core), ag_slot(n, q), 2, sib).start()

    def ag_end(n, buf, w, q):
        ag_wait(n, buf, w, q, 2, 4)

    def ag_drain(n, buf, w):
        ag_copy(n, buf.at[:, :, 0 : 7 * w], 0, 0, sib).wait_send()

    order = (xo, xr, xl, x)
    rs_refs = (rs0, rs1)

    def rs_copy(src, dst, n, q, i, where):
        return remote(
            rs_refs[n].at[(q, *src)], rs_refs[n].at[(q, *dst)], rs_send.at[n], rs_recv.at[2 * nq * n + q, i], where
        )

    def sib_copy(n, q):
        return rs_copy((slice(0, 4),), (slice(4, 8),), n, q, 0, sib)

    def opp_copy(n, q, i):
        part = pl.ds(i * half, half)
        return rs_copy((8, part), (9, part), n, q, 1, x_right if i == 0 else x_left)

    def nb_copy(n, q, i):
        return rs_copy((10 + i,), (12 + i,), n, q, 2, x_right if i == 0 else x_left)

    def rs_partials(n, q):
        buf = rs_refs[n]
        width_k = units if n == 0 else 2 * units
        k_range = pl.ds(pl.multiple_of(mine * units, LANES), units) if n == 0 else slice(None)
        h = hid[q * rows : (q + 1) * rows, 0:width_k]
        for k in range(4):
            buf[q, k] = jnp.dot(h, wd[2 * order[k] + other, k_range, :], preferred_element_type=F32).astype(BF16)
        sib_copy(n, q).start()
        for k in range(4):
            acc[q, k] = jnp.dot(h, wd[2 * order[k] + core, k_range, :], preferred_element_type=F32)

    def rs_opposite(n, q):
        buf = rs_refs[n]
        sib_copy(n, q).wait_recv()
        buf[q, 8] = (acc[q, 0] + buf[q, 4].astype(F32)).astype(BF16)
        opp_copy(n, q, 0).start()
        opp_copy(n, q, 1).start()

    def rs_neighbours(n, q):
        buf = rs_refs[n]
        rs_copy((9,), (9,), n, q, 1, sib).wait_recv()
        for i in range(2):
            near, far = pl.ds(i * half, half), pl.ds((1 - i) * half, half)
            buf[q, 10 + i, near] = (
                acc[q, 1 + i, near] + buf[q, 5 + i, near].astype(F32) + buf[q, 9, near].astype(F32)
            ).astype(BF16)
            buf[q, 10 + i, far] = (acc[q, 1 + i, far] + buf[q, 5 + i, far].astype(F32)).astype(BF16)
            nb_copy(n, q, i).start()

    def rs_total(n, q):
        buf = rs_refs[n]
        rs_copy((slice(12, 14),), (slice(12, 14),), n, q, 2, sib).wait_recv()
        return acc[q, 3] + buf[q, 7].astype(F32) + buf[q, 12].astype(F32) + buf[q, 13].astype(F32)

    def rs_drain(n):
        ref = rs_refs[n].at[:, 0:7]
        remote(ref, ref, rs_send.at[n], rs_recv.at[0, 0], sib).wait_send()

    def norm_rows(buf, q, r, base):
        @pl.loop(0, rows // 16, unroll=4)
        def _(i):
            rws = pl.ds(pl.multiple_of(i * 16, 16), 16)
            v = buf[q, rws, :].astype(F32)
            inverse = lax.rsqrt(jnp.sum(v * v, axis=1, keepdims=True) / feat + EPS)
            ub[pl.ds(pl.multiple_of(base + i * 16, 16), 16), :] = (v * inverse * gf[r : r + 1, :]).astype(BF16)

    def gate_up(a, b):
        return (jax.nn.silu(a) * b).astype(BF16)

    def hidden_rows(lo, count, columns, n_pairs):
        r = jnp.dot(ub[lo : lo + count, :], gu[:, columns], preferred_element_type=F32)
        for n in range(n_pairs):
            a, b = r[:, 2 * n * LANES : (2 * n + 1) * LANES], r[:, (2 * n + 1) * LANES : (2 * n + 2) * LANES]
            hid[lo : lo + count, n * LANES : (n + 1) * LANES] = gate_up(a, b)

    my_half = pl.ds(pl.multiple_of(mine * 2 * units, LANES), 2 * units)

    def pair_sum(s, lo, count):
        up = lax.rem(z + s, 2) == 1
        f = jnp.where(up, lax.rem(z + s - 1, n_fs), lax.rem(z + n_fs - s, n_fs))
        ks = pl.ds(pl.multiple_of(f // 2 * (2 * k_rows), 2 * k_rows), 2 * k_rows)
        return jnp.dot(ub[lo : lo + count, ks], gu[ks, my_half], preferred_element_type=F32)

    def gather_pair(s, lo, count):
        r = pair_sum(s, lo, count)
        part[lo : lo + count, :] = r if s == 1 else part[lo : lo + count, :] + r

    def last_pair(lo, count):
        r = part[lo : lo + count, :] + pair_sum(steps, lo, count)
        for n in range(pairs):
            a, b = r[:, 2 * n * LANES : (2 * n + 1) * LANES], r[:, (2 * n + 1) * LANES : (2 * n + 2) * LANES]
            hid[lo : lo + count, n * LANES : (n + 1) * LANES] = gate_up(a, b)

    def conv(q):
        r = jnp.dot(ub[q * rows : (q + 1) * rows, :], vm[:, : 2 * chan_w], preferred_element_type=F32)
        glued = r[:, :chan_w] * jax.nn.sigmoid(r[:, chan_w:])
        for i in range(rows // LEN):
            pad[i, 32:, :] = glued[i * LEN : (i + 1) * LEN]
        n_taps = taps_in.shape[0]
        taps = taps_in[...].astype(F32)
        for i in range(rows // LEN):
            total = jnp.zeros((LEN, chan_w), F32)
            for k in range(n_taps):
                total = total + taps[k : k + 1, :] * pad[i, 33 - n_taps + k : 33 - n_taps + k + LEN, :]
            cvb[q, i * LEN : (i + 1) * LEN, pl.ds(pl.multiple_of(t * chan_w, chan_w), chan_w)] = total.astype(BF16)

    def channel_norm(q):
        @pl.loop(0, rows // 16, unroll=4)
        def _(i):
            rws = pl.ds(pl.multiple_of(i * 16, 16), 16)
            v = cvb[q, rws, :].astype(F32)
            mu = jnp.sum(v, axis=1, keepdims=True) / chan
            msq = jnp.sum(v * v, axis=1, keepdims=True) / chan
            w = (v - mu) * lax.rsqrt(msq - mu * mu + EPS) * cgb[3:4, :] + cgb[11:12, :]
            mixed[rws, :] = jax.nn.silu(w).astype(BF16)

    def own_cols(buf, q):
        return buf[q, :, own_w]

    def z_begin(kinds):
        for kind in kinds:
            for way in range(2):
                z_copy(kind, way, 1).start()

    def relays(kinds, s):
        for kind in kinds:
            relay(kind, s)

    first_kinds = (A0, A1, B)

    def phase(name):
        return jax.named_scope(name)

    chunks = range(nq)
    z_begin(first_kinds)
    for q in chunks:
        stream_copy(q).start()
    ag_start(0, sb0, width, nq)

    def pk_copy(i):
        return remote(pk.at[t], pk.at[t], pk_send.at[0], pk_recv.at[0], {"tp": lax.rem(t + i, n_tp)})

    pk_all = remote(pk.at[0 : n_tp - 1], pk.at[0 : n_tp - 1], pk_send.at[0], pk_recv.at[0], sib)

    for i in range(1, n_tp):
        pk_copy(i).start()
    spread_mix(z)
    pad[:, :32, :] = jnp.zeros((pad.shape[0], 32, chan_w), F32)

    with phase("w1"):
        relays(first_kinds, 1)
    with phase("ag0"):
        ref = sb0.at[0:nq, :, 0:width]
        remote(ref, ref, yx_send.at[0], yx_recv.at[nq], partner).wait_recv()
        ag_start(0, sb0, width, 0)
        ag_relay(0, sb0, width, nq)
    with phase("w2"):
        relays(first_kinds, 2)
    ag_relay(0, sb0, width, 0)
    ag_opposite(0, sb0, width, nq)
    with phase("w3"):
        relays(first_kinds, 3)
    ag_opposite(0, sb0, width, 0)
    ag_end(0, sb0, width, nq)
    pk_all.wait_recv()
    for b in range(n_tp):
        gf[:, b * width : (b + 1) * width] = pk[b]
        cgb[0:8, b * chan_w : (b + 1) * chan_w] = pk[b][:, :chan_w]
        cgb[8:16, b * chan_w : (b + 1) * chan_w] = pk[b][:, chan_w : 2 * chan_w]
    tokens = nq * rows
    pl.loop(nq, 2 * nq)(lambda q: norm_rows(sb0, q, 0, q * rows))
    with phase("w4"):
        relays(first_kinds, 4)
    ag_end(0, sb0, width, 0)
    pl.loop(0, nq)(lambda q: norm_rows(sb0, q, 0, q * rows))

    def relay_and_sum(s, work):
        for kind, some in zip(first_kinds, work):
            relay(kind, s)
            for i, lo in some:
                gather_pair(i, lo, tokens)

    with phase("w5"):
        relay_and_sum(5, (((1, 0),), ((1, tokens),), ((2, 0), (2, tokens))))
    with phase("w6"):
        relay_and_sum(6, (((3, 0),), ((3, tokens),), ((4, 0), (4, tokens))))
    with phase("w7"):
        relay_and_sum(7, (((5, 0),), ((5, tokens), (6, 0)), ((6, tokens), (7, 0), (7, tokens))))
    leap_send(X, 1)
    with phase("w8"):
        relays((A0, A1), 8)

    def late(*steps_of):
        with phase("late"):
            for kind, i in steps_of:
                leap(kind, i)

    def y_late(lo, hi):
        @pl.loop(lo, hi)
        def _(i):
            y_copy(piece(A1, lax.rem(z + i, n_fs)), 1).start()

    with phase("hid_theirs"):
        last_pair(0, tokens)
    with phase("w8b"):
        relay(B, 8)
    with phase("part_theirs"):
        for q in chunks:
            rs_partials(0, q)
    with phase("hid_ours"):
        last_pair(tokens, tokens)
    late((X, 1))
    leap_send(M, 1)
    y_late(1, 5)

    def pass_over(q):
        ybo[q] = rs_total(0, q).astype(BF16)
        part_copy(q).start()

    def first(q):
        total = rs_total(0, nq + q)
        part_copy(q).wait_recv()
        sb1[q, :, own_w] = (own_cols(sb0, nq + q).astype(F32) + 0.5 * (total + ybi[q].astype(F32))).astype(BF16)
        ag_start(1, sb1, width, q)

    with phase("rs_a"):
        for q in chunks:
            rs_opposite(0, q)
            rs_partials(0, nq + q)
        for q in chunks:
            rs_opposite(0, nq + q)
    with phase("rs_b"):
        rs_neighbours(0, 0)
    late((X, 2), (M, 1))
    leap_send(D, 1)
    with phase("rs_c"):
        rs_neighbours(0, 1)
        rs_neighbours(0, 2)
        rs_neighbours(0, nq)
        pass_over(0)
        rs_neighbours(0, nq + 1)
        pass_over(1)
    late((X, 3), (M, 2))
    with phase("rs_d"):
        rs_neighbours(0, nq + 2)
        pass_over(2)
    with phase("first"):
        for q in chunks:
            first(q)
    late((X, 4), (M, 3), (D, 1))
    y_late(5, n_fs)
    with phase("ag1"):
        for q in chunks:
            ag_relay(1, sb1, width, q)
    late((M, 4))
    with phase("opp1"):
        ag_opposite(1, sb1, width, 0)
        ag_opposite(1, sb1, width, 1)

    def conv_stage(q):
        ag_end(1, sb1, width, q)
        norm_rows(sb1, q, 1, q * rows)
        conv(q)
        ag_start(2, cvb, chan_w, q)

    with phase("ywaitx"):
        y_all(2).wait_recv()
    with phase("conv0"):
        conv_stage(0)
    with phase("conv12"):
        ag_opposite(1, sb1, width, 2)
        conv_stage(1)
        conv_stage(2)
    late((D, 2))
    with phase("ag2"):
        for q in chunks:
            ag_relay(2, cvb, chan_w, q)
        ag_opposite(2, cvb, chan_w, 0)
        ag_opposite(2, cvb, chan_w, 1)

    def mix_stage(q):
        ag_end(2, cvb, chan_w, q)
        channel_norm(q)
        branch = jnp.dot(mixed[...], mxb[...], preferred_element_type=F32)
        sb3[q, :, own_w] = (own_cols(sb1, q).astype(F32) + branch).astype(BF16)
        ag_start(3, sb3, width, q)

    with phase("mixw"):
        pltpu.make_async_copy(mxb, mxb, mx_recv.at[0]).wait()
    with phase("mix0"):
        mix_stage(0)
    with phase("mix12"):
        ag_opposite(2, cvb, chan_w, 2)
        mix_stage(1)
        mix_stage(2)
    late((D, 3))
    with phase("ag3"):
        for q in chunks:
            ag_relay(3, sb3, width, q)
        ag_opposite(3, sb3, width, 0)
        ag_opposite(3, sb3, width, 1)
    late((D, 4))
    with phase("ywait"):
        for i in range(2):
            y_all(i).wait_recv()

    def ffn_stage(q):
        ag_end(3, sb3, width, q)
        norm_rows(sb3, q, 2, q * rows)
        hidden_rows(q * rows, rows, slice(None), 2 * pairs)
        rs_partials(1, q)

    def last(q):
        total = rs_total(1, q)
        out[q * rows : (q + 1) * rows, :] = (own_cols(sb3, q).astype(F32) + 0.5 * total).astype(BF16)

    with phase("ffn0"):
        ffn_stage(0)
    with phase("ffn1"):
        ag_opposite(3, sb3, width, 2)
        ffn_stage(1)
    with phase("ffn2"):
        rs_opposite(1, 0)
        ffn_stage(2)
    with phase("rs1"):
        rs_opposite(1, 1)
        rs_opposite(1, 2)
        for q in chunks:
            rs_neighbours(1, q)
    with phase("last"):
        for q in chunks:
            last(q)

    for kind in range(6):
        ref = many(kind, n_fs - 1)
        remote(ref, ref, z_send.at[kind], z_recv.at[0], z_right).wait_send()
    for i in range(3):
        y_all(i).wait_send()
    pk_all.wait_send()
    ref = mxb.at[pl.ds(0, (n_tp - 1) * chan_w), :]
    remote(ref, ref, mx_send.at[0], mx_recv.at[0], sib).wait_send()
    ref = sb0.at[0:nq, :, 0:width]
    remote(ref, ref, yx_send.at[0], yx_recv.at[0], partner).wait_send()
    remote(ybo, ybo, yx_send.at[1], yx_recv.at[0], partner).wait_send()
    for n, buf, w in ((0, sb0, width), (1, sb1, width), (2, cvb, chan_w), (3, sb3, width)):
        ag_drain(n, buf, w)
    for n in range(2):
        rs_drain(n)


def solution(mesh):
    n_fs, n_tp = mesh.shape["fs"], mesh.shape["tp"]

    def local(
        stream_in,
        gain_before,
        gain_mixer,
        gain_after,
        w_gate,
        w_upward,
        w_down,
        w_value,
        w_glu_gate,
        conv_taps,
        chan_gain,
        chan_bias,
        w_mix_out,
    ):
        tokens, width = stream_in.shape
        k_rows, hidden = w_gate.shape
        chan_w = w_value.shape[1]
        units = -(-(hidden // 2) // LANES) * LANES
        nq = CHUNKS
        rows = tokens // nq
        feat, chan = width * n_tp, chan_w * n_tp
        vmem = pltpu.VMEM
        dma = pltpu.SemaphoreType.DMA
        any_space = pl.BlockSpec(memory_space=pl.ANY)
        in_vmem = pl.BlockSpec(memory_space=pltpu.VMEM)
        return pl.pallas_call(
            lambda *refs: layer_kernel(n_fs, n_tp, *refs),
            out_shape=jax.ShapeDtypeStruct((tokens, width), BF16),
            in_specs=[any_space, in_vmem, in_vmem] + [any_space] * 4 + [in_vmem] * 6,
            out_specs=in_vmem,
            scratch_shapes=[
                vmem((n_fs * k_rows, 4 * units), BF16),
                vmem((n_fs // 2, 2 * units, 2 * LANES), BF16),
                vmem((n_fs * k_rows, 3 * chan_w), BF16),
                vmem((chan, 2 * LANES), BF16),
                vmem((n_tp, 8, width), F32),
                vmem((8, feat), F32),
                vmem((16, chan), F32),
                vmem((2 * nq, rows, feat), BF16),
                vmem((nq, rows, feat), BF16),
                vmem((nq, rows, feat), BF16),
                vmem((nq, rows, chan), BF16),
                vmem((2 * tokens, feat), BF16),
                vmem((rows, chan), BF16),
                vmem((2 * tokens, 2 * units), BF16),
                vmem((rows // LEN, LEN + 32, chan_w), F32),
                vmem((nq, rows, width), BF16),
                vmem((nq, rows, width), BF16),
                vmem((2 * nq, 4, rows, width), F32),
                vmem((2 * nq, 14, rows, width), BF16),
                vmem((nq, 14, rows, width), BF16),
                dma((3,)),
                dma((6 * (n_fs // 2) + 3 * (n_fs // 4),)),
                dma((6,)),
                dma((3,)),
                dma((3,)),
                dma((1,)),
                dma((1,)),
                dma((1,)),
                dma((1,)),
                dma((2 + 3 * nq, 3)),
                dma((4,)),
                dma((3 * nq, 3)),
                dma((2,)),
                dma((nq + 1,)),
                dma((2,)),
                vmem((2 * tokens, 2 * units), F32),
            ],
            compiler_params=pltpu.CompilerParams(
                collective_id=0, has_side_effects=True, vmem_limit_bytes=60 * 1024 * 1024
            ),
        )(
            stream_in,
            w_gate.T,
            w_upward.T,
            w_down,
            w_value,
            w_glu_gate,
            w_mix_out,
            conv_taps,
            gain_before,
            gain_mixer,
            gain_after,
            chan_gain,
            chan_bias,
        )

    in_specs = (
        P(("grp", "fs"), "tp"),
        P("tp"),
        P("tp"),
        P("tp"),
        P("fs", "tp"),
        P("fs", "tp"),
        P("tp", "fs"),
        P("fs", "tp"),
        P("fs", "tp"),
        P(None, "tp"),
        P("tp"),
        P("tp"),
        P("tp", "fs"),
    )
    out_specs = P(("grp", "fs"), "tp")
    return jax.shard_map(local, mesh=mesh, in_specs=in_specs, out_specs=out_specs, check_vma=False)
```

```python
import jax
import jax.numpy as jnp
from jax import lax
from jax.experimental import pallas as pl
from jax.experimental.pallas import tpu as pltpu
from jax.sharding import PartitionSpec as P

MESH = pl.DeviceIdType.MESH
LEN = 128
EPS = 1e-06
LANES = 128
CHUNKS = 3
BF16, F32 = jnp.bfloat16, jnp.float32


def remote(src, dst, send_sem, recv_sem, where):
    return pltpu.make_async_remote_copy(
        src_ref=src,
        dst_ref=dst,
        send_sem=send_sem,
        recv_sem=recv_sem,
        device_id=where,
        device_id_type=MESH,
    )


def layer_kernel(
    n_fs,
    n_tp,
    s_in,
    gate_in,
    up_in,
    wd_in,
    value_in,
    glu_in,
    mix_in,
    taps_in,
    before_in,
    mixer_in,
    after_in,
    cgain_in,
    cbias_in,
    out,
    gu,
    wd,
    vm,
    mxb,
    pk,
    gf,
    cgb,
    sb0,
    sb1,
    sb3,
    cvb,
    ub,
    mixed,
    hid,
    pad,
    ybo,
    ybi,
    acc,
    rs0,
    rs1,
    load_sem,
    z_recv,
    z_send,
    y_recv,
    y_send,
    pk_recv,
    pk_send,
    mx_recv,
    mx_send,
    ag_recv,
    ag_send,
    rs_recv,
    rs_send,
    yx_recv,
    yx_send,
    part,
    g3,
    shard,
):
    z, t, g = lax.axis_index("fs"), lax.axis_index("tp"), lax.axis_index("grp")
    parity = lax.rem(g, 2)
    partner = {"grp": g + 1 - 2 * parity}
    z_right = {"fs": lax.rem(z + 1, n_fs)}
    z_left = {"fs": lax.rem(z + n_fs - 1, n_fs)}
    z_two = ({"fs": lax.rem(z + 2, n_fs)}, {"fs": lax.rem(z + n_fs - 2, n_fs)})
    chips = n_tp // 2
    x, core = t // 2, lax.rem(t, 2)
    xr, xl, xo = lax.rem(x + 1, chips), lax.rem(x + 3, chips), lax.rem(x + 2, chips)
    other = 1 - core
    sib = {"tp": 2 * x + other}
    x_right, x_left = {"tp": 2 * xr + core}, {"tp": 2 * xl + core}

    nq, rows, width = sb1.shape[0], sb1.shape[1], s_in.shape[1]
    half = rows // 2
    feat = width * n_tp
    k_rows, chan_w = value_in.shape
    chan = chan_w * n_tp
    steps = n_fs // 2
    own_units = gate_in.shape[0] // 2
    units = wd.shape[1] // 2
    pairs = units // LANES
    mine, theirs = parity, 1 - parity

    own_k = pl.ds(pl.multiple_of(z * k_rows, k_rows), k_rows)

    own_w = pl.ds(pl.multiple_of(t * width, width), width)

    rest = g3.shape[2] // 2

    def own_loads():
        for j, ref in enumerate((gate_in, up_in)):
            yield pltpu.make_async_copy(ref, shard.at[j], load_sem.at[3])
            for h in range(2):
                yield pltpu.make_async_copy(
                    ref.at[(h + 1) * own_units - rest : (h + 1) * own_units, :],
                    g3.at[h, z, j * rest : (j + 1) * rest, :],
                    load_sem.at[4],
                )
        for h in range(2):
            yield pltpu.make_async_copy(
                wd_in.at[h * own_units : (h + 1) * own_units, :],
                wd.at[
                    z // 2,
                    h * units : h * units + own_units,
                    pl.ds(pl.multiple_of(lax.rem(z, 2) * LANES, LANES), LANES),
                ],
                load_sem.at[0],
            )
        for i, ref in enumerate((value_in, glu_in, mix_in)):
            yield pltpu.make_async_copy(ref, vm.at[own_k, i * chan_w : (i + 1) * chan_w], load_sem.at[1])
        for q in range(nq):
            yield pltpu.make_async_copy(
                s_in.at[pl.ds(q * rows, rows), :],
                sb0.at[nq + q, :, pl.ds(pl.multiple_of(t * width, width), width)],
                load_sem.at[2],
            )

    for copy in own_loads():
        copy.start()

    barrier = pltpu.get_barrier_semaphore()
    peers = [z_right, z_left, *z_two, partner] + [{"tp": lax.rem(t + i, n_tp)} for i in range(1, n_tp)]
    for peer in peers:
        pl.semaphore_signal(barrier, inc=1, device_id=peer, device_id_type=MESH)

    def unpack(h, f):
        rws = pl.ds(pl.multiple_of(f * k_rows, k_rows), k_rows)
        for j in range(2):
            v = jnp.concatenate([g3[h, f, j * rest : (j + 1) * rest, :], jnp.zeros((LANES - rest, k_rows), BF16)], axis=0)
            c = pl.multiple_of(h * 2 * units + 2 * units - (2 - j) * LANES, LANES)
            gu[rws, pl.ds(c, LANES)] = v.T

    pltpu.make_async_copy(shard, shard, load_sem.at[3]).wait()
    pltpu.make_async_copy(g3.at[:, z], g3.at[:, z], load_sem.at[4]).wait()
    for h in range(2):
        for i in range(pairs - 1):
            for j in range(2):
                lo, c = h * own_units + i * LANES, h * 2 * units + (2 * i + j) * LANES
                gu[own_k, c : c + LANES] = shard[j, lo : lo + LANES, :].T
        unpack(h, z)
        wd[:, h * units + own_units : (h + 1) * units, :] = jnp.zeros((wd.shape[0], units - own_units, wd.shape[2]), BF16)
    for i, ref in enumerate((before_in, mixer_in, after_in)):
        pk[t, i : i + 1, :] = ref[...].astype(F32).reshape(1, width)
    pk[t, 3:4, :chan_w] = cgain_in[...].astype(F32).reshape(1, chan_w)
    pk[t, 3:4, chan_w:] = cbias_in[...].astype(F32).reshape(1, chan_w)
    pk[t, 4:8, :] = jnp.zeros((4, width), F32)

    pl.semaphore_wait(barrier, len(peers))

    ref = vm.at[own_k, :]
    pltpu.make_async_copy(wd_in, wd_in, load_sem.at[0]).wait()
    pltpu.make_async_copy(ref, ref, load_sem.at[1]).wait()
    pltpu.make_async_copy(s_in, s_in, load_sem.at[2]).wait()

    wide = 2 * LANES * (pairs - 1)
    A0, A1, B, X, M, D = range(6)

    def piece(kind, f, part=None):
        if kind in (B, D):
            size = own_units if part is None else own_units // 2
            q0 = (mine if kind == B else theirs) * units + (0 if part is None else part * size)
            return wd.at[
                f // 2,
                pl.ds(pl.multiple_of(q0, 16), size),
                pl.ds(pl.multiple_of(lax.rem(f, 2) * LANES, LANES), LANES),
            ]
        if kind == A1:
            return g3.at[mine, f] if part is None else g3.at[mine, f, part * rest : (part + 1) * rest]
        size = k_rows if part is None else k_rows // 2
        r0 = pl.ds(pl.multiple_of(f * k_rows + (0 if part is None else part * size), size), size)
        c0 = mine * 2 * units
        if kind == A0:
            return gu.at[r0, pl.ds(pl.multiple_of(c0, LANES), wide)]
        if kind == X:
            return vm.at[r0, pl.ds(pl.multiple_of(mine * chan_w, LANES), chan_w)]
        return vm.at[r0, 2 * chan_w : 3 * chan_w]

    def many(kind, count):
        if kind in (B, D):
            if count <= wd.shape[0]:
                return wd.at[0:count, 0:own_units, 0:LANES]
            total = count * own_units // 2
            for a in range(1, wd.shape[0] + 1):
                if total % (16 * a) == 0 and total // a <= wd.shape[1]:
                    return wd.at[0:a, 0 : total // a, :]
        if kind == A0:
            return gu.at[0 : count * k_rows, 0:wide]
        if kind == A1:
            return g3.at[0, 0:count]
        return vm.at[0 : count * k_rows, 0:chan_w]

    def origin(way, s):
        return lax.rem(z + n_fs - s, n_fs) if way == 0 else lax.rem(z + s, n_fs)

    def z_sem(kind, way, s):
        return z_recv.at[(kind * 2 + way) * steps + s - 1]

    def z_copy(kind, way, s_next):
        ref = piece(kind, origin(way, s_next - 1), None if s_next < steps else way)
        return remote(ref, ref, z_send.at[kind], z_sem(kind, way, s_next), z_right if way == 0 else z_left)

    def y_copy(ref, i):
        return remote(ref, ref, y_send.at[i], y_recv.at[i], partner)

    def y_all(i):
        return y_copy(many((A0, A1, X)[i], n_fs - 1), i)

    def stream_copy(q):
        return remote(sb0.at[nq + q, :, own_w], sb0.at[q, :, own_w], yx_send.at[0], yx_recv.at[nq], partner)

    def part_copy(q):
        return remote(ybo.at[q], ybi.at[q], yx_send.at[1], yx_recv.at[q], partner)

    def spread_mix(f):
        dest, b = f // 2, lax.rem(f, 2)
        src = piece(M, f)
        dst = mxb.at[
            pl.ds(pl.multiple_of(t * chan_w, chan_w), chan_w), pl.ds(pl.multiple_of(b * LANES, LANES), LANES)
        ]

        @pl.when(dest != t)
        def _():
            remote(src, dst, mx_send.at[0], mx_recv.at[0], {"tp": dest}).start()

        @pl.when(dest == t)
        def _():
            pltpu.make_async_copy(src, dst, mx_recv.at[0]).start()

    def relay(kind, s):
        for way in range(2):
            part = None if s < steps else way
            ref = piece(kind, origin(way, s), part)
            remote(ref, ref, z_send.at[kind], z_sem(kind, way, s), z_right).wait_recv()
            if s < steps:
                z_copy(kind, way, s + 1).start()
            if kind == A0:
                y_copy(ref, 0).start()
            if kind == A1 and (s < steps or way == 1):
                unpack(mine, origin(way, s))

    def leap_sem(kind, k):
        return z_recv.at[2 * X * steps + (kind - X) * (steps // 2) + k - 1]

    def leap_send(kind, k):
        for far in (True, False):
            for way in range(2):
                part = way if far and 2 * k == steps else None
                ref = piece(kind, origin(way, 2 * k - 2), part)
                where = z_two[way] if far else (z_right, z_left)[way]
                remote(ref, ref, z_send.at[kind], leap_sem(kind, k), where).start()

    def leap(kind, k):
        ref = many(kind, 4 if 2 * k < steps else 3)
        remote(ref, ref, z_send.at[kind], leap_sem(kind, k), z_right).wait_recv()
        if 2 * k < steps:
            leap_send(kind, k + 1)
        for way, d in ((0, 2 * k), (1, 2 * k), (0, 2 * k - 1), (1, 2 * k - 1)):
            if d == steps and way == 1:
                continue
            if kind == X:
                y_copy(piece(X, origin(way, d)), 2).start()
            if kind == M:
                spread_mix(origin(way, d))

    def block(buf, w, q, b, part=None):
        rws = slice(None) if part is None else pl.ds(part * half, half)
        return buf.at[q, rws, pl.ds(pl.multiple_of(b * w, w), w)]

    def ag_copy(n, ref, slot, i, where):
        return remote(ref, ref, ag_send.at[n], ag_recv.at[slot, i], where)

    def ag_slot(n, q):
        return q // nq if n == 0 else 2 + (n - 1) * nq + q

    def ag_chunks(n, q):
        return slice(q, q + nq) if n == 0 else q

    def ag_start(n, buf, w, q):
        slot, own = ag_slot(n, q), block(buf, w, ag_chunks(n, q), t)
        ag_copy(n, own, slot, 0, x_right).start()
        ag_copy(n, own, slot, 0, x_left).start()
        ag_copy(n, own, slot, 2, sib).start()

    def ag_wait(n, buf, w, q, i, count):
        ag_copy(n, buf.at[ag_chunks(n, q), :, 0 : count * w], ag_slot(n, q), i, sib).wait_recv()

    def ag_relay(n, buf, w, q):
        slot, c = ag_slot(n, q), ag_chunks(n, q)
        b_l, b_r = 2 * xl + core, 2 * xr + core
        ag_wait(n, buf, w, q, 0, 2)
        ag_copy(n, block(buf, w, c, b_l, 0), slot, 1, x_right).start()
        ag_copy(n, block(buf, w, c, b_r, 1), slot, 1, x_left).start()
        ag_copy(n, block(buf, w, c, b_l), slot, 2, sib).start()
        ag_copy(n, block(buf, w, c, b_r), slot, 2, sib).start()

    def ag_opposite(n, buf, w, q):
        ag_wait(n, buf, w, q, 1, 1)
        ag_copy(n, block(buf, w, ag_chunks(n, q), 2 * xo + core), ag_slot(n, q), 2, sib).start()

    def ag_end(n, buf, w, q):
        ag_wait(n, buf, w, q, 2, 4)

    def ag_drain(n, buf, w):
        ag_copy(n, buf.at[:, :, 0 : 7 * w], 0, 0, sib).wait_send()

    order = (xo, xr, xl, x)
    rs_refs = (rs0, rs1)

    def rs_copy(src, dst, n, q, i, where):
        return remote(
            rs_refs[n].at[(q, *src)], rs_refs[n].at[(q, *dst)], rs_send.at[n], rs_recv.at[2 * nq * n + q, i], where
        )

    def sib_copy(n, q):
        return rs_copy((slice(0, 4),), (slice(4, 8),), n, q, 0, sib)

    def opp_copy(n, q, i):
        part = pl.ds(i * half, half)
        return rs_copy((8, part), (9, part), n, q, 1, x_right if i == 0 else x_left)

    def nb_copy(n, q, i):
        return rs_copy((10 + i,), (12 + i,), n, q, 2, x_right if i == 0 else x_left)

    def rs_partials(n, q):
        buf = rs_refs[n]
        width_k = units if n == 0 else 2 * units
        k_range = pl.ds(pl.multiple_of(mine * units, LANES), units) if n == 0 else slice(None)
        h = hid[q * rows : (q + 1) * rows, 0:width_k]
        for k in range(4):
            buf[q, k] = jnp.dot(h, wd[2 * order[k] + other, k_range, :], preferred_element_type=F32).astype(BF16)
        sib_copy(n, q).start()
        for k in range(4):
            acc[q, k] = jnp.dot(h, wd[2 * order[k] + core, k_range, :], preferred_element_type=F32)

    def rs_opposite(n, q):
        buf = rs_refs[n]
        sib_copy(n, q).wait_recv()
        buf[q, 8] = (acc[q, 0] + buf[q, 4].astype(F32)).astype(BF16)
        opp_copy(n, q, 0).start()
        opp_copy(n, q, 1).start()

    def rs_neighbours(n, q):
        buf = rs_refs[n]
        rs_copy((9,), (9,), n, q, 1, sib).wait_recv()
        for i in range(2):
            near, far = pl.ds(i * half, half), pl.ds((1 - i) * half, half)
            buf[q, 10 + i, near] = (
                acc[q, 1 + i, near] + buf[q, 5 + i, near].astype(F32) + buf[q, 9, near].astype(F32)
            ).astype(BF16)
            buf[q, 10 + i, far] = (acc[q, 1 + i, far] + buf[q, 5 + i, far].astype(F32)).astype(BF16)
            nb_copy(n, q, i).start()

    def rs_total(n, q):
        buf = rs_refs[n]
        rs_copy((slice(12, 14),), (slice(12, 14),), n, q, 2, sib).wait_recv()
        return acc[q, 3] + buf[q, 7].astype(F32) + buf[q, 12].astype(F32) + buf[q, 13].astype(F32)

    def rs_drain(n):
        ref = rs_refs[n].at[:, 0:7]
        remote(ref, ref, rs_send.at[n], rs_recv.at[0, 0], sib).wait_send()

    def norm_rows(buf, q, r, base):
        @pl.loop(0, rows // 16, unroll=4)
        def _(i):
            rws = pl.ds(pl.multiple_of(i * 16, 16), 16)
            v = buf[q, rws, :].astype(F32)
            inverse = lax.rsqrt(jnp.sum(v * v, axis=1, keepdims=True) / feat + EPS)
            ub[pl.ds(pl.multiple_of(base + i * 16, 16), 16), :] = (v * inverse * gf[r : r + 1, :]).astype(BF16)

    def gate_up(a, b):
        return (jax.nn.silu(a) * b).astype(BF16)

    def hidden_rows(lo, count, columns, n_pairs):
        r = jnp.dot(ub[lo : lo + count, :], gu[:, columns], preferred_element_type=F32)
        for n in range(n_pairs):
            a, b = r[:, 2 * n * LANES : (2 * n + 1) * LANES], r[:, (2 * n + 1) * LANES : (2 * n + 2) * LANES]
            hid[lo : lo + count, n * LANES : (n + 1) * LANES] = gate_up(a, b)

    my_half = pl.ds(pl.multiple_of(mine * 2 * units, LANES), 2 * units)

    def pair_sum(s, lo, count):
        up = lax.rem(z + s, 2) == 1
        f = jnp.where(up, lax.rem(z + s - 1, n_fs), lax.rem(z + n_fs - s, n_fs))
        ks = pl.ds(pl.multiple_of(f // 2 * (2 * k_rows), 2 * k_rows), 2 * k_rows)
        return jnp.dot(ub[lo : lo + count, ks], gu[ks, my_half], preferred_element_type=F32)

    def gather_pair(s, lo, count):
        r = pair_sum(s, lo, count)
        part[lo : lo + count, :] = r if s == 1 else part[lo : lo + count, :] + r

    def last_pair(lo, count):
        r = part[lo : lo + count, :] + pair_sum(steps, lo, count)
        for n in range(pairs):
            a, b = r[:, 2 * n * LANES : (2 * n + 1) * LANES], r[:, (2 * n + 1) * LANES : (2 * n + 2) * LANES]
            hid[lo : lo + count, n * LANES : (n + 1) * LANES] = gate_up(a, b)

    def conv(q):
        r = jnp.dot(ub[q * rows : (q + 1) * rows, :], vm[:, : 2 * chan_w], preferred_element_type=F32)
        glued = r[:, :chan_w] * jax.nn.sigmoid(r[:, chan_w:])
        for i in range(rows // LEN):
            pad[i, 32:, :] = glued[i * LEN : (i + 1) * LEN]
        n_taps = taps_in.shape[0]
        taps = taps_in[...].astype(F32)
        for i in range(rows // LEN):
            total = jnp.zeros((LEN, chan_w), F32)
            for k in range(n_taps):
                total = total + taps[k : k + 1, :] * pad[i, 33 - n_taps + k : 33 - n_taps + k + LEN, :]
            cvb[q, i * LEN : (i + 1) * LEN, pl.ds(pl.multiple_of(t * chan_w, chan_w), chan_w)] = total.astype(BF16)

    def channel_norm(q):
        @pl.loop(0, rows // 16, unroll=4)
        def _(i):
            rws = pl.ds(pl.multiple_of(i * 16, 16), 16)
            v = cvb[q, rws, :].astype(F32)
            mu = jnp.sum(v, axis=1, keepdims=True) / chan
            msq = jnp.sum(v * v, axis=1, keepdims=True) / chan
            w = (v - mu) * lax.rsqrt(msq - mu * mu + EPS) * cgb[3:4, :] + cgb[11:12, :]
            mixed[rws, :] = jax.nn.silu(w).astype(BF16)

    def own_cols(buf, q):
        return buf[q, :, own_w]

    def z_begin(kinds):
        for kind in kinds:
            for way in range(2):
                z_copy(kind, way, 1).start()

    def relays(kinds, s):
        for kind in kinds:
            relay(kind, s)

    first_kinds = (A0, A1, B)

    def phase(name):
        return jax.named_scope(name)

    chunks = range(nq)
    z_begin(first_kinds)
    for q in chunks:
        stream_copy(q).start()
    ag_start(0, sb0, width, nq)

    def pk_copy(i):
        return remote(pk.at[t], pk.at[t], pk_send.at[0], pk_recv.at[0], {"tp": lax.rem(t + i, n_tp)})

    pk_all = remote(pk.at[0 : n_tp - 1], pk.at[0 : n_tp - 1], pk_send.at[0], pk_recv.at[0], sib)

    for i in range(1, n_tp):
        pk_copy(i).start()
    spread_mix(z)
    pad[:, :32, :] = jnp.zeros((pad.shape[0], 32, chan_w), F32)

    with phase("w1"):
        relays(first_kinds, 1)
    with phase("ag0"):
        ref = sb0.at[0:nq, :, 0:width]
        remote(ref, ref, yx_send.at[0], yx_recv.at[nq], partner).wait_recv()
        ag_start(0, sb0, width, 0)
        ag_relay(0, sb0, width, nq)
    with phase("w2"):
        relays(first_kinds, 2)
    ag_relay(0, sb0, width, 0)
    ag_opposite(0, sb0, width, nq)
    with phase("w3"):
        relays(first_kinds, 3)
    ag_opposite(0, sb0, width, 0)
    ag_end(0, sb0, width, nq)
    pk_all.wait_recv()
    for b in range(n_tp):
        gf[:, b * width : (b + 1) * width] = pk[b]
        cgb[0:8, b * chan_w : (b + 1) * chan_w] = pk[b][:, :chan_w]
        cgb[8:16, b * chan_w : (b + 1) * chan_w] = pk[b][:, chan_w : 2 * chan_w]
    tokens = nq * rows
    pl.loop(nq, 2 * nq)(lambda q: norm_rows(sb0, q, 0, q * rows))
    with phase("w4"):
        relays(first_kinds, 4)
    ag_end(0, sb0, width, 0)
    pl.loop(0, nq)(lambda q: norm_rows(sb0, q, 0, q * rows))

    def relay_and_sum(s, work):
        for kind, some in zip(first_kinds, work):
            relay(kind, s)
            for i, lo in some:
                gather_pair(i, lo, tokens)

    with phase("w5"):
        relay_and_sum(5, (((1, 0),), ((1, tokens),), ((2, 0), (2, tokens))))
    with phase("w6"):
        relay_and_sum(6, (((3, 0),), ((3, tokens),), ((4, 0), (4, tokens))))
    with phase("w7"):
        relay_and_sum(7, (((5, 0),), ((5, tokens), (6, 0)), ((6, tokens), (7, 0), (7, tokens))))
    leap_send(X, 1)
    with phase("w8"):
        relays((A0, A1), 8)

    def late(*steps_of):
        with phase("late"):
            for kind, i in steps_of:
                leap(kind, i)

    def y_late(lo, hi):
        @pl.loop(lo, hi)
        def _(i):
            y_copy(piece(A1, lax.rem(z + i, n_fs)), 1).start()

    with phase("hid_theirs"):
        last_pair(0, tokens)
    with phase("w8b"):
        relay(B, 8)
    with phase("part_theirs"):
        for q in chunks:
            rs_partials(0, q)
    with phase("hid_ours"):
        last_pair(tokens, tokens)
    late((X, 1))
    leap_send(M, 1)
    y_late(1, 5)

    def pass_over(q):
        ybo[q] = rs_total(0, q).astype(BF16)
        part_copy(q).start()

    def first(q):
        total = rs_total(0, nq + q)
        part_copy(q).wait_recv()
        sb1[q, :, own_w] = (own_cols(sb0, nq + q).astype(F32) + 0.5 * (total + ybi[q].astype(F32))).astype(BF16)
        ag_start(1, sb1, width, q)

    with phase("rs_a"):
        for q in chunks:
            rs_opposite(0, q)
            rs_partials(0, nq + q)
        for q in chunks:
            rs_opposite(0, nq + q)
    with phase("rs_b"):
        rs_neighbours(0, 0)
    late((X, 2), (M, 1))
    leap_send(D, 1)
    with phase("rs_c"):
        rs_neighbours(0, 1)
        rs_neighbours(0, 2)
        rs_neighbours(0, nq)
        pass_over(0)
        rs_neighbours(0, nq + 1)
        pass_over(1)
    late((X, 3), (M, 2))
    with phase("rs_d"):
        rs_neighbours(0, nq + 2)
        pass_over(2)
    with phase("first"):
        for q in chunks:
            first(q)
    late((X, 4), (M, 3), (D, 1))
    y_late(5, n_fs)
    with phase("ag1"):
        for q in chunks:
            ag_relay(1, sb1, width, q)
    late((M, 4))
    with phase("opp1"):
        ag_opposite(1, sb1, width, 0)
        ag_opposite(1, sb1, width, 1)

    def conv_stage(q):
        ag_end(1, sb1, width, q)
        norm_rows(sb1, q, 1, q * rows)
        conv(q)
        ag_start(2, cvb, chan_w, q)

    with phase("ywaitx"):
        y_all(2).wait_recv()
    with phase("conv0"):
        conv_stage(0)
    with phase("conv12"):
        ag_opposite(1, sb1, width, 2)
        conv_stage(1)
        conv_stage(2)
    late((D, 2))
    with phase("ag2"):
        for q in chunks:
            ag_relay(2, cvb, chan_w, q)
        y_all(1).wait_recv()
        pl.loop(1, n_fs)(lambda i: unpack(theirs, lax.rem(z + i, n_fs)))
        ag_opposite(2, cvb, chan_w, 0)
        ag_opposite(2, cvb, chan_w, 1)

    def mix_stage(q):
        ag_end(2, cvb, chan_w, q)
        channel_norm(q)
        branch = jnp.dot(mixed[...], mxb[...], preferred_element_type=F32)
        sb3[q, :, own_w] = (own_cols(sb1, q).astype(F32) + branch).astype(BF16)
        ag_start(3, sb3, width, q)

    with phase("mixw"):
        pltpu.make_async_copy(mxb, mxb, mx_recv.at[0]).wait()
    with phase("mix0"):
        mix_stage(0)
    with phase("mix12"):
        ag_opposite(2, cvb, chan_w, 2)
        mix_stage(1)
        mix_stage(2)
    late((D, 3))
    with phase("ag3"):
        for q in chunks:
            ag_relay(3, sb3, width, q)
        ag_opposite(3, sb3, width, 0)
        ag_opposite(3, sb3, width, 1)
    late((D, 4))
    with phase("ywait"):
        y_all(0).wait_recv()

    def ffn_stage(q):
        ag_end(3, sb3, width, q)
        norm_rows(sb3, q, 2, q * rows)
        hidden_rows(q * rows, rows, slice(None), 2 * pairs)
        rs_partials(1, q)

    def last(q):
        total = rs_total(1, q)
        out[q * rows : (q + 1) * rows, :] = (own_cols(sb3, q).astype(F32) + 0.5 * total).astype(BF16)

    with phase("ffn0"):
        ffn_stage(0)
    with phase("ffn1"):
        ag_opposite(3, sb3, width, 2)
        ffn_stage(1)
    with phase("ffn2"):
        rs_opposite(1, 0)
        ffn_stage(2)
    with phase("rs1"):
        rs_opposite(1, 1)
        rs_opposite(1, 2)
        for q in chunks:
            rs_neighbours(1, q)
    with phase("last"):
        for q in chunks:
            last(q)

    for kind in range(6):
        ref = many(kind, n_fs - 1)
        remote(ref, ref, z_send.at[kind], z_recv.at[0], z_right).wait_send()
    for i in range(3):
        y_all(i).wait_send()
    pk_all.wait_send()
    ref = mxb.at[pl.ds(0, (n_tp - 1) * chan_w), :]
    remote(ref, ref, mx_send.at[0], mx_recv.at[0], sib).wait_send()
    ref = sb0.at[0:nq, :, 0:width]
    remote(ref, ref, yx_send.at[0], yx_recv.at[0], partner).wait_send()
    remote(ybo, ybo, yx_send.at[1], yx_recv.at[0], partner).wait_send()
    for n, buf, w in ((0, sb0, width), (1, sb1, width), (2, cvb, chan_w), (3, sb3, width)):
        ag_drain(n, buf, w)
    for n in range(2):
        rs_drain(n)


def solution(mesh):
    n_fs, n_tp = mesh.shape["fs"], mesh.shape["tp"]

    def local(
        stream_in,
        gain_before,
        gain_mixer,
        gain_after,
        w_gate,
        w_upward,
        w_down,
        w_value,
        w_glu_gate,
        conv_taps,
        chan_gain,
        chan_bias,
        w_mix_out,
    ):
        tokens, width = stream_in.shape
        k_rows, hidden = w_gate.shape
        chan_w = w_value.shape[1]
        units = -(-(hidden // 2) // LANES) * LANES
        nq = CHUNKS
        rows = tokens // nq
        feat, chan = width * n_tp, chan_w * n_tp
        vmem = pltpu.VMEM
        dma = pltpu.SemaphoreType.DMA
        any_space = pl.BlockSpec(memory_space=pl.ANY)
        in_vmem = pl.BlockSpec(memory_space=pltpu.VMEM)
        return pl.pallas_call(
            lambda *refs: layer_kernel(n_fs, n_tp, *refs),
            out_shape=jax.ShapeDtypeStruct((tokens, width), BF16),
            in_specs=[any_space] * 7 + [in_vmem] * 6,
            out_specs=in_vmem,
            scratch_shapes=[
                vmem((n_fs * k_rows, 4 * units), BF16),
                vmem((n_fs // 2, 2 * units, 2 * LANES), BF16),
                vmem((n_fs * k_rows, 3 * chan_w), BF16),
                vmem((chan, 2 * LANES), BF16),
                vmem((n_tp, 8, width), F32),
                vmem((8, feat), F32),
                vmem((16, chan), F32),
                vmem((2 * nq, rows, feat), BF16),
                vmem((nq, rows, feat), BF16),
                vmem((nq, rows, feat), BF16),
                vmem((nq, rows, chan), BF16),
                vmem((2 * tokens, feat), BF16),
                vmem((rows, chan), BF16),
                vmem((2 * tokens, 2 * units), BF16),
                vmem((rows // LEN, LEN + 32, chan_w), F32),
                vmem((nq, rows, width), BF16),
                vmem((nq, rows, width), BF16),
                vmem((2 * nq, 4, rows, width), F32),
                vmem((2 * nq, 14, rows, width), BF16),
                vmem((nq, 14, rows, width), BF16),
                dma((5,)),
                dma((6 * (n_fs // 2) + 3 * (n_fs // 4),)),
                dma((6,)),
                dma((3,)),
                dma((3,)),
                dma((1,)),
                dma((1,)),
                dma((1,)),
                dma((1,)),
                dma((2 + 3 * nq, 3)),
                dma((4,)),
                dma((3 * nq, 3)),
                dma((2,)),
                dma((nq + 1,)),
                dma((2,)),
                vmem((2 * tokens, 2 * units), F32),
                vmem((2, n_fs, 2 * ((hidden // 2 - 1) % LANES + 1), k_rows), BF16),
                vmem((2, hidden, k_rows), BF16),
            ],
            compiler_params=pltpu.CompilerParams(
                collective_id=0, has_side_effects=True, vmem_limit_bytes=60 * 1024 * 1024
            ),
        )(
            stream_in,
            w_gate.T,
            w_upward.T,
            w_down,
            w_value,
            w_glu_gate,
            w_mix_out,
            conv_taps,
            gain_before,
            gain_mixer,
            gain_after,
            chan_gain,
            chan_bias,
        )

    in_specs = (
        P(("grp", "fs"), "tp"),
        P("tp"),
        P("tp"),
        P("tp"),
        P("fs", "tp"),
        P("fs", "tp"),
        P("tp", "fs"),
        P("fs", "tp"),
        P("fs", "tp"),
        P(None, "tp"),
        P("tp"),
        P("tp"),
        P("tp", "fs"),
    )
    out_specs = P(("grp", "fs"), "tp")
    return jax.shard_map(local, mesh=mesh, in_specs=in_specs, out_specs=out_specs, check_vma=False)
```

```python
import jax
import jax.numpy as jnp
from jax import lax
from jax.experimental import pallas as pl
from jax.experimental.pallas import tpu as pltpu
from jax.sharding import PartitionSpec as P

MESH = pl.DeviceIdType.MESH
LEN = 128
EPS = 1e-06
LANES = 128
CHUNKS = 3
Y_ROWS = 160
BF16, F32 = jnp.bfloat16, jnp.float32


def remote(src, dst, send_sem, recv_sem, where):
    return pltpu.make_async_remote_copy(
        src_ref=src,
        dst_ref=dst,
        send_sem=send_sem,
        recv_sem=recv_sem,
        device_id=where,
        device_id_type=MESH,
    )


def layer_kernel(
    n_fs,
    n_tp,
    s_in,
    gate_in,
    up_in,
    wd_in,
    value_in,
    glu_in,
    mix_in,
    taps_in,
    before_in,
    mixer_in,
    after_in,
    cgain_in,
    cbias_in,
    out,
    gu,
    wd,
    vm,
    mxb,
    pk,
    gf,
    cgb,
    sb0,
    sb1,
    sb3,
    cvb,
    ub,
    mixed,
    hid,
    pad,
    ybo,
    ybi,
    acc,
    rs0,
    rs1,
    load_sem,
    z_recv,
    z_send,
    y_recv,
    y_send,
    pk_recv,
    pk_send,
    mx_recv,
    mx_send,
    ag_recv,
    ag_send,
    rs_recv,
    rs_send,
    yx_recv,
    yx_send,
    part,
    g3,
    shard,
):
    z, t, g = lax.axis_index("fs"), lax.axis_index("tp"), lax.axis_index("grp")
    parity = lax.rem(g, 2)
    partner = {"grp": g + 1 - 2 * parity}
    z_right = {"fs": lax.rem(z + 1, n_fs)}
    z_left = {"fs": lax.rem(z + n_fs - 1, n_fs)}
    z_two = ({"fs": lax.rem(z + 2, n_fs)}, {"fs": lax.rem(z + n_fs - 2, n_fs)})
    chips = n_tp // 2
    x, core = t // 2, lax.rem(t, 2)
    xr, xl, xo = lax.rem(x + 1, chips), lax.rem(x + 3, chips), lax.rem(x + 2, chips)
    other = 1 - core
    sib = {"tp": 2 * x + other}
    x_right, x_left = {"tp": 2 * xr + core}, {"tp": 2 * xl + core}

    nq, rows, width = sb1.shape[0], sb1.shape[1], s_in.shape[1]
    half = rows // 2
    feat = width * n_tp
    k_rows, chan_w = value_in.shape
    chan = chan_w * n_tp
    steps = n_fs // 2
    own_units = gate_in.shape[0] // 2
    units = wd.shape[1] // 2
    pairs = units // LANES
    mine, theirs = parity, 1 - parity

    own_k = pl.ds(pl.multiple_of(z * k_rows, k_rows), k_rows)

    own_w = pl.ds(pl.multiple_of(t * width, width), width)

    rest = g3.shape[2] // 2

    def own_loads():
        for j, ref in enumerate((gate_in, up_in)):
            yield pltpu.make_async_copy(ref, shard.at[j], load_sem.at[3])
            for h in range(2):
                yield pltpu.make_async_copy(
                    ref.at[(h + 1) * own_units - rest : (h + 1) * own_units, :],
                    g3.at[h, z, j * rest : (j + 1) * rest, :],
                    load_sem.at[4],
                )
        for h in range(2):
            yield pltpu.make_async_copy(
                wd_in.at[h * own_units : (h + 1) * own_units, :],
                wd.at[
                    z // 2,
                    h * units : h * units + own_units,
                    pl.ds(pl.multiple_of(lax.rem(z, 2) * LANES, LANES), LANES),
                ],
                load_sem.at[0],
            )
        for i, ref in enumerate((value_in, glu_in, mix_in)):
            yield pltpu.make_async_copy(ref, vm.at[own_k, i * chan_w : (i + 1) * chan_w], load_sem.at[1])
        for q in range(nq):
            yield pltpu.make_async_copy(
                s_in.at[pl.ds(q * rows, rows), :],
                sb0.at[nq + q, :, pl.ds(pl.multiple_of(t * width, width), width)],
                load_sem.at[2],
            )

    for copy in own_loads():
        copy.start()

    barrier = pltpu.get_barrier_semaphore()
    peers = [z_right, z_left, *z_two, partner] + [{"tp": lax.rem(t + i, n_tp)} for i in range(1, n_tp)]
    for peer in peers:
        pl.semaphore_signal(barrier, inc=1, device_id=peer, device_id_type=MESH)

    def unpack(h, f):
        rws = pl.ds(pl.multiple_of(f * k_rows, k_rows), k_rows)
        for j in range(2):
            v = jnp.concatenate([g3[h, f, j * rest : (j + 1) * rest, :], jnp.zeros((LANES - rest, k_rows), BF16)], axis=0)
            c = pl.multiple_of(h * 2 * units + 2 * units - (2 - j) * LANES, LANES)
            gu[rws, pl.ds(c, LANES)] = v.T

    pltpu.make_async_copy(shard, shard, load_sem.at[3]).wait()
    pltpu.make_async_copy(g3.at[:, z], g3.at[:, z], load_sem.at[4]).wait()
    for h in range(2):
        for i in range(pairs - 1):
            for j in range(2):
                lo, c = h * own_units + i * LANES, h * 2 * units + (2 * i + j) * LANES
                gu[own_k, c : c + LANES] = shard[j, lo : lo + LANES, :].T
        unpack(h, z)
        wd[:, h * units + own_units : (h + 1) * units, :] = jnp.zeros((wd.shape[0], units - own_units, wd.shape[2]), BF16)
    for i, ref in enumerate((before_in, mixer_in, after_in)):
        pk[t, i : i + 1, :] = ref[...].astype(F32).reshape(1, width)
    pk[t, 3:4, :chan_w] = cgain_in[...].astype(F32).reshape(1, chan_w)
    pk[t, 3:4, chan_w:] = cbias_in[...].astype(F32).reshape(1, chan_w)
    pk[t, 4:8, :] = jnp.zeros((4, width), F32)

    pl.semaphore_wait(barrier, len(peers))

    ref = vm.at[own_k, :]
    pltpu.make_async_copy(wd_in, wd_in, load_sem.at[0]).wait()
    pltpu.make_async_copy(ref, ref, load_sem.at[1]).wait()
    pltpu.make_async_copy(s_in, s_in, load_sem.at[2]).wait()

    wide = 2 * LANES * (pairs - 1)
    A0, A1, B, X, M, D, Y = range(7)

    def down_rows(kind):
        return {B: own_units, D: own_units - Y_ROWS, Y: Y_ROWS}[kind]

    def piece(kind, f, part=None):
        if kind in (B, D, Y):
            size = down_rows(kind) if part is None else down_rows(kind) // 2
            q0 = (theirs * units + Y_ROWS if kind == D else mine * units) + (0 if part is None else part * size)
            return wd.at[
                f // 2,
                pl.ds(pl.multiple_of(q0, 16), size),
                pl.ds(pl.multiple_of(lax.rem(f, 2) * LANES, LANES), LANES),
            ]
        if kind == A1:
            return g3.at[mine, f] if part is None else g3.at[mine, f, part * rest : (part + 1) * rest]
        size = k_rows if part is None else k_rows // 2
        r0 = pl.ds(pl.multiple_of(f * k_rows + (0 if part is None else part * size), size), size)
        c0 = mine * 2 * units
        if kind == A0:
            return gu.at[r0, pl.ds(pl.multiple_of(c0, LANES), wide)]
        if kind == X:
            return vm.at[r0, pl.ds(pl.multiple_of(mine * chan_w, LANES), chan_w)]
        return vm.at[r0, 2 * chan_w : 3 * chan_w]

    def many(kind, count):
        if kind in (B, D, Y):
            size = down_rows(kind)
            if count <= wd.shape[0]:
                return wd.at[0:count, 0:size, 0:LANES]
            total = count * size // 2
            for a in range(1, wd.shape[0] + 1):
                if total % (16 * a) == 0 and total // a <= wd.shape[1]:
                    return wd.at[0:a, 0 : total // a, :]
        if kind == A0:
            return gu.at[0 : count * k_rows, 0:wide]
        if kind == A1:
            return g3.at[0, 0:count]
        return vm.at[0 : count * k_rows, 0:chan_w]

    def origin(way, s):
        return lax.rem(z + n_fs - s, n_fs) if way == 0 else lax.rem(z + s, n_fs)

    def z_sem(kind, way, s):
        return z_recv.at[(kind * 2 + way) * steps + s - 1]

    def z_copy(kind, way, s_next):
        ref = piece(kind, origin(way, s_next - 1), None if s_next < steps else way)
        return remote(ref, ref, z_send.at[kind], z_sem(kind, way, s_next), z_right if way == 0 else z_left)

    def y_copy(ref, i):
        return remote(ref, ref, y_send.at[i], y_recv.at[i], partner)

    def y_all(i):
        return y_copy(many((A0, A1, X, Y)[i], n_fs - 1), i)

    def stream_copy(q):
        return remote(sb0.at[nq + q, :, own_w], sb0.at[q, :, own_w], yx_send.at[0], yx_recv.at[nq], partner)

    def part_copy(q):
        return remote(ybo.at[q], ybi.at[q], yx_send.at[1], yx_recv.at[q], partner)

    def spread_mix(f):
        dest, b = f // 2, lax.rem(f, 2)
        src = piece(M, f)
        dst = mxb.at[
            pl.ds(pl.multiple_of(t * chan_w, chan_w), chan_w), pl.ds(pl.multiple_of(b * LANES, LANES), LANES)
        ]

        @pl.when(dest != t)
        def _():
            remote(src, dst, mx_send.at[0], mx_recv.at[0], {"tp": dest}).start()

        @pl.when(dest == t)
        def _():
            pltpu.make_async_copy(src, dst, mx_recv.at[0]).start()

    def relay(kind, s):
        for way in range(2):
            part = None if s < steps else way
            ref = piece(kind, origin(way, s), part)
            remote(ref, ref, z_send.at[kind], z_sem(kind, way, s), z_right).wait_recv()
            if s < steps:
                z_copy(kind, way, s + 1).start()
            if kind == A0:
                y_copy(ref, 0).start()
            if kind == A1 and (s < steps or way == 1):
                unpack(mine, origin(way, s))

    def leap_sem(kind, k):
        return z_recv.at[2 * X * steps + (kind - X) * (steps // 2) + k - 1]

    def leap_send(kind, k):
        for far in (True, False):
            for way in range(2):
                part = way if far and 2 * k == steps else None
                ref = piece(kind, origin(way, 2 * k - 2), part)
                where = z_two[way] if far else (z_right, z_left)[way]
                remote(ref, ref, z_send.at[kind], leap_sem(kind, k), where).start()

    def leap(kind, k):
        ref = many(kind, 4 if 2 * k < steps else 3)
        remote(ref, ref, z_send.at[kind], leap_sem(kind, k), z_right).wait_recv()
        if 2 * k < steps:
            leap_send(kind, k + 1)
        for way, d in ((0, 2 * k), (1, 2 * k), (0, 2 * k - 1), (1, 2 * k - 1)):
            if d == steps and way == 1:
                continue
            if kind == X:
                y_copy(piece(X, origin(way, d)), 2).start()
            if kind == M:
                spread_mix(origin(way, d))

    def block(buf, w, q, b, part=None):
        rws = slice(None) if part is None else pl.ds(part * half, half)
        return buf.at[q, rws, pl.ds(pl.multiple_of(b * w, w), w)]

    def ag_copy(n, ref, slot, i, where):
        return remote(ref, ref, ag_send.at[n], ag_recv.at[slot, i], where)

    def ag_slot(n, q):
        return q // nq if n == 0 else 2 + (n - 1) * nq + q

    def ag_chunks(n, q):
        return slice(q, q + nq) if n == 0 else q

    def ag_start(n, buf, w, q):
        slot, own = ag_slot(n, q), block(buf, w, ag_chunks(n, q), t)
        ag_copy(n, own, slot, 0, x_right).start()
        ag_copy(n, own, slot, 0, x_left).start()
        ag_copy(n, own, slot, 2, sib).start()

    def ag_wait(n, buf, w, q, i, count):
        ag_copy(n, buf.at[ag_chunks(n, q), :, 0 : count * w], ag_slot(n, q), i, sib).wait_recv()

    def ag_relay(n, buf, w, q):
        slot, c = ag_slot(n, q), ag_chunks(n, q)
        b_l, b_r = 2 * xl + core, 2 * xr + core
        ag_wait(n, buf, w, q, 0, 2)
        ag_copy(n, block(buf, w, c, b_l, 0), slot, 1, x_right).start()
        ag_copy(n, block(buf, w, c, b_r, 1), slot, 1, x_left).start()
        ag_copy(n, block(buf, w, c, b_l), slot, 2, sib).start()
        ag_copy(n, block(buf, w, c, b_r), slot, 2, sib).start()

    def ag_opposite(n, buf, w, q):
        ag_wait(n, buf, w, q, 1, 1)
        ag_copy(n, block(buf, w, ag_chunks(n, q), 2 * xo + core), ag_slot(n, q), 2, sib).start()

    def ag_end(n, buf, w, q):
        ag_wait(n, buf, w, q, 2, 4)

    def ag_drain(n, buf, w):
        ag_copy(n, buf.at[:, :, 0 : 7 * w], 0, 0, sib).wait_send()

    order = (xo, xr, xl, x)
    rs_refs = (rs0, rs1)

    def rs_copy(src, dst, n, q, i, where):
        return remote(
            rs_refs[n].at[(q, *src)], rs_refs[n].at[(q, *dst)], rs_send.at[n], rs_recv.at[2 * nq * n + q, i], where
        )

    def sib_copy(n, q):
        return rs_copy((slice(0, 4),), (slice(4, 8),), n, q, 0, sib)

    def opp_copy(n, q, i):
        part = pl.ds(i * half, half)
        return rs_copy((8, part), (9, part), n, q, 1, x_right if i == 0 else x_left)

    def nb_copy(n, q, i):
        return rs_copy((10 + i,), (12 + i,), n, q, 2, x_right if i == 0 else x_left)

    def rs_partials(n, q):
        buf = rs_refs[n]
        width_k = units if n == 0 else 2 * units
        k_range = pl.ds(pl.multiple_of(mine * units, LANES), units) if n == 0 else slice(None)
        h = hid[q * rows : (q + 1) * rows, 0:width_k]
        for k in range(4):
            buf[q, k] = jnp.dot(h, wd[2 * order[k] + other, k_range, :], preferred_element_type=F32).astype(BF16)
        sib_copy(n, q).start()
        for k in range(4):
            acc[q, k] = jnp.dot(h, wd[2 * order[k] + core, k_range, :], preferred_element_type=F32)

    def rs_opposite(n, q):
        buf = rs_refs[n]
        sib_copy(n, q).wait_recv()
        buf[q, 8] = (acc[q, 0] + buf[q, 4].astype(F32)).astype(BF16)
        opp_copy(n, q, 0).start()
        opp_copy(n, q, 1).start()

    def rs_neighbours(n, q):
        buf = rs_refs[n]
        rs_copy((9,), (9,), n, q, 1, sib).wait_recv()
        for i in range(2):
            near, far = pl.ds(i * half, half), pl.ds((1 - i) * half, half)
            buf[q, 10 + i, near] = (
                acc[q, 1 + i, near] + buf[q, 5 + i, near].astype(F32) + buf[q, 9, near].astype(F32)
            ).astype(BF16)
            buf[q, 10 + i, far] = (acc[q, 1 + i, far] + buf[q, 5 + i, far].astype(F32)).astype(BF16)
            nb_copy(n, q, i).start()

    def rs_total(n, q):
        buf = rs_refs[n]
        rs_copy((slice(12, 14),), (slice(12, 14),), n, q, 2, sib).wait_recv()
        return acc[q, 3] + buf[q, 7].astype(F32) + buf[q, 12].astype(F32) + buf[q, 13].astype(F32)

    def rs_drain(n):
        ref = rs_refs[n].at[:, 0:7]
        remote(ref, ref, rs_send.at[n], rs_recv.at[0, 0], sib).wait_send()

    def norm_rows(buf, q, r, base):
        @pl.loop(0, rows // 16, unroll=4)
        def _(i):
            rws = pl.ds(pl.multiple_of(i * 16, 16), 16)
            v = buf[q, rws, :].astype(F32)
            inverse = lax.rsqrt(jnp.sum(v * v, axis=1, keepdims=True) / feat + EPS)
            ub[pl.ds(pl.multiple_of(base + i * 16, 16), 16), :] = (v * inverse * gf[r : r + 1, :]).astype(BF16)

    def gate_up(a, b):
        return (jax.nn.silu(a) * b).astype(BF16)

    def hidden_rows(lo, count, columns, n_pairs):
        r = jnp.dot(ub[lo : lo + count, :], gu[:, columns], preferred_element_type=F32)
        for n in range(n_pairs):
            a, b = r[:, 2 * n * LANES : (2 * n + 1) * LANES], r[:, (2 * n + 1) * LANES : (2 * n + 2) * LANES]
            hid[lo : lo + count, n * LANES : (n + 1) * LANES] = gate_up(a, b)

    my_half = pl.ds(pl.multiple_of(mine * 2 * units, LANES), 2 * units)

    def pair_sum(s, lo, count):
        up = lax.rem(z + s, 2) == 1
        f = jnp.where(up, lax.rem(z + s - 1, n_fs), lax.rem(z + n_fs - s, n_fs))
        ks = pl.ds(pl.multiple_of(f // 2 * (2 * k_rows), 2 * k_rows), 2 * k_rows)
        return jnp.dot(ub[lo : lo + count, ks], gu[ks, my_half], preferred_element_type=F32)

    def gather_pair(s, lo, count):
        r = pair_sum(s, lo, count)
        part[lo : lo + count, :] = r if s == 1 else part[lo : lo + count, :] + r

    def last_pair(lo, count):
        r = part[lo : lo + count, :] + pair_sum(steps, lo, count)
        for n in range(pairs):
            a, b = r[:, 2 * n * LANES : (2 * n + 1) * LANES], r[:, (2 * n + 1) * LANES : (2 * n + 2) * LANES]
            hid[lo : lo + count, n * LANES : (n + 1) * LANES] = gate_up(a, b)

    def conv(q):
        r = jnp.dot(ub[q * rows : (q + 1) * rows, :], vm[:, : 2 * chan_w], preferred_element_type=F32)
        glued = r[:, :chan_w] * jax.nn.sigmoid(r[:, chan_w:])
        for i in range(rows // LEN):
            pad[i, 32:, :] = glued[i * LEN : (i + 1) * LEN]
        n_taps = taps_in.shape[0]
        taps = taps_in[...].astype(F32)
        for i in range(rows // LEN):
            total = jnp.zeros((LEN, chan_w), F32)
            for k in range(n_taps):
                total = total + taps[k : k + 1, :] * pad[i, 33 - n_taps + k : 33 - n_taps + k + LEN, :]
            cvb[q, i * LEN : (i + 1) * LEN, pl.ds(pl.multiple_of(t * chan_w, chan_w), chan_w)] = total.astype(BF16)

    def channel_norm(q):
        @pl.loop(0, rows // 16, unroll=4)
        def _(i):
            rws = pl.ds(pl.multiple_of(i * 16, 16), 16)
            v = cvb[q, rws, :].astype(F32)
            mu = jnp.sum(v, axis=1, keepdims=True) / chan
            msq = jnp.sum(v * v, axis=1, keepdims=True) / chan
            w = (v - mu) * lax.rsqrt(msq - mu * mu + EPS) * cgb[3:4, :] + cgb[11:12, :]
            mixed[rws, :] = jax.nn.silu(w).astype(BF16)

    def own_cols(buf, q):
        return buf[q, :, own_w]

    def z_begin(kinds):
        for kind in kinds:
            for way in range(2):
                z_copy(kind, way, 1).start()

    def relays(kinds, s):
        for kind in kinds:
            relay(kind, s)

    first_kinds = (A0, A1, B)

    def phase(name):
        return jax.named_scope(name)

    chunks = range(nq)
    z_begin(first_kinds)
    for q in chunks:
        stream_copy(q).start()
    ag_start(0, sb0, width, nq)

    def pk_copy(i):
        return remote(pk.at[t], pk.at[t], pk_send.at[0], pk_recv.at[0], {"tp": lax.rem(t + i, n_tp)})

    pk_all = remote(pk.at[0 : n_tp - 1], pk.at[0 : n_tp - 1], pk_send.at[0], pk_recv.at[0], sib)

    for i in range(1, n_tp):
        pk_copy(i).start()
    spread_mix(z)
    pad[:, :32, :] = jnp.zeros((pad.shape[0], 32, chan_w), F32)

    with phase("w1"):
        relays(first_kinds, 1)
    with phase("ag0"):
        ref = sb0.at[0:nq, :, 0:width]
        remote(ref, ref, yx_send.at[0], yx_recv.at[nq], partner).wait_recv()
        ag_start(0, sb0, width, 0)
        ag_relay(0, sb0, width, nq)
    with phase("w2"):
        relays(first_kinds, 2)
    ag_relay(0, sb0, width, 0)
    ag_opposite(0, sb0, width, nq)
    with phase("w3"):
        relays(first_kinds, 3)
    ag_opposite(0, sb0, width, 0)
    ag_end(0, sb0, width, nq)
    pk_all.wait_recv()
    for b in range(n_tp):
        gf[:, b * width : (b + 1) * width] = pk[b]
        cgb[0:8, b * chan_w : (b + 1) * chan_w] = pk[b][:, :chan_w]
        cgb[8:16, b * chan_w : (b + 1) * chan_w] = pk[b][:, chan_w : 2 * chan_w]
    tokens = nq * rows
    pl.loop(nq, 2 * nq)(lambda q: norm_rows(sb0, q, 0, q * rows))
    with phase("w4"):
        relays(first_kinds, 4)
    ag_end(0, sb0, width, 0)
    pl.loop(0, nq)(lambda q: norm_rows(sb0, q, 0, q * rows))

    def relay_and_sum(s, work):
        for kind, some in zip(first_kinds, work):
            relay(kind, s)
            for i, lo in some:
                gather_pair(i, lo, tokens)

    with phase("w5"):
        relay_and_sum(5, (((1, 0),), ((1, tokens),), ((2, 0), (2, tokens))))
    with phase("w6"):
        relay_and_sum(6, (((3, 0),), ((3, tokens),), ((4, 0), (4, tokens))))
    with phase("w7"):
        relay_and_sum(7, (((5, 0),), ((5, tokens), (6, 0)), ((6, tokens), (7, 0), (7, tokens))))
    leap_send(X, 1)
    with phase("w8"):
        relays((A0, A1), 8)

    def late(*steps_of):
        with phase("late"):
            for kind, i in steps_of:
                leap(kind, i)

    def y_late(lo, hi):
        @pl.loop(lo, hi)
        def _(i):
            y_copy(piece(A1, lax.rem(z + i, n_fs)), 1).start()

    with phase("hid_theirs"):
        last_pair(0, tokens)
    with phase("w8b"):
        relay(B, 8)
    with phase("part_theirs"):
        for q in chunks:
            rs_partials(0, q)
    with phase("hid_ours"):
        last_pair(tokens, tokens)
    late((X, 1))
    leap_send(M, 1)
    y_late(1, 8)

    def pass_over(q):
        ybo[q] = rs_total(0, q).astype(BF16)
        part_copy(q).start()

    def first(q):
        total = rs_total(0, nq + q)
        part_copy(q).wait_recv()
        sb1[q, :, own_w] = (own_cols(sb0, nq + q).astype(F32) + 0.5 * (total + ybi[q].astype(F32))).astype(BF16)
        ag_start(1, sb1, width, q)

    with phase("rs_a"):
        for q in chunks:
            rs_opposite(0, q)
            rs_partials(0, nq + q)
        for q in chunks:
            rs_opposite(0, nq + q)
    with phase("rs_b"):
        rs_neighbours(0, 0)
        rs_neighbours(0, 1)
    late((X, 2), (M, 1))
    leap_send(D, 1)
    with phase("rs_c"):
        rs_neighbours(0, 2)
        rs_neighbours(0, nq)
        pass_over(0)
        rs_neighbours(0, nq + 1)
        pass_over(1)
    late((X, 3), (M, 2))
    with phase("rs_d"):
        rs_neighbours(0, nq + 2)
        pass_over(2)
    with phase("first"):
        for q in chunks:
            first(q)
    late((X, 4), (M, 3), (D, 1))
    y_late(8, n_fs)
    pl.loop(1, n_fs)(lambda i: y_copy(piece(Y, lax.rem(z + i, n_fs)), 3).start())
    with phase("ag1"):
        for q in chunks:
            ag_relay(1, sb1, width, q)
    late((M, 4))
    with phase("opp1"):
        ag_opposite(1, sb1, width, 0)
        ag_opposite(1, sb1, width, 1)

    def conv_stage(q):
        ag_end(1, sb1, width, q)
        norm_rows(sb1, q, 1, q * rows)
        conv(q)
        ag_start(2, cvb, chan_w, q)

    with phase("ywaitx"):
        y_all(2).wait_recv()
    with phase("conv0"):
        conv_stage(0)
    with phase("conv12"):
        ag_opposite(1, sb1, width, 2)
        conv_stage(1)
        conv_stage(2)
    late((D, 2))
    with phase("ag2"):
        for q in chunks:
            ag_relay(2, cvb, chan_w, q)
        y_all(1).wait_recv()
        pl.loop(1, n_fs)(lambda i: unpack(theirs, lax.rem(z + i, n_fs)))
        ag_opposite(2, cvb, chan_w, 0)
        ag_opposite(2, cvb, chan_w, 1)

    def mix_stage(q):
        ag_end(2, cvb, chan_w, q)
        channel_norm(q)
        branch = jnp.dot(mixed[...], mxb[...], preferred_element_type=F32)
        sb3[q, :, own_w] = (own_cols(sb1, q).astype(F32) + branch).astype(BF16)
        ag_start(3, sb3, width, q)

    with phase("mixw"):
        pltpu.make_async_copy(mxb, mxb, mx_recv.at[0]).wait()
    with phase("mix0"):
        mix_stage(0)
    with phase("mix12"):
        ag_opposite(2, cvb, chan_w, 2)
        mix_stage(1)
        mix_stage(2)
    late((D, 3))
    with phase("ag3"):
        for q in chunks:
            ag_relay(3, sb3, width, q)
        ag_opposite(3, sb3, width, 0)
        ag_opposite(3, sb3, width, 1)
    late((D, 4))
    with phase("ywait"):
        y_all(0).wait_recv()
        y_all(3).wait_recv()

    def ffn_stage(q):
        ag_end(3, sb3, width, q)
        norm_rows(sb3, q, 2, q * rows)
        hidden_rows(q * rows, rows, slice(None), 2 * pairs)
        rs_partials(1, q)

    def last(q):
        total = rs_total(1, q)
        out[q * rows : (q + 1) * rows, :] = (own_cols(sb3, q).astype(F32) + 0.5 * total).astype(BF16)

    with phase("ffn0"):
        ffn_stage(0)
    with phase("ffn1"):
        ag_opposite(3, sb3, width, 2)
        ffn_stage(1)
    with phase("ffn2"):
        rs_opposite(1, 0)
        ffn_stage(2)
    with phase("rs1"):
        rs_opposite(1, 1)
        rs_opposite(1, 2)
        for q in chunks:
            rs_neighbours(1, q)
    with phase("last"):
        for q in chunks:
            last(q)

    for kind in range(6):
        ref = many(kind, n_fs - 1)
        remote(ref, ref, z_send.at[kind], z_recv.at[0], z_right).wait_send()
    for i in range(4):
        y_all(i).wait_send()
    pk_all.wait_send()
    ref = mxb.at[pl.ds(0, (n_tp - 1) * chan_w), :]
    remote(ref, ref, mx_send.at[0], mx_recv.at[0], sib).wait_send()
    ref = sb0.at[0:nq, :, 0:width]
    remote(ref, ref, yx_send.at[0], yx_recv.at[0], partner).wait_send()
    remote(ybo, ybo, yx_send.at[1], yx_recv.at[0], partner).wait_send()
    for n, buf, w in ((0, sb0, width), (1, sb1, width), (2, cvb, chan_w), (3, sb3, width)):
        ag_drain(n, buf, w)
    for n in range(2):
        rs_drain(n)


def solution(mesh):
    n_fs, n_tp = mesh.shape["fs"], mesh.shape["tp"]

    def local(
        stream_in,
        gain_before,
        gain_mixer,
        gain_after,
        w_gate,
        w_upward,
        w_down,
        w_value,
        w_glu_gate,
        conv_taps,
        chan_gain,
        chan_bias,
        w_mix_out,
    ):
        tokens, width = stream_in.shape
        k_rows, hidden = w_gate.shape
        chan_w = w_value.shape[1]
        units = -(-(hidden // 2) // LANES) * LANES
        nq = CHUNKS
        rows = tokens // nq
        feat, chan = width * n_tp, chan_w * n_tp
        vmem = pltpu.VMEM
        dma = pltpu.SemaphoreType.DMA
        any_space = pl.BlockSpec(memory_space=pl.ANY)
        in_vmem = pl.BlockSpec(memory_space=pltpu.VMEM)
        return pl.pallas_call(
            lambda *refs: layer_kernel(n_fs, n_tp, *refs),
            out_shape=jax.ShapeDtypeStruct((tokens, width), BF16),
            in_specs=[any_space] * 7 + [in_vmem] * 6,
            out_specs=in_vmem,
            scratch_shapes=[
                vmem((n_fs * k_rows, 4 * units), BF16),
                vmem((n_fs // 2, 2 * units, 2 * LANES), BF16),
                vmem((n_fs * k_rows, 3 * chan_w), BF16),
                vmem((chan, 2 * LANES), BF16),
                vmem((n_tp, 8, width), F32),
                vmem((8, feat), F32),
                vmem((16, chan), F32),
                vmem((2 * nq, rows, feat), BF16),
                vmem((nq, rows, feat), BF16),
                vmem((nq, rows, feat), BF16),
                vmem((nq, rows, chan), BF16),
                vmem((2 * tokens, feat), BF16),
                vmem((rows, chan), BF16),
                vmem((2 * tokens, 2 * units), BF16),
                vmem((rows // LEN, LEN + 32, chan_w), F32),
                vmem((nq, rows, width), BF16),
                vmem((nq, rows, width), BF16),
                vmem((2 * nq, 4, rows, width), F32),
                vmem((2 * nq, 14, rows, width), BF16),
                vmem((nq, 14, rows, width), BF16),
                dma((5,)),
                dma((6 * (n_fs // 2) + 3 * (n_fs // 4),)),
                dma((6,)),
                dma((4,)),
                dma((4,)),
                dma((1,)),
                dma((1,)),
                dma((1,)),
                dma((1,)),
                dma((2 + 3 * nq, 3)),
                dma((4,)),
                dma((3 * nq, 3)),
                dma((2,)),
                dma((nq + 1,)),
                dma((2,)),
                vmem((2 * tokens, 2 * units), F32),
                vmem((2, n_fs, 2 * ((hidden // 2 - 1) % LANES + 1), k_rows), BF16),
                vmem((2, hidden, k_rows), BF16),
            ],
            compiler_params=pltpu.CompilerParams(
                collective_id=0, has_side_effects=True, vmem_limit_bytes=60 * 1024 * 1024
            ),
        )(
            stream_in,
            w_gate.T,
            w_upward.T,
            w_down,
            w_value,
            w_glu_gate,
            w_mix_out,
            conv_taps,
            gain_before,
            gain_mixer,
            gain_after,
            chan_gain,
            chan_bias,
        )

    in_specs = (
        P(("grp", "fs"), "tp"),
        P("tp"),
        P("tp"),
        P("tp"),
        P("fs", "tp"),
        P("fs", "tp"),
        P("tp", "fs"),
        P("fs", "tp"),
        P("fs", "tp"),
        P(None, "tp"),
        P("tp"),
        P("tp"),
        P("tp", "fs"),
    )
    out_specs = P(("grp", "fs"), "tp")
    return jax.shard_map(local, mesh=mesh, in_specs=in_specs, out_specs=out_specs, check_vma=False)
```

```python
import jax
import jax.numpy as jnp
from jax import lax
from jax.experimental import pallas as pl
from jax.experimental.pallas import tpu as pltpu
from jax.sharding import PartitionSpec as P

MESH = pl.DeviceIdType.MESH
LEN = 128
EPS = 1e-06
LANES = 128
CHUNKS = 3
BF16, F32 = jnp.bfloat16, jnp.float32


def remote(src, dst, send_sem, recv_sem, where):
    return pltpu.make_async_remote_copy(
        src_ref=src,
        dst_ref=dst,
        send_sem=send_sem,
        recv_sem=recv_sem,
        device_id=where,
        device_id_type=MESH,
    )


def layer_kernel(
    n_fs,
    n_tp,
    s_in,
    gate_in,
    up_in,
    wd_in,
    value_in,
    glu_in,
    mix_in,
    taps_in,
    before_in,
    mixer_in,
    after_in,
    cgain_in,
    cbias_in,
    out,
    gu,
    wd,
    vm,
    mxb,
    pk,
    gf,
    cgb,
    sb0,
    sb1,
    sb3,
    cvb,
    ub,
    mixed,
    hid,
    pad,
    ybo,
    ybi,
    acc,
    rs0,
    rs1,
    load_sem,
    z_recv,
    z_send,
    y_recv,
    y_send,
    pk_recv,
    pk_send,
    mx_recv,
    mx_send,
    ag_recv,
    ag_send,
    rs_recv,
    rs_send,
    yx_recv,
    yx_send,
    part,
    g3,
    shard,
):
    z, t, g = lax.axis_index("fs"), lax.axis_index("tp"), lax.axis_index("grp")
    parity = lax.rem(g, 2)
    partner = {"grp": g + 1 - 2 * parity}
    z_right = {"fs": lax.rem(z + 1, n_fs)}
    z_left = {"fs": lax.rem(z + n_fs - 1, n_fs)}
    z_two = ({"fs": lax.rem(z + 2, n_fs)}, {"fs": lax.rem(z + n_fs - 2, n_fs)})
    chips = n_tp // 2
    x, core = t // 2, lax.rem(t, 2)
    xr, xl, xo = lax.rem(x + 1, chips), lax.rem(x + 3, chips), lax.rem(x + 2, chips)
    other = 1 - core
    sib = {"tp": 2 * x + other}
    x_right, x_left = {"tp": 2 * xr + core}, {"tp": 2 * xl + core}

    nq, rows, width = sb1.shape[0], sb1.shape[1], s_in.shape[1]
    half = rows // 2
    feat = width * n_tp
    k_rows, chan_w = value_in.shape
    chan = chan_w * n_tp
    steps = n_fs // 2
    own_units = gate_in.shape[0] // 2
    units = wd.shape[1] // 2
    pairs = units // LANES
    mine, theirs = parity, 1 - parity

    own_k = pl.ds(pl.multiple_of(z * k_rows, k_rows), k_rows)

    own_w = pl.ds(pl.multiple_of(t * width, width), width)

    rest = g3.shape[2] // 2

    def own_loads():
        for j, ref in enumerate((gate_in, up_in)):
            yield pltpu.make_async_copy(ref, shard.at[j], load_sem.at[3])
            for h in range(2):
                yield pltpu.make_async_copy(
                    ref.at[(h + 1) * own_units - rest : (h + 1) * own_units, :],
                    g3.at[h, z, j * rest : (j + 1) * rest, :],
                    load_sem.at[4],
                )
        for h in range(2):
            yield pltpu.make_async_copy(
                wd_in.at[h * own_units : (h + 1) * own_units, :],
                wd.at[
                    z // 2,
                    h * units : h * units + own_units,
                    pl.ds(pl.multiple_of(lax.rem(z, 2) * LANES, LANES), LANES),
                ],
                load_sem.at[0],
            )
        for i, ref in enumerate((value_in, glu_in, mix_in)):
            yield pltpu.make_async_copy(ref, vm.at[own_k, i * chan_w : (i + 1) * chan_w], load_sem.at[1])
        for q in range(nq):
            yield pltpu.make_async_copy(
                s_in.at[pl.ds(q * rows, rows), :],
                sb0.at[nq + q, :, pl.ds(pl.multiple_of(t * width, width), width)],
                load_sem.at[2],
            )

    for copy in own_loads():
        copy.start()

    barrier = pltpu.get_barrier_semaphore()
    peers = [z_right, z_left, *z_two, partner] + [{"tp": lax.rem(t + i, n_tp)} for i in range(1, n_tp)]
    for peer in peers:
        pl.semaphore_signal(barrier, inc=1, device_id=peer, device_id_type=MESH)

    def unpack(h, f):
        rws = pl.ds(pl.multiple_of(f * k_rows, k_rows), k_rows)
        for j in range(2):
            v = jnp.concatenate([g3[h, f, j * rest : (j + 1) * rest, :], jnp.zeros((LANES - rest, k_rows), BF16)], axis=0)
            c = pl.multiple_of(h * 2 * units + 2 * units - (2 - j) * LANES, LANES)
            gu[rws, pl.ds(c, LANES)] = v.T

    pltpu.make_async_copy(shard, shard, load_sem.at[3]).wait()
    pltpu.make_async_copy(g3.at[:, z], g3.at[:, z], load_sem.at[4]).wait()
    for h in range(2):
        for i in range(pairs - 1):
            for j in range(2):
                lo, c = h * own_units + i * LANES, h * 2 * units + (2 * i + j) * LANES
                gu[own_k, c : c + LANES] = shard[j, lo : lo + LANES, :].T
        unpack(h, z)
        wd[:, h * units + own_units : (h + 1) * units, :] = jnp.zeros((wd.shape[0], units - own_units, wd.shape[2]), BF16)
    for i, ref in enumerate((before_in, mixer_in, after_in)):
        pk[t, i : i + 1, :] = ref[...].astype(F32).reshape(1, width)
    pk[t, 3:4, :chan_w] = cgain_in[...].astype(F32).reshape(1, chan_w)
    pk[t, 3:4, chan_w:] = cbias_in[...].astype(F32).reshape(1, chan_w)
    pk[t, 4:8, :] = jnp.zeros((4, width), F32)

    pl.semaphore_wait(barrier, len(peers))

    ref = vm.at[own_k, :]
    pltpu.make_async_copy(wd_in, wd_in, load_sem.at[0]).wait()
    pltpu.make_async_copy(ref, ref, load_sem.at[1]).wait()
    pltpu.make_async_copy(s_in, s_in, load_sem.at[2]).wait()

    wide = 2 * LANES * (pairs - 1)
    A0, A1, B, X, M, D = range(6)

    def piece(kind, f, part=None):
        if kind in (B, D):
            size = own_units if part is None else own_units // 2
            q0 = (mine if kind == B else theirs) * units + (0 if part is None else part * size)
            return wd.at[
                f // 2,
                pl.ds(pl.multiple_of(q0, 16), size),
                pl.ds(pl.multiple_of(lax.rem(f, 2) * LANES, LANES), LANES),
            ]
        if kind == A1:
            return g3.at[mine, f] if part is None else g3.at[mine, f, part * rest : (part + 1) * rest]
        size = k_rows if part is None else k_rows // 2
        r0 = pl.ds(pl.multiple_of(f * k_rows + (0 if part is None else part * size), size), size)
        c0 = mine * 2 * units
        if kind == A0:
            return gu.at[r0, pl.ds(pl.multiple_of(c0, LANES), wide)]
        if kind == X:
            return vm.at[r0, pl.ds(pl.multiple_of(mine * chan_w, LANES), chan_w)]
        return vm.at[r0, 2 * chan_w : 3 * chan_w]

    def many(kind, count):
        if kind in (B, D):
            if count <= wd.shape[0]:
                return wd.at[0:count, 0:own_units, 0:LANES]
            total = count * own_units // 2
            for a in range(1, wd.shape[0] + 1):
                if total % (16 * a) == 0 and total // a <= wd.shape[1]:
                    return wd.at[0:a, 0 : total // a, :]
        if kind == A0:
            return gu.at[0 : count * k_rows, 0:wide]
        if kind == A1:
            return g3.at[0, 0:count]
        return vm.at[0 : count * k_rows, 0:chan_w]

    def origin(way, s):
        return lax.rem(z + n_fs - s, n_fs) if way == 0 else lax.rem(z + s, n_fs)

    def z_sem(kind, way, s):
        return z_recv.at[(kind * 2 + way) * steps + s - 1]

    def z_copy(kind, way, s_next):
        ref = piece(kind, origin(way, s_next - 1), None if s_next < steps else way)
        return remote(ref, ref, z_send.at[kind], z_sem(kind, way, s_next), z_right if way == 0 else z_left)

    def y_copy(ref, i):
        return remote(ref, ref, y_send.at[i], y_recv.at[i], partner)

    def y_all(i):
        return y_copy(many((A0, A1, X)[i], n_fs - 1), i)

    def stream_copy(q):
        return remote(sb0.at[nq + q, :, own_w], sb0.at[q, :, own_w], yx_send.at[0], yx_recv.at[nq], partner)

    def part_copy(q):
        return remote(ybo.at[q], ybi.at[q], yx_send.at[1], yx_recv.at[q], partner)

    def spread_mix(f):
        dest, b = f // 2, lax.rem(f, 2)
        src = piece(M, f)
        dst = mxb.at[
            pl.ds(pl.multiple_of(t * chan_w, chan_w), chan_w), pl.ds(pl.multiple_of(b * LANES, LANES), LANES)
        ]

        @pl.when(dest != t)
        def _():
            remote(src, dst, mx_send.at[0], mx_recv.at[0], {"tp": dest}).start()

        @pl.when(dest == t)
        def _():
            pltpu.make_async_copy(src, dst, mx_recv.at[0]).start()

    def relay(kind, s):
        for way in range(2):
            part = None if s < steps else way
            ref = piece(kind, origin(way, s), part)
            remote(ref, ref, z_send.at[kind], z_sem(kind, way, s), z_right).wait_recv()
            if s < steps:
                z_copy(kind, way, s + 1).start()
            if kind == A0:
                y_copy(ref, 0).start()
            if kind == A1 and (s < steps or way == 1):
                unpack(mine, origin(way, s))

    def leap_sem(kind, k):
        return z_recv.at[2 * X * steps + (kind - X) * (steps // 2) + k - 1]

    def leap_send(kind, k):
        for far in (True, False):
            for way in range(2):
                part = way if far and 2 * k == steps else None
                ref = piece(kind, origin(way, 2 * k - 2), part)
                where = z_two[way] if far else (z_right, z_left)[way]
                remote(ref, ref, z_send.at[kind], leap_sem(kind, k), where).start()

    def leap(kind, k):
        ref = many(kind, 4 if 2 * k < steps else 3)
        remote(ref, ref, z_send.at[kind], leap_sem(kind, k), z_right).wait_recv()
        if 2 * k < steps:
            leap_send(kind, k + 1)
        for way, d in ((0, 2 * k), (1, 2 * k), (0, 2 * k - 1), (1, 2 * k - 1)):
            if d == steps and way == 1:
                continue
            if kind == X:
                y_copy(piece(X, origin(way, d)), 2).start()
            if kind == M:
                spread_mix(origin(way, d))

    def block(buf, w, q, b, part=None):
        rws = slice(None) if part is None else pl.ds(part * half, half)
        return buf.at[q, rws, pl.ds(pl.multiple_of(b * w, w), w)]

    def ag_copy(n, ref, slot, i, where):
        return remote(ref, ref, ag_send.at[n], ag_recv.at[slot, i], where)

    def ag_slot(n, q):
        return q // nq if n == 0 else 2 + (n - 1) * nq + q

    def ag_chunks(n, q):
        return slice(q, q + nq) if n == 0 else q

    def ag_start(n, buf, w, q):
        slot, own = ag_slot(n, q), block(buf, w, ag_chunks(n, q), t)
        ag_copy(n, own, slot, 0, x_right).start()
        ag_copy(n, own, slot, 0, x_left).start()
        ag_copy(n, own, slot, 2, sib).start()

    def ag_wait(n, buf, w, q, i, count):
        ag_copy(n, buf.at[ag_chunks(n, q), :, 0 : count * w], ag_slot(n, q), i, sib).wait_recv()

    def ag_relay(n, buf, w, q):
        slot, c = ag_slot(n, q), ag_chunks(n, q)
        b_l, b_r = 2 * xl + core, 2 * xr + core
        ag_wait(n, buf, w, q, 0, 2)
        ag_copy(n, block(buf, w, c, b_l, 0), slot, 1, x_right).start()
        ag_copy(n, block(buf, w, c, b_r, 1), slot, 1, x_left).start()
        ag_copy(n, block(buf, w, c, b_l), slot, 2, sib).start()
        ag_copy(n, block(buf, w, c, b_r), slot, 2, sib).start()

    def ag_opposite(n, buf, w, q):
        ag_wait(n, buf, w, q, 1, 1)
        ag_copy(n, block(buf, w, ag_chunks(n, q), 2 * xo + core), ag_slot(n, q), 2, sib).start()

    def ag_end(n, buf, w, q):
        ag_wait(n, buf, w, q, 2, 4)

    def ag_drain(n, buf, w):
        ag_copy(n, buf.at[:, :, 0 : 7 * w], 0, 0, sib).wait_send()

    order = (xo, xr, xl, x)
    rs_refs = (rs0, rs1)

    def rs_copy(src, dst, n, q, i, where):
        return remote(
            rs_refs[n].at[(q, *src)], rs_refs[n].at[(q, *dst)], rs_send.at[n], rs_recv.at[2 * nq * n + q, i], where
        )

    def sib_first(n, q):
        return rs_copy((0,), (4,), n, q, 0, sib)

    def sib_rest(n, q):
        return rs_copy((slice(1, 4),), (slice(5, 8),), n, q, 3, sib)

    def opp_copy(n, q, i):
        part = pl.ds(i * half, half)
        return rs_copy((8, part), (9, part), n, q, 1, x_right if i == 0 else x_left)

    def nb_copy(n, q, i):
        return rs_copy((10 + i,), (12 + i,), n, q, 2, x_right if i == 0 else x_left)

    def rs_partials(n, q):
        buf = rs_refs[n]
        width_k = units if n == 0 else 2 * units
        k_range = pl.ds(pl.multiple_of(mine * units, LANES), units) if n == 0 else slice(None)
        h = hid[q * rows : (q + 1) * rows, 0:width_k]

        def partial(k, side):
            return jnp.dot(h, wd[2 * order[k] + side, k_range, :], preferred_element_type=F32)

        buf[q, 0] = partial(0, other).astype(BF16)
        sib_first(n, q).start()
        for k in range(1, 4):
            buf[q, k] = partial(k, other).astype(BF16)
        sib_rest(n, q).start()
        for k in range(4):
            acc[q, k] = partial(k, core)

    def rs_opposite(n, q):
        buf = rs_refs[n]
        sib_first(n, q).wait_recv()
        buf[q, 8] = (acc[q, 0] + buf[q, 4].astype(F32)).astype(BF16)
        opp_copy(n, q, 0).start()
        opp_copy(n, q, 1).start()

    def rs_neighbours(n, q):
        buf = rs_refs[n]
        sib_rest(n, q).wait_recv()
        rs_copy((9,), (9,), n, q, 1, sib).wait_recv()
        for i in range(2):
            near, far = pl.ds(i * half, half), pl.ds((1 - i) * half, half)
            buf[q, 10 + i, near] = (
                acc[q, 1 + i, near] + buf[q, 5 + i, near].astype(F32) + buf[q, 9, near].astype(F32)
            ).astype(BF16)
            buf[q, 10 + i, far] = (acc[q, 1 + i, far] + buf[q, 5 + i, far].astype(F32)).astype(BF16)
            nb_copy(n, q, i).start()

    def rs_total(n, q):
        buf = rs_refs[n]
        rs_copy((slice(12, 14),), (slice(12, 14),), n, q, 2, sib).wait_recv()
        return acc[q, 3] + buf[q, 7].astype(F32) + buf[q, 12].astype(F32) + buf[q, 13].astype(F32)

    def rs_drain(n):
        ref = rs_refs[n].at[:, 0:7]
        remote(ref, ref, rs_send.at[n], rs_recv.at[0, 0], sib).wait_send()

    def norm_rows(buf, q, r, base):
        @pl.loop(0, rows // 16, unroll=4)
        def _(i):
            rws = pl.ds(pl.multiple_of(i * 16, 16), 16)
            v = buf[q, rws, :].astype(F32)
            inverse = lax.rsqrt(jnp.sum(v * v, axis=1, keepdims=True) / feat + EPS)
            ub[pl.ds(pl.multiple_of(base + i * 16, 16), 16), :] = (v * inverse * gf[r : r + 1, :]).astype(BF16)

    def gate_up(a, b):
        return (jax.nn.silu(a) * b).astype(BF16)

    def hidden_rows(lo, count, columns, n_pairs):
        r = jnp.dot(ub[lo : lo + count, :], gu[:, columns], preferred_element_type=F32)
        for n in range(n_pairs):
            a, b = r[:, 2 * n * LANES : (2 * n + 1) * LANES], r[:, (2 * n + 1) * LANES : (2 * n + 2) * LANES]
            hid[lo : lo + count, n * LANES : (n + 1) * LANES] = gate_up(a, b)

    my_half = pl.ds(pl.multiple_of(mine * 2 * units, LANES), 2 * units)

    def pair_sum(s, lo, count):
        up = lax.rem(z + s, 2) == 1
        f = jnp.where(up, lax.rem(z + s - 1, n_fs), lax.rem(z + n_fs - s, n_fs))
        ks = pl.ds(pl.multiple_of(f // 2 * (2 * k_rows), 2 * k_rows), 2 * k_rows)
        return jnp.dot(ub[lo : lo + count, ks], gu[ks, my_half], preferred_element_type=F32)

    def gather_pair(s, lo, count):
        r = pair_sum(s, lo, count)
        part[lo : lo + count, :] = r if s == 1 else part[lo : lo + count, :] + r

    def last_pair(lo, count):
        r = part[lo : lo + count, :] + pair_sum(steps, lo, count)
        for n in range(pairs):
            a, b = r[:, 2 * n * LANES : (2 * n + 1) * LANES], r[:, (2 * n + 1) * LANES : (2 * n + 2) * LANES]
            hid[lo : lo + count, n * LANES : (n + 1) * LANES] = gate_up(a, b)

    def conv(q):
        r = jnp.dot(ub[q * rows : (q + 1) * rows, :], vm[:, : 2 * chan_w], preferred_element_type=F32)
        glued = r[:, :chan_w] * jax.nn.sigmoid(r[:, chan_w:])
        for i in range(rows // LEN):
            pad[i, 32:, :] = glued[i * LEN : (i + 1) * LEN]
        n_taps = taps_in.shape[0]
        taps = taps_in[...].astype(F32)
        for i in range(rows // LEN):
            total = jnp.zeros((LEN, chan_w), F32)
            for k in range(n_taps):
                total = total + taps[k : k + 1, :] * pad[i, 33 - n_taps + k : 33 - n_taps + k + LEN, :]
            cvb[q, i * LEN : (i + 1) * LEN, pl.ds(pl.multiple_of(t * chan_w, chan_w), chan_w)] = total.astype(BF16)

    def channel_norm(q):
        @pl.loop(0, rows // 16, unroll=4)
        def _(i):
            rws = pl.ds(pl.multiple_of(i * 16, 16), 16)
            v = cvb[q, rws, :].astype(F32)
            mu = jnp.sum(v, axis=1, keepdims=True) / chan
            msq = jnp.sum(v * v, axis=1, keepdims=True) / chan
            w = (v - mu) * lax.rsqrt(msq - mu * mu + EPS) * cgb[3:4, :] + cgb[11:12, :]
            mixed[rws, :] = jax.nn.silu(w).astype(BF16)

    def own_cols(buf, q):
        return buf[q, :, own_w]

    def z_begin(kinds):
        for kind in kinds:
            for way in range(2):
                z_copy(kind, way, 1).start()

    def relays(kinds, s):
        for kind in kinds:
            relay(kind, s)

    first_kinds = (A0, A1, B)

    def phase(name):
        return jax.named_scope(name)

    chunks = range(nq)
    z_begin(first_kinds)
    for q in chunks:
        stream_copy(q).start()
    ag_start(0, sb0, width, nq)

    def pk_copy(i):
        return remote(pk.at[t], pk.at[t], pk_send.at[0], pk_recv.at[0], {"tp": lax.rem(t + i, n_tp)})

    pk_all = remote(pk.at[0 : n_tp - 1], pk.at[0 : n_tp - 1], pk_send.at[0], pk_recv.at[0], sib)

    for i in range(1, n_tp):
        pk_copy(i).start()
    spread_mix(z)
    pad[:, :32, :] = jnp.zeros((pad.shape[0], 32, chan_w), F32)

    with phase("w1"):
        relays(first_kinds, 1)
    with phase("ag0"):
        ref = sb0.at[0:nq, :, 0:width]
        remote(ref, ref, yx_send.at[0], yx_recv.at[nq], partner).wait_recv()
        ag_start(0, sb0, width, 0)
        ag_relay(0, sb0, width, nq)
    with phase("w2"):
        relays(first_kinds, 2)
    ag_relay(0, sb0, width, 0)
    ag_opposite(0, sb0, width, nq)
    with phase("w3"):
        relays(first_kinds, 3)
    ag_opposite(0, sb0, width, 0)
    ag_end(0, sb0, width, nq)
    pk_all.wait_recv()
    for b in range(n_tp):
        gf[:, b * width : (b + 1) * width] = pk[b]
        cgb[0:8, b * chan_w : (b + 1) * chan_w] = pk[b][:, :chan_w]
        cgb[8:16, b * chan_w : (b + 1) * chan_w] = pk[b][:, chan_w : 2 * chan_w]
    tokens = nq * rows
    pl.loop(nq, 2 * nq)(lambda q: norm_rows(sb0, q, 0, q * rows))
    with phase("w4"):
        relays(first_kinds, 4)
    ag_end(0, sb0, width, 0)
    pl.loop(0, nq)(lambda q: norm_rows(sb0, q, 0, q * rows))

    def relay_and_sum(s, work):
        for kind, some in zip(first_kinds, work):
            relay(kind, s)
            for i, lo in some:
                gather_pair(i, lo, tokens)

    with phase("w5"):
        relay_and_sum(5, (((1, 0),), ((1, tokens),), ((2, 0), (2, tokens))))
    with phase("w6"):
        relay_and_sum(6, (((3, 0),), ((3, tokens),), ((4, 0), (4, tokens))))
    with phase("w7"):
        relay_and_sum(7, (((5, 0),), ((5, tokens), (6, 0)), ((6, tokens), (7, 0), (7, tokens))))
    leap_send(X, 1)
    with phase("w8"):
        relays((A0, A1), 8)

    def late(*steps_of):
        with phase("late"):
            for kind, i in steps_of:
                leap(kind, i)

    def y_late(lo, hi):
        @pl.loop(lo, hi)
        def _(i):
            y_copy(piece(A1, lax.rem(z + i, n_fs)), 1).start()

    with phase("hid_theirs"):
        last_pair(0, tokens)
    with phase("w8b"):
        relay(B, 8)
    with phase("part_theirs"):
        for q in chunks:
            rs_partials(0, q)
    with phase("hid_ours"):
        last_pair(tokens, tokens)
    late((X, 1))
    leap_send(M, 1)
    y_late(1, 5)

    def pass_over(q):
        ybo[q] = rs_total(0, q).astype(BF16)
        part_copy(q).start()

    def first(q):
        total = rs_total(0, nq + q)
        part_copy(q).wait_recv()
        sb1[q, :, own_w] = (own_cols(sb0, nq + q).astype(F32) + 0.5 * (total + ybi[q].astype(F32))).astype(BF16)
        ag_start(1, sb1, width, q)

    with phase("rs_a"):
        for q in chunks:
            rs_opposite(0, q)
            rs_partials(0, nq + q)
        for q in chunks:
            rs_opposite(0, nq + q)
    with phase("rs_b"):
        rs_neighbours(0, 0)
    late((X, 2), (M, 1))
    leap_send(D, 1)
    with phase("rs_c"):
        rs_neighbours(0, 1)
        rs_neighbours(0, 2)
        rs_neighbours(0, nq)
        pass_over(0)
        rs_neighbours(0, nq + 1)
        pass_over(1)
    late((X, 3), (M, 2))
    with phase("rs_d"):
        rs_neighbours(0, nq + 2)
        pass_over(2)
    with phase("first"):
        for q in chunks:
            first(q)
    late((X, 4), (M, 3), (D, 1))
    y_late(5, n_fs)
    with phase("ag1"):
        for q in chunks:
            ag_relay(1, sb1, width, q)
    late((M, 4))
    with phase("opp1"):
        ag_opposite(1, sb1, width, 0)
        ag_opposite(1, sb1, width, 1)

    def conv_stage(q):
        ag_end(1, sb1, width, q)
        norm_rows(sb1, q, 1, q * rows)
        conv(q)
        ag_start(2, cvb, chan_w, q)

    with phase("ywaitx"):
        y_all(2).wait_recv()
    with phase("conv0"):
        conv_stage(0)
    with phase("conv12"):
        ag_opposite(1, sb1, width, 2)
        conv_stage(1)
        conv_stage(2)
    late((D, 2))
    with phase("ag2"):
        for q in chunks:
            ag_relay(2, cvb, chan_w, q)
        y_all(1).wait_recv()
        pl.loop(1, n_fs)(lambda i: unpack(theirs, lax.rem(z + i, n_fs)))
        ag_opposite(2, cvb, chan_w, 0)
        ag_opposite(2, cvb, chan_w, 1)

    def mix_stage(q):
        ag_end(2, cvb, chan_w, q)
        channel_norm(q)
        branch = jnp.dot(mixed[...], mxb[...], preferred_element_type=F32)
        sb3[q, :, own_w] = (own_cols(sb1, q).astype(F32) + branch).astype(BF16)
        ag_start(3, sb3, width, q)

    with phase("mixw"):
        pltpu.make_async_copy(mxb, mxb, mx_recv.at[0]).wait()
    with phase("mix0"):
        mix_stage(0)
    with phase("mix12"):
        ag_opposite(2, cvb, chan_w, 2)
        mix_stage(1)
        mix_stage(2)
    late((D, 3))
    with phase("ag3"):
        for q in chunks:
            ag_relay(3, sb3, width, q)
        ag_opposite(3, sb3, width, 0)
        ag_opposite(3, sb3, width, 1)
    late((D, 4))
    with phase("ywait"):
        y_all(0).wait_recv()

    def ffn_stage(q):
        ag_end(3, sb3, width, q)
        norm_rows(sb3, q, 2, q * rows)
        hidden_rows(q * rows, rows, slice(None), 2 * pairs)
        rs_partials(1, q)

    def last(q):
        total = rs_total(1, q)
        out[q * rows : (q + 1) * rows, :] = (own_cols(sb3, q).astype(F32) + 0.5 * total).astype(BF16)

    with phase("ffn0"):
        ffn_stage(0)
    with phase("ffn1"):
        ag_opposite(3, sb3, width, 2)
        ffn_stage(1)
    with phase("ffn2"):
        rs_opposite(1, 0)
        ffn_stage(2)
    with phase("rs1"):
        rs_opposite(1, 1)
        rs_opposite(1, 2)
        for q in chunks:
            rs_neighbours(1, q)
    with phase("last"):
        for q in chunks:
            last(q)

    for kind in range(6):
        ref = many(kind, n_fs - 1)
        remote(ref, ref, z_send.at[kind], z_recv.at[0], z_right).wait_send()
    for i in range(3):
        y_all(i).wait_send()
    pk_all.wait_send()
    ref = mxb.at[pl.ds(0, (n_tp - 1) * chan_w), :]
    remote(ref, ref, mx_send.at[0], mx_recv.at[0], sib).wait_send()
    ref = sb0.at[0:nq, :, 0:width]
    remote(ref, ref, yx_send.at[0], yx_recv.at[0], partner).wait_send()
    remote(ybo, ybo, yx_send.at[1], yx_recv.at[0], partner).wait_send()
    for n, buf, w in ((0, sb0, width), (1, sb1, width), (2, cvb, chan_w), (3, sb3, width)):
        ag_drain(n, buf, w)
    for n in range(2):
        rs_drain(n)


def solution(mesh):
    n_fs, n_tp = mesh.shape["fs"], mesh.shape["tp"]

    def local(
        stream_in,
        gain_before,
        gain_mixer,
        gain_after,
        w_gate,
        w_upward,
        w_down,
        w_value,
        w_glu_gate,
        conv_taps,
        chan_gain,
        chan_bias,
        w_mix_out,
    ):
        tokens, width = stream_in.shape
        k_rows, hidden = w_gate.shape
        chan_w = w_value.shape[1]
        units = -(-(hidden // 2) // LANES) * LANES
        nq = CHUNKS
        rows = tokens // nq
        feat, chan = width * n_tp, chan_w * n_tp
        vmem = pltpu.VMEM
        dma = pltpu.SemaphoreType.DMA
        any_space = pl.BlockSpec(memory_space=pl.ANY)
        in_vmem = pl.BlockSpec(memory_space=pltpu.VMEM)
        return pl.pallas_call(
            lambda *refs: layer_kernel(n_fs, n_tp, *refs),
            out_shape=jax.ShapeDtypeStruct((tokens, width), BF16),
            in_specs=[any_space] * 7 + [in_vmem] * 6,
            out_specs=in_vmem,
            scratch_shapes=[
                vmem((n_fs * k_rows, 4 * units), BF16),
                vmem((n_fs // 2, 2 * units, 2 * LANES), BF16),
                vmem((n_fs * k_rows, 3 * chan_w), BF16),
                vmem((chan, 2 * LANES), BF16),
                vmem((n_tp, 8, width), F32),
                vmem((8, feat), F32),
                vmem((16, chan), F32),
                vmem((2 * nq, rows, feat), BF16),
                vmem((nq, rows, feat), BF16),
                vmem((nq, rows, feat), BF16),
                vmem((nq, rows, chan), BF16),
                vmem((2 * tokens, feat), BF16),
                vmem((rows, chan), BF16),
                vmem((2 * tokens, 2 * units), BF16),
                vmem((rows // LEN, LEN + 32, chan_w), F32),
                vmem((nq, rows, width), BF16),
                vmem((nq, rows, width), BF16),
                vmem((2 * nq, 4, rows, width), F32),
                vmem((2 * nq, 14, rows, width), BF16),
                vmem((nq, 14, rows, width), BF16),
                dma((5,)),
                dma((6 * (n_fs // 2) + 3 * (n_fs // 4),)),
                dma((6,)),
                dma((3,)),
                dma((3,)),
                dma((1,)),
                dma((1,)),
                dma((1,)),
                dma((1,)),
                dma((2 + 3 * nq, 3)),
                dma((4,)),
                dma((3 * nq, 4)),
                dma((2,)),
                dma((nq + 1,)),
                dma((2,)),
                vmem((2 * tokens, 2 * units), F32),
                vmem((2, n_fs, 2 * ((hidden // 2 - 1) % LANES + 1), k_rows), BF16),
                vmem((2, hidden, k_rows), BF16),
            ],
            compiler_params=pltpu.CompilerParams(
                collective_id=0, has_side_effects=True, vmem_limit_bytes=60 * 1024 * 1024
            ),
        )(
            stream_in,
            w_gate.T,
            w_upward.T,
            w_down,
            w_value,
            w_glu_gate,
            w_mix_out,
            conv_taps,
            gain_before,
            gain_mixer,
            gain_after,
            chan_gain,
            chan_bias,
        )

    in_specs = (
        P(("grp", "fs"), "tp"),
        P("tp"),
        P("tp"),
        P("tp"),
        P("fs", "tp"),
        P("fs", "tp"),
        P("tp", "fs"),
        P("fs", "tp"),
        P("fs", "tp"),
        P(None, "tp"),
        P("tp"),
        P("tp"),
        P("tp", "fs"),
    )
    out_specs = P(("grp", "fs"), "tp")
    return jax.shard_map(local, mesh=mesh, in_specs=in_specs, out_specs=out_specs, check_vma=False)
```
